512 devices in a mesh: ra: 32 (over z, x), cb: 16 (over y, core).
Axes of the slice: x: 4, y: 8, z: 8, core: 2. Of those that a mesh axis runs over, the one named last changes fastest.
Arguments:
- tokens: bfloat16 [384, 4096], P(None, 'ra'), may hold values from -260 to 260
- up_weight: float32 [2, 4096, 16384], P(None, 'ra', 'cb'), may hold values from -0.1875 to 0.1875
- up_scale: float32 [2, 16384], P(None, 'cb'), may hold values from 0.5 to 2
- down_weight: float32 [2, 16384, 4096], P(None, 'cb', 'ra'), may hold values from -0.046875 to 0.046875
- down_scale: float32 [2, 4096], P(None, 'ra'), may hold values from 0.7 to 14
- pre_gain: float32 [2, 4096], P(None, 'ra'), may hold values from 0.1 to 1.9
- post_gain: float32 [2, 4096], P(None, 'ra'), may hold values from 0.1 to 1.9
Outputs:
- stream_out: bfloat16 [384, 4096], P(None, 'ra')
The draws below stay inside these ranges and needn't reach their ends.
All inputs are finite; a program needn't handle non-finite values.
Results may differ from the reference program's by a relative error of at most 0.023.
Values may be sent and summed in bfloat16 or wider, within the bound.
No kernel may reach another device: no remote copies, remote signals or barrier semaphores. Data moves between devices by JAX's collectives and lax.ppermute only.
A program may use at most 64 MiB of HBM per device.

```python
import math
import jax
import jax.numpy as jnp
from jax import lax

D = 4096
FF = 16384
LAYERS = 2
TOKENS = 384
N_CB = 16


def draw_tokens(key, part):
    first = jax.random.fold_in(key, 11)
    second = jax.random.fold_in(key, 12)
    third = jax.random.fold_in(key, 13)
    column_scale = 10.0 ** (jnp.arange(D, dtype=jnp.float32) / D) * jax.random.uniform(second, (D,), jnp.float32, 0.7, 1.4)
    row_scale = 10.0 ** jax.random.uniform(third, (TOKENS, 1), jnp.float32)
    base = jnp.clip(jax.random.normal(first, (TOKENS, D), jnp.float32), -6.0, 6.0)
    return (0.3 * base * row_scale * column_scale[None, :]).astype(jnp.bfloat16)


def draw_down_scale(key, part):
    first = jax.random.fold_in(key, 21)
    rising = 10.0 ** (jnp.arange(D, dtype=jnp.float32) / D)
    rough = jnp.exp(jax.random.uniform(first, (LAYERS, D), jnp.float32, jnp.log(0.7), jnp.log(1.4)))
    return (rough * rising[None, :]).astype(jnp.float32)


def strengthened(entries, rng, source, target, parts, factor):
    def block_of(dim):
        return (jnp.arange(entries.shape[dim]) // (entries.shape[dim] // parts)).reshape((-1,) + (1,) * (entries.ndim - 1 - dim))

    one_side = jax.random.permutation(rng, parts)[block_of(target)]
    second = (block_of(target) + parts // 2) % parts
    return jnp.where((block_of(source) == one_side) | (block_of(source) == second), factor * entries, entries)


def block_scale(stream_key, dims, shards, smallest, largest):
    def one(dim, shards_of):
        draws = jax.random.uniform(jax.random.fold_in(jax.random.fold_in(stream_key, 6), dim), (shards_of,), jnp.float32, smallest / len(shards), largest / len(shards))
        return jnp.repeat(jnp.exp(draws), dims[dim] // shards_of).reshape((-1,) + (1,) * (len(dims) - dim - 1))

    factor_of = one(*shards[0])
    for cut in shards[1:]:
        factor_of = factor_of * one(*cut)
    return factor_of


def gaussian(key, dims, width, bound, pieces=(), held_as=jnp.bfloat16):
    loudness = block_scale(key, dims, pieces, -0.22, 0.18) if pieces else 1.0
    values = jax.random.normal(key, dims, jnp.float32) * width * loudness
    return jnp.minimum(jnp.maximum(values, -bound), bound).astype(held_as)


def heavy_noise(own_key, extent, deviation, limit, split, heavy, held_as=jnp.bfloat16):
    drawn = deviation * jax.random.normal(own_key, extent, jnp.float32)
    if split:
        drawn = drawn * block_scale(own_key, extent, split, -0.22, 0.18)
    return jnp.clip(strengthened(drawn, jax.random.fold_in(own_key, 3), *heavy), -limit, limit).astype(held_as)


def setup_inputs(seed: int = 0) -> dict:
    key_of = jax.random.split(jax.random.key(seed), 8)
    return {
        "tokens": draw_tokens(jax.random.fold_in(key_of[7], 71), 0),
        "up_weight": heavy_noise(key_of[1], (LAYERS, D, FF), D ** -0.5, 0.1875, ((1, 32), (2, 16)), (1, 2, 32, 2.75), jnp.float32),
        "up_scale": jnp.clip(jnp.exp(math.log(2.0) - 1.3862944 * jax.random.uniform(key_of[2], (LAYERS, FF), jnp.float32) ** block_scale(key_of[2], (LAYERS, FF), ((1, 16),), -0.2, 0.2)), 0.5, 2.0),
        "down_weight": gaussian(key_of[3], (LAYERS, FF, D), FF ** -0.5, 0.046875, ((1, 16), (2, 32)), jnp.float32),
        "down_scale": draw_down_scale(jax.random.fold_in(key_of[7], 71), 0),
        "pre_gain": jnp.clip(1.0 + 0.18 * jax.random.normal(key_of[5], (LAYERS, D), jnp.float32), 0.1, 1.9),
        "post_gain": jnp.clip(1.0 + 0.18 * jax.random.normal(key_of[6], (LAYERS, D), jnp.float32), 0.1, 1.9),
    }


norm_eps = 1e-06
residual_keep = 0.5

def reference(tokens, up_weight, up_scale, down_weight, down_scale, pre_gain, post_gain):
    stream = tokens
    for sublayer in range(LAYERS):
        values = stream.astype(jnp.float32)
        scaled = (values * pre_gain[sublayer][None, :]).astype(jnp.bfloat16)
        whole_up = jnp.dot(scaled, up_weight[sublayer].astype(jnp.bfloat16), preferred_element_type=jnp.float32)
        whole_up = whole_up * up_scale[sublayer][None, :]
        hidden = jnp.square(jax.nn.relu(whole_up)).astype(jnp.bfloat16)
        block_hidden = hidden.reshape(TOKENS, N_CB, FF // N_CB).astype(jnp.float32)
        block_down = down_weight[sublayer].astype(jnp.bfloat16).reshape(N_CB, FF // N_CB, D).astype(jnp.float32)
        partials = jnp.einsum('mbf,bfd->bmd', block_hidden, block_down).astype(jnp.bfloat16)
        partials = lax.optimization_barrier(partials).astype(jnp.float32)
        branch_in = lax.optimization_barrier(jnp.sum(partials, axis=0)) * down_scale[sublayer][None, :]
        inv_post = lax.rsqrt(lax.optimization_barrier(jnp.mean(branch_in * branch_in, axis=1, keepdims=True)) + norm_eps)
        branch = branch_in * inv_post * post_gain[sublayer][None, :]
        stream = (residual_keep * values + branch).astype(jnp.bfloat16)
    return stream
```

```python
import jax
import jax.numpy as jnp
from jax import lax
from jax.sharding import Mesh, PartitionSpec as P


norm_eps = 1e-06
residual_keep = 0.5
Z, X, Y, C = 8, 4, 8, 2
bf16 = jnp.bfloat16
f32 = jnp.float32


def exchange(pieces, axis):
    return lax.all_to_all(pieces, axis, split_axis=0, concat_axis=0, tiled=True)


def to_all(shard, axis):
    size = lax.axis_size(axis)
    return exchange(jnp.broadcast_to(shard[None], (size, *shard.shape)), axis)


def high_low(v):
    high = lax.reduce_precision(v, 8, 7)
    return high.astype(bf16), (v - high).astype(bf16)


def other_core(v):
    return lax.ppermute(v, "core", [(0, 1), (1, 0)])


def half(v, which, axis, size):
    return lax.dynamic_slice_in_dim(v, which * size, size, axis)


def hidden_of(part):
    tokens, width = part.shape
    share = width // Z
    pieces = part.astype(bf16).reshape(tokens, Z, share).transpose(1, 0, 2)
    summed = exchange(pieces, "z").astype(f32).sum(axis=0)
    chunk = jnp.square(jnp.maximum(summed, 0.0)).astype(bf16)
    whole = to_all(chunk, "z")
    return whole.transpose(1, 0, 2).reshape(tokens, width)


def down_sum(hidden, weight):
    core = lax.axis_index("core")
    part = jnp.stack(
        [jnp.dot(hidden, weight[i], preferred_element_type=f32) for i in range(X)]
    )
    t = hidden.shape[0] // C
    got = other_core(half(part.astype(bf16), 1 - core, 1, t))
    mine = half(part, core, 1, t) + got.astype(f32)
    return to_all(mine.astype(bf16), "y").astype(f32).sum(axis=0)


def inv_norm(branch_in, width):
    squares = jnp.sum(branch_in * branch_in, axis=(0, 2))
    squares = to_all(squares[None], "z").sum(axis=0)[0]
    return lax.rsqrt(squares / width + norm_eps)[None, :, None]


def inner(tokens, up_weight, up_scale, down_weight, down_scale, pre_gain, post_gain):
    n_tok, feats = tokens.shape
    hid = up_weight.shape[2]
    width = feats * X * Z
    t_x = n_tok // X
    t_c = t_x // C
    core = lax.axis_index("core")

    scaled = (tokens.astype(f32) * pre_gain[0][None, :]).astype(bf16)
    part = jnp.dot(scaled, up_weight[0].astype(bf16), preferred_element_type=f32)
    part = (part * up_scale[0][None, :]).astype(bf16)
    body = jnp.concatenate([part, tokens], axis=1).reshape(X, t_x, hid + feats)
    vectors = [down_scale[0], post_gain[0], pre_gain[1], down_scale[1], post_gain[1]]
    highs, lows = zip(*[high_low(v) for v in vectors])
    spare = jnp.zeros((hid + feats - feats * len(vectors),), bf16)
    rows = jnp.stack([jnp.concatenate([*highs, spare]), jnp.concatenate([*lows, spare])])
    rows = jnp.concatenate([rows, jnp.zeros((6, hid + feats), bf16)])
    sent = jnp.concatenate([body, jnp.broadcast_to(rows[None], (X, *rows.shape))], axis=1)
    came = exchange(sent, "x")
    part = came[:, :t_x, :hid].astype(f32).sum(axis=0)

    def from_here(v):
        return lax.dynamic_slice_in_dim(jnp.concatenate([v, v]), lax.axis_index("x"), X, 0)

    def from_zero(v):
        back = (X - lax.axis_index("x")) % X
        return lax.dynamic_slice_in_dim(jnp.concatenate([v, v]), back, X, 0)

    own_tokens = from_here(half(came[:, :t_x, hid:], core, 1, t_c)).astype(f32)
    vec = came[:, t_x].astype(f32) + came[:, t_x + 1].astype(f32)
    vec = from_here(vec[:, : feats * len(vectors)].reshape(X, len(vectors), feats))
    down_0, post_0, pre_1, down_1, post_1 = [vec[:, k][:, None, :] for k in range(len(vectors))]

    def gathered(w, after):
        w, _ = lax.optimization_barrier((w.astype(bf16), after))
        blocks = [w]
        for s in (1, 2, 3):
            blocks.append(lax.ppermute(w, "x", [(i, (i - s) % X) for i in range(X)]))
        return blocks

    down_w0 = gathered(down_weight[0], came)
    hidden = hidden_of(part)
    up_w1 = gathered(up_weight[1], came)
    summed = down_sum(hidden, down_w0)
    branch_in = summed * down_0
    branch = branch_in * inv_norm(branch_in, width) * post_0
    stream = (residual_keep * own_tokens + branch).astype(bf16)

    values = stream.astype(f32)
    scaled = (values * pre_1).astype(bf16)
    got = other_core(scaled)
    first = jnp.where(core == 0, scaled, got)
    second = jnp.where(core == 0, got, scaled)
    scaled = jnp.concatenate([first, second], axis=1).transpose(1, 0, 2).reshape(t_x, X * feats)
    part = jnp.dot(scaled, jnp.concatenate(up_w1), preferred_element_type=f32)
    part = part * up_scale[1][None, :]
    down_w1 = gathered(down_weight[1], came)
    hidden = hidden_of(part)
    summed = down_sum(hidden, down_w1)
    branch_in = summed * down_1
    branch = branch_in * inv_norm(branch_in, width) * post_1
    out = (residual_keep * values + branch).astype(bf16)
    out = from_zero(out)
    out = jnp.broadcast_to(out[:, None], (X, C, t_c, feats)).reshape(X * C, t_c, feats)
    return exchange(out, ("x", "core")).reshape(n_tok, feats)


def solution(mesh):
    split = Mesh(mesh.devices.reshape(Z, X, Y, C), ("z", "x", "y", "core"))
    ra, cb = ("z", "x"), ("y", "core")
    return jax.shard_map(
        inner,
        mesh=split,
        in_specs=(
            P(None, ra),
            P(None, ra, cb),
            P(None, cb),
            P(None, cb, ra),
            P(None, ra),
            P(None, ra),
            P(None, ra),
        ),
        out_specs=P(None, ra),
        check_vma=False,
    )
```

```python
import jax
import jax.numpy as jnp
from jax import lax
from jax.sharding import Mesh, PartitionSpec as P


norm_eps = 1e-06
residual_keep = 0.5
Z, X, Y, C = 8, 4, 8, 2
bf16 = jnp.bfloat16
f32 = jnp.float32


def exchange(pieces, axis):
    return lax.all_to_all(pieces, axis, split_axis=0, concat_axis=0, tiled=True)


def to_all(shard, axis):
    size = lax.axis_size(axis)
    return exchange(jnp.broadcast_to(shard[None], (size, *shard.shape)), axis)


def high_low(v):
    high = lax.reduce_precision(v, 8, 7)
    return high.astype(bf16), (v - high).astype(bf16)


def other_core(v):
    return lax.ppermute(v, "core", [(0, 1), (1, 0)])


def half(v, which, axis, size):
    return lax.dynamic_slice_in_dim(v, which * size, size, axis)


def hidden_of(part):
    summed = exchange(part.astype(bf16), "z").astype(f32).sum(axis=0)
    chunk = jnp.square(jnp.maximum(summed, 0.0)).astype(bf16)
    whole = to_all(chunk, "z")
    return whole.transpose(1, 0, 2).reshape(whole.shape[1], -1)


def down_sum(hidden, weight):
    core = lax.axis_index("core")
    part = jnp.stack(
        [jnp.dot(hidden, weight[i], preferred_element_type=f32) for i in range(X)]
    )
    t = hidden.shape[0] // C
    got = other_core(half(part.astype(bf16), 1 - core, 1, t))
    mine = half(part, core, 1, t) + got.astype(f32)
    return to_all(mine.astype(bf16), "y").astype(f32).sum(axis=0)


def inv_norm(branch_in, width):
    squares = jnp.sum(branch_in * branch_in, axis=(0, 2))
    squares = to_all(squares[None], "z").sum(axis=0)[0]
    return lax.rsqrt(squares / width + norm_eps)[None, :, None]


def inner(tokens, up_weight, up_scale, down_weight, down_scale, pre_gain, post_gain):
    n_tok, feats = tokens.shape
    hid = up_weight.shape[2]
    width = feats * X * Z
    t_x = n_tok // X
    t_c = t_x // C
    x, core = lax.axis_index("x"), lax.axis_index("core")

    scaled = (tokens.astype(f32) * pre_gain[0][None, :]).astype(bf16)
    part = jnp.dot(scaled, up_weight[0].astype(bf16), preferred_element_type=f32)
    part = (part * up_scale[0][None, :]).astype(bf16).reshape(X, t_x, hid)
    part = exchange(part, "x").astype(f32).sum(axis=0)

    def from_x(send):
        blocks = []
        for s in (1, 2, 3):
            pairs = [(i, (i - s) % X) for i in range(X)]
            blocks.append(lax.ppermute(send(s), "x", pairs))
        return blocks

    vectors = [down_scale[0], post_gain[0], pre_gain[1], down_scale[1], post_gain[1]]
    highs, lows = high_low(jnp.stack(vectors))
    nothing = jnp.zeros((3, feats), bf16)
    columns = jnp.concatenate([highs, nothing, lows, nothing])
    down_w0 = down_weight[0].astype(bf16)

    def tokens_of(s):
        return lax.dynamic_slice_in_dim(tokens, (x - s) % X * t_x, t_x, 0)

    came = from_x(lambda s: jnp.concatenate([down_w0, columns, tokens_of(s)]))
    down_w0 = [down_w0, *(b[:hid] for b in came)]
    columns = jnp.stack([columns, *(b[hid : hid + 16] for b in came)]).astype(f32)
    columns = columns[:, :8] + columns[:, 8:]
    down_0, post_0, pre_1, down_1, post_1 = [columns[:, k : k + 1] for k in range(5)]
    own_tokens = jnp.stack([tokens_of(0), *(b[hid + 16 :] for b in came)])
    own_tokens = half(own_tokens, core, 1, t_c).astype(f32)

    up_w1 = up_weight[1].astype(bf16).reshape(feats, Z, hid // Z).transpose(1, 0, 2)
    down_w1 = down_weight[1].astype(bf16)
    both = jnp.concatenate([up_w1.reshape(hid, feats), down_w1])
    came = from_x(lambda s: both)
    up_w1 = jnp.concatenate([up_w1, *(b[:hid].reshape(up_w1.shape) for b in came)], axis=1)
    down_w1 = [down_w1, *(b[hid:] for b in came)]

    hidden = hidden_of(part.reshape(t_x, Z, hid // Z).transpose(1, 0, 2))
    summed = down_sum(hidden, down_w0)
    branch_in = summed * down_0
    branch = branch_in * inv_norm(branch_in, width) * post_0
    stream = (residual_keep * own_tokens + branch).astype(bf16)

    values = stream.astype(f32)
    scaled = (values * pre_1).astype(bf16)
    got = other_core(scaled)
    first = jnp.where(core == 0, scaled, got)
    second = jnp.where(core == 0, got, scaled)
    scaled = jnp.concatenate([first, second], axis=1).transpose(1, 0, 2).reshape(t_x, X * feats)
    part = jnp.stack(
        [jnp.dot(scaled, up_w1[c], preferred_element_type=f32) for c in range(Z)]
    )
    hidden = hidden_of(part * up_scale[1].reshape(Z, 1, hid // Z))
    summed = down_sum(hidden, down_w1)
    branch_in = summed * down_1
    branch = branch_in * inv_norm(branch_in, width) * post_1
    out = (residual_keep * values + branch).astype(bf16)
    out = lax.dynamic_slice_in_dim(jnp.concatenate([out, out]), (X - x) % X, X, 0)
    out = jnp.broadcast_to(out[:, None], (X, C, t_c, feats)).reshape(X * C, t_c, feats)
    return exchange(out, ("x", "core")).reshape(n_tok, feats)


def solution(mesh):
    split = Mesh(mesh.devices.reshape(Z, X, Y, C), ("z", "x", "y", "core"))
    ra, cb = ("z", "x"), ("y", "core")
    return jax.shard_map(
        inner,
        mesh=split,
        in_specs=(
            P(None, ra),
            P(None, ra, cb),
            P(None, cb),
            P(None, cb, ra),
            P(None, ra),
            P(None, ra),
            P(None, ra),
        ),
        out_specs=P(None, ra),
        check_vma=False,
    )
```

```python
import jax
import jax.numpy as jnp
from jax import lax
from jax.sharding import Mesh, PartitionSpec as P


norm_eps = 1e-06
residual_keep = 0.5
Z, X, Y, C = 8, 4, 8, 2
bf16 = jnp.bfloat16
f32 = jnp.float32


def exchange(pieces, axis):
    return lax.all_to_all(pieces, axis, split_axis=0, concat_axis=0, tiled=True)


def to_all(shard, axis):
    size = lax.axis_size(axis)
    return exchange(jnp.broadcast_to(shard[None], (size, *shard.shape)), axis)


def high_low(v):
    high = lax.reduce_precision(v, 8, 7)
    return high.astype(bf16), (v - high).astype(bf16)


def shared(chunk):
    whole = to_all(chunk, "z")
    return whole.transpose(1, 0, 2).reshape(whole.shape[1], -1)


def activation(up):
    return jnp.square(jnp.maximum(up, 0.0)).astype(bf16)


def down_share(hidden, weight):
    part = jnp.stack(
        [jnp.dot(hidden, weight[i], preferred_element_type=f32) for i in range(X)]
    ).astype(bf16)
    pieces = part.reshape(Y * C, -1, part.shape[2])
    return exchange(pieces, ("y", "core")).astype(f32).sum(axis=0).astype(bf16)


def down_whole(mine):
    return to_all(mine, ("y", "core")).reshape(X, -1, mine.shape[1])


def after(blocks, value):
    return [lax.optimization_barrier((b, value))[0] for b in blocks]


def inner(tokens, up_weight, up_scale, down_weight, down_scale, pre_gain, post_gain):
    n_tok, feats = tokens.shape
    hid = up_weight.shape[2]
    width = feats * X * Z
    t_x = n_tok // X
    x = lax.axis_index("x")

    scaled = (tokens.astype(f32) * pre_gain[0][None, :]).astype(bf16)
    part = jnp.dot(scaled, up_weight[0].astype(bf16), preferred_element_type=f32)
    part = (part * up_scale[0][None, :]).astype(bf16).reshape(X, t_x, hid)
    part = exchange(part, "x").astype(f32).sum(axis=0)

    def from_x(send):
        blocks = []
        for s in (1, 2, 3):
            pairs = [(i, (i - s) % X) for i in range(X)]
            blocks.append(lax.ppermute(send(s), "x", pairs))
        return blocks

    vectors = [down_scale[0], post_gain[0], pre_gain[1], down_scale[1], post_gain[1]]
    highs, lows = high_low(jnp.stack(vectors))
    nothing = jnp.zeros((3, feats), bf16)
    columns = jnp.concatenate([highs, nothing, lows, nothing])
    down_w0 = down_weight[0].astype(bf16)

    def tokens_of(s):
        return lax.dynamic_slice_in_dim(tokens, (x - s) % X * t_x, t_x, 0)

    first = from_x(lambda s: jnp.concatenate([down_w0, columns, tokens_of(s)]))

    up_w1 = up_weight[1].astype(bf16).reshape(feats, Z, hid // Z).transpose(1, 0, 2)
    down_w1 = down_weight[1].astype(bf16)
    both = jnp.concatenate([up_w1.reshape(hid, feats), down_w1])
    second = from_x(lambda s: both)

    pieces = part.astype(bf16).reshape(t_x, Z, hid // Z).transpose(1, 0, 2)
    summed = exchange(pieces, "z").astype(f32).sum(axis=0)
    hidden = shared(activation(summed))
    came = after(first, hidden)
    down_w0 = [down_w0, *(b[:hid] for b in came)]
    columns = jnp.stack([columns, *(b[hid : hid + 16] for b in came)]).astype(f32)
    columns = columns[:, :8] + columns[:, 8:]
    down_0, post_0, pre_1, down_1, post_1 = [columns[:, k : k + 1] for k in range(5)]
    own_tokens = jnp.stack([tokens_of(0), *(b[hid + 16 :] for b in came)])
    own_tokens = own_tokens.astype(f32)
    mine = down_share(hidden, down_w0)
    came = after(second, mine)
    up_w1 = jnp.concatenate([up_w1, *(b[:hid].reshape(up_w1.shape) for b in came)], axis=1)
    down_w1 = [down_w1, *(b[hid:] for b in came)]
    branch_in = down_whole(mine).astype(f32) * down_0

    kept = residual_keep * own_tokens
    squares = jnp.sum(branch_in * branch_in, axis=(0, 2))
    terms = jnp.concatenate([kept * pre_1, branch_in * (post_0 * pre_1)], axis=1).astype(bf16)
    terms = terms.transpose(1, 0, 2).reshape(2 * t_x, X * feats)
    part = jnp.stack(
        [jnp.dot(terms, up_w1[c], preferred_element_type=f32) for c in range(Z)]
    )
    part = (part * up_scale[1].reshape(Z, 1, hid // Z)).astype(bf16)
    rows = jnp.stack(high_low(jnp.pad(squares, (0, feats - t_x))))
    rows = jnp.broadcast_to(jnp.pad(rows, ((0, 6), (0, 0)))[None], (Z, 8, feats))
    came = exchange(jnp.concatenate([part, rows], axis=1), "z").astype(f32)
    summed = came[:, : 2 * t_x].sum(axis=0)
    squares = came[:, 2 * t_x : 2 * t_x + 2].sum(axis=(0, 1))[:t_x]
    inv = lax.rsqrt(squares / width + norm_eps)[:, None]
    hidden = shared(activation(summed[:t_x] + summed[t_x:] * inv))
    stream = (kept + branch_in * inv[None] * post_0).astype(bf16)

    branch_in = down_whole(down_share(hidden, down_w1)).astype(f32) * down_1
    squares = jnp.sum(branch_in * branch_in, axis=(0, 2))
    squares = to_all(squares[None], "z").sum(axis=0)[0]
    inv = lax.rsqrt(squares / width + norm_eps)[None, :, None]
    out = (residual_keep * stream.astype(f32) + branch_in * inv * post_1).astype(bf16)
    out = lax.dynamic_slice_in_dim(jnp.concatenate([out, out]), (X - x) % X, X, 0)
    return exchange(out, "x").reshape(n_tok, feats)


def solution(mesh):
    split = Mesh(mesh.devices.reshape(Z, X, Y, C), ("z", "x", "y", "core"))
    ra, cb = ("z", "x"), ("y", "core")
    return jax.shard_map(
        inner,
        mesh=split,
        in_specs=(
            P(None, ra),
            P(None, ra, cb),
            P(None, cb),
            P(None, cb, ra),
            P(None, ra),
            P(None, ra),
            P(None, ra),
        ),
        out_specs=P(None, ra),
        check_vma=False,
    )
```

```python
import jax
import jax.numpy as jnp
from jax import lax
from jax.experimental import pallas as pl
from jax.experimental.pallas import tpu as pltpu
from jax.sharding import Mesh, PartitionSpec as P


norm_eps = 1e-06
residual_keep = 0.5
Z, X, Y, C = 8, 4, 8, 2
bf16 = jnp.bfloat16
f32 = jnp.float32


def exchange(pieces, axis):
    return lax.all_to_all(pieces, axis, split_axis=0, concat_axis=0, tiled=True)


def to_all(shard, axis):
    size = lax.axis_size(axis)
    return exchange(jnp.broadcast_to(shard[None], (size, *shard.shape)), axis)


def high_low(v):
    high = lax.reduce_precision(v, 8, 7)
    return high.astype(bf16), (v - high).astype(bf16)


def activation(up):
    return jnp.square(jnp.maximum(up, 0.0)).astype(bf16)


def near(v):
    return pltpu.with_memory_space_constraint(v, pltpu.VMEM)


def down_kernel(row, hidden_ref, *refs):
    weights, out_ref, held, sems = refs[:X], refs[X], refs[X + 1], refs[X + 2]
    copies = []
    for i, w in enumerate(weights):
        rows = w.at[pl.ds(row if w.shape[0] > held.shape[1] else 0, held.shape[1])]
        copies.append(pltpu.make_async_copy(rows, held.at[i], sems.at[i]))
        copies[-1].start()
    hidden = jnp.concatenate([hidden_ref[z] for z in range(Z)], axis=1)
    for i in range(X):
        copies[i].wait()
        out_ref[i] = jnp.dot(hidden, held[i], preferred_element_type=f32).astype(bf16)


def down_product(hidden, blocks, row):
    _, t, share = hidden.shape
    feats = blocks[0].shape[1]
    return pl.pallas_call(
        lambda *refs: down_kernel(row, *refs),
        out_shape=pltpu.VMEM((X, t, feats), bf16),
        in_specs=[
            pl.BlockSpec(memory_space=pltpu.VMEM),
            *[pl.BlockSpec(memory_space=pl.ANY)] * X,
        ],
        out_specs=pl.BlockSpec(memory_space=pltpu.VMEM),
        scratch_shapes=[
            pltpu.VMEM((X, Z * share, feats), bf16),
            pltpu.SemaphoreType.DMA((X,)),
        ],
        compiler_params=pltpu.CompilerParams(vmem_limit_bytes=8 << 20),
        name="down_product",
    )(near(hidden), *blocks)


def down_sum(hidden, blocks, row):
    part = down_product(hidden, blocks, row)
    pieces = part.reshape(Y * C, -1, part.shape[2])
    mine = exchange(pieces, ("y", "core")).astype(f32).sum(axis=0).astype(bf16)
    return to_all(mine, ("y", "core")).reshape(part.shape)


def turn_kernel(at, sum_ref, extra_ref, scale_ref, *refs):
    firsts, seconds = refs[: X - 1], refs[X - 1 : 2 * X - 1]
    out_ref, kept_ref, branch_ref, columns_ref = refs[2 * X - 1 : 2 * X + 3]
    extra, held, sems, held_sems = refs[2 * X + 3 :]
    t, feats = sum_ref.shape[1:]
    copies = []
    for i, block in enumerate(firsts):
        rows = block.at[pl.ds(at, extra.shape[1])]
        copies.append(pltpu.make_async_copy(rows, extra.at[i], sems.at[i]))
        copies[-1].start()
    held_copies = []
    for i, block in enumerate(seconds):
        here = held.at[:, pl.ds(i * feats, feats)]
        held_copies.append(pltpu.make_async_copy(block.at[pl.ds(0, Z)], here, held_sems.at[i]))
        held_copies[-1].start()
    for copy in copies:
        copy.wait()
    kept_terms, branch_terms, squares = [], [], jnp.zeros((8, t), f32)
    for i in range(X):
        block = extra_ref[...] if i == 0 else extra[i - 1]
        columns = block[:8].astype(f32) + block[8:16].astype(f32)
        columns_ref[i] = columns
        down_0, post_0, pre_1 = [columns[k : k + 1] for k in range(3)]
        kept = residual_keep * block[16:].astype(f32)
        branch_in = sum_ref[i].astype(f32) * down_0
        branch = branch_in * post_0
        kept_ref[i] = kept
        branch_ref[i] = branch
        kept_terms.append((kept * pre_1).astype(bf16))
        branch_terms.append((branch * pre_1).astype(bf16))
        squares += lax.dot_general(
            jnp.ones((8, feats), f32),
            branch_in * branch_in,
            (((1,), (1,)), ((), ())),
            precision=lax.Precision.HIGHEST,
            preferred_element_type=f32,
        )
    high = squares.astype(bf16).astype(f32)
    row = lax.broadcasted_iota(jnp.int32, squares.shape, 0)
    squares = jnp.where(row == 0, high, jnp.where(row == 1, squares - high, 0.0)).astype(bf16)
    terms = jnp.concatenate(
        [jnp.concatenate(kept_terms, axis=1), jnp.concatenate(branch_terms, axis=1)], axis=0
    )
    for copy in held_copies:
        copy.wait()
    for c in range(Z):
        part = jnp.dot(terms, held[c], preferred_element_type=f32)
        out_ref[c, : 2 * t] = (part * scale_ref[c]).astype(bf16)
        out_ref[c, 2 * t :] = jnp.zeros((8, feats), bf16)
        out_ref[c, 2 * t :, :t] = squares


def turn(summed, extra, scale, firsts, seconds, at):
    _, t, feats = summed.shape
    return pl.pallas_call(
        lambda *refs: turn_kernel(at, *refs),
        out_shape=(
            pltpu.VMEM((Z, 2 * t + 8, feats), bf16),
            pltpu.VMEM((X, t, feats), f32),
            pltpu.VMEM((X, t, feats), f32),
            pltpu.VMEM((X, 8, feats), f32),
        ),
        in_specs=[
            *[pl.BlockSpec(memory_space=pltpu.VMEM)] * 3,
            *[pl.BlockSpec(memory_space=pl.ANY)] * (2 * X - 1),
        ],
        out_specs=(pl.BlockSpec(memory_space=pltpu.VMEM),) * 4,
        scratch_shapes=[
            pltpu.VMEM((X - 1, 16 + t, feats), bf16),
            pltpu.VMEM((Z, X * feats, feats), bf16),
            pltpu.SemaphoreType.DMA((X - 1,)),
            pltpu.SemaphoreType.DMA((X,)),
        ],
        compiler_params=pltpu.CompilerParams(vmem_limit_bytes=12 << 20),
        name="turn",
    )(near(summed), near(extra), near(scale), *firsts, *seconds)


def inner(tokens, up_weight, up_scale, down_weight, down_scale, pre_gain, post_gain):
    n_tok, feats = tokens.shape
    hid = up_weight.shape[2]
    width = feats * X * Z
    t_x = n_tok // X
    x = lax.axis_index("x")

    scaled = (tokens.astype(f32) * pre_gain[0][None, :]).astype(bf16)
    part = jnp.dot(scaled, up_weight[0].astype(bf16), preferred_element_type=f32)
    part = (part * up_scale[0][None, :]).astype(bf16).reshape(X, t_x, hid)
    part = exchange(part, "x").astype(f32).sum(axis=0)

    def from_x(send):
        blocks = []
        for s in (1, 2, 3):
            pairs = [(i, (i - s) % X) for i in range(X)]
            blocks.append(lax.ppermute(send(s), "x", pairs))
        return blocks

    vectors = [down_scale[0], post_gain[0], pre_gain[1], down_scale[1], post_gain[1]]
    highs, lows = high_low(jnp.stack(vectors))
    nothing = jnp.zeros((3, feats), bf16)
    columns = jnp.concatenate([highs, nothing, lows, nothing])
    down_w0 = down_weight[0].astype(bf16)

    def tokens_of(s):
        return lax.dynamic_slice_in_dim(tokens, (x - s) % X * t_x, t_x, 0)

    first = from_x(lambda s: jnp.concatenate([down_w0, columns, tokens_of(s)]))

    up_w1 = up_weight[1].astype(bf16).reshape(feats, Z, hid // Z).transpose(1, 0, 2)
    down_w1 = down_weight[1].astype(bf16)
    both = jnp.concatenate([up_w1.reshape(hid, feats), down_w1])
    second = [both, *from_x(lambda s: both)]

    pieces = part.astype(bf16).reshape(t_x, Z, hid // Z).transpose(1, 0, 2)
    summed = exchange(pieces, "z").astype(f32).sum(axis=0)
    hidden = to_all(activation(summed), "z")
    summed = down_sum(hidden, [down_w0, *first], 0)

    extra = jnp.concatenate([columns, tokens_of(0)])
    scale = up_scale[1].reshape(Z, 1, hid // Z)
    blocks = [b.reshape(2 * Z, feats, hid // Z) for b in second]
    part, kept, branch, columns = turn(summed, extra, scale, first, blocks, hid)
    came = exchange(part, "z").astype(f32)
    summed = came[:, : 2 * t_x].sum(axis=0)
    squares = came[:, 2 * t_x : 2 * t_x + 2].sum(axis=(0, 1))[:t_x]
    inv = lax.rsqrt(squares / width + norm_eps)[:, None]
    hidden = to_all(activation(summed[:t_x] + summed[t_x:] * inv), "z")
    stream = (kept + branch * inv[None]).astype(bf16)
    down_1, post_1 = columns[:, 3:4], columns[:, 4:5]

    branch_in = down_sum(hidden, second, hid).astype(f32) * down_1
    squares = jnp.sum(branch_in * branch_in, axis=(0, 2))
    squares = to_all(squares[None], "z").sum(axis=0)[0]
    inv = lax.rsqrt(squares / width + norm_eps)[None, :, None]
    out = (residual_keep * stream.astype(f32) + branch_in * inv * post_1).astype(bf16)
    out = lax.dynamic_slice_in_dim(jnp.concatenate([out, out]), (X - x) % X, X, 0)
    return exchange(out, "x").reshape(n_tok, feats)


def solution(mesh):
    split = Mesh(mesh.devices.reshape(Z, X, Y, C), ("z", "x", "y", "core"))
    ra, cb = ("z", "x"), ("y", "core")
    return jax.shard_map(
        inner,
        mesh=split,
        in_specs=(
            P(None, ra),
            P(None, ra, cb),
            P(None, cb),
            P(None, cb, ra),
            P(None, ra),
            P(None, ra),
            P(None, ra),
        ),
        out_specs=P(None, ra),
        check_vma=False,
    )
```

```python
import jax
import jax.numpy as jnp
from jax import lax
from jax.experimental import pallas as pl
from jax.experimental.pallas import tpu as pltpu
from jax.sharding import Mesh, PartitionSpec as P


norm_eps = 1e-06
residual_keep = 0.5
Z, X, Y, C = 8, 4, 8, 2
bf16 = jnp.bfloat16
f32 = jnp.float32
VMEM = pl.BlockSpec(memory_space=pltpu.VMEM)
ANY = pl.BlockSpec(memory_space=pl.ANY)


def exchange(pieces, axis):
    return lax.all_to_all(pieces, axis, split_axis=0, concat_axis=0, tiled=True)


def to_all(shard, axis):
    size = lax.axis_size(axis)
    return exchange(jnp.broadcast_to(shard[None], (size, *shard.shape)), axis)


def activation(up):
    return jnp.square(jnp.maximum(up, 0.0)).astype(bf16)


def near(v):
    return pltpu.with_memory_space_constraint(v, pltpu.VMEM)


def far(v):
    return pltpu.with_memory_space_constraint(v, pltpu.HBM)


def after(blocks, value):
    return [lax.optimization_barrier((b, value))[0] for b in blocks]


def limit(mib):
    return pltpu.CompilerParams(vmem_limit_bytes=mib << 20)


def up_kernel(tokens_ref, gain_ref, weight_ref, scale_ref, out_ref):
    scaled = (tokens_ref[...].astype(f32) * gain_ref[0:1]).astype(bf16)
    part = jnp.dot(scaled, weight_ref[0].astype(bf16), preferred_element_type=f32)
    out_ref[...] = (part * scale_ref[0:1]).astype(bf16)


def up_product(tokens, gain, weight, scale):
    n_tok, feats = tokens.shape
    hid = weight.shape[2]
    step = hid // 4
    return pl.pallas_call(
        up_kernel,
        grid=(hid // step,),
        out_shape=jax.ShapeDtypeStruct((n_tok, hid), bf16),
        in_specs=[
            pl.BlockSpec((n_tok, feats), lambda i: (0, 0)),
            pl.BlockSpec(gain.shape, lambda i: (0, 0)),
            pl.BlockSpec((1, feats, step), lambda i: (0, 0, i)),
            pl.BlockSpec((scale.shape[0], step), lambda i: (0, i)),
        ],
        out_specs=pl.BlockSpec((n_tok, step), lambda i: (0, i)),
        compiler_params=limit(12),
        name="up_product",
    )(far(tokens), far(gain), far(weight), far(scale))


def pack_kernel(down_ref, up_ref, tokens_ref, scale_ref, pre_ref, post_ref, *outs):
    one, two, three, late, own = outs
    hid, feats = down_ref.shape[1:]
    t_x = own.shape[0] - 16
    x = lax.axis_index("x")
    scale, pre, post = scale_ref[...], pre_ref[...], post_ref[...]
    columns = [scale[0:1], post[0:1], pre[1:2], scale[1:2], post[1:2], jnp.zeros((3, feats), f32)]
    columns = jnp.concatenate(columns, axis=0)
    high = columns.astype(bf16).astype(f32)
    columns = jnp.concatenate([high, columns - high], axis=0).astype(bf16)
    for s, ref in ((0, own), (1, one), (2, two), (3, three)):
        at = 0 if s == 0 else hid
        if s:
            ref[:hid] = down_ref[0].astype(bf16)
        ref[at : at + 16] = columns
        rows = pl.multiple_of(lax.rem(x + (X - s), X) * t_x, 32)
        ref[at + 16 : at + 16 + t_x] = tokens_ref[pl.ds(rows, t_x)]
    for ref, at in ((one, hid + 16 + t_x), (three, hid + 16 + t_x), (late, 0)):
        for c in range(hid // feats):
            block = up_ref[0, :, c * feats : (c + 1) * feats].astype(bf16)
            ref[at + c * feats : at + (c + 1) * feats] = block
        ref[at + hid : at + 2 * hid] = down_ref[1].astype(bf16)


def packed(down_weight, up_weight, tokens, scale, pre, post):
    _, hid, feats = down_weight.shape
    t_x = tokens.shape[0] // X
    near_rows, far_rows = hid + 16 + t_x, 2 * hid
    whole = lambda v: pl.BlockSpec(v.shape, lambda i: (0,) * v.ndim)
    rows = (near_rows + far_rows, near_rows, near_rows + far_rows, far_rows, 16 + t_x)
    return pl.pallas_call(
        pack_kernel,
        grid=(1,),
        out_shape=tuple(jax.ShapeDtypeStruct((r, feats), bf16) for r in rows),
        in_specs=[
            whole(down_weight),
            pl.BlockSpec((1, feats, hid), lambda i: (1, 0, 0)),
            *[whole(v) for v in (tokens, scale, pre, post)],
        ],
        out_specs=tuple(pl.BlockSpec((r, feats), lambda i: (0, 0)) for r in rows),
        compiler_params=limit(20),
        name="packed",
    )(*[far(v) for v in (down_weight, up_weight, tokens, scale, pre, post)])


def down_kernel(starts, hidden_ref, *refs):
    weights, out_ref, held, sems = refs[:X], refs[X], refs[X + 1], refs[X + 2]
    copies = []
    for i, w in enumerate(weights):
        rows = w.at[pl.ds(starts[i], held.shape[1])]
        copies.append(pltpu.make_async_copy(rows, held.at[i], sems.at[i]))
        copies[-1].start()
    hidden = jnp.concatenate([hidden_ref[z] for z in range(Z)], axis=1)
    for i in range(X):
        copies[i].wait()
        out_ref[i] = jnp.dot(hidden, held[i], preferred_element_type=f32).astype(bf16)


def down_product(hidden, blocks, starts):
    _, t, share = hidden.shape
    feats = blocks[0].shape[1]
    return pl.pallas_call(
        lambda *refs: down_kernel(starts, *refs),
        out_shape=pltpu.VMEM((X, t, feats), bf16),
        in_specs=[VMEM, *[ANY] * X],
        out_specs=VMEM,
        scratch_shapes=[
            pltpu.VMEM((X, Z * share, feats), bf16),
            pltpu.SemaphoreType.DMA((X,)),
        ],
        compiler_params=limit(8),
        name="down_product",
    )(near(hidden), *blocks)


def down_sum(hidden, blocks, starts):
    part = down_product(hidden, blocks, starts)
    pieces = part.reshape(Y * C, -1, part.shape[2])
    mine = exchange(pieces, ("y", "core")).astype(f32).sum(axis=0).astype(bf16)
    return to_all(mine, ("y", "core")).reshape(part.shape)


def squares_in_rows(values):
    total = 0.0
    for v in values:
        total += lax.dot_general(
            jnp.ones((8, v.shape[1]), f32),
            v * v,
            (((1,), (1,)), ((), ())),
            precision=lax.Precision.HIGHEST,
            preferred_element_type=f32,
        )
    return total


def inverse(row, width, t):
    inv = lax.rsqrt(row * (1.0 / width) + norm_eps)
    return jnp.transpose(jnp.broadcast_to(inv, (128, 128)))[:t]


def turn_kernel(firsts_at, seconds_at, sum_ref, own_ref, scale_ref, *refs):
    firsts, seconds = refs[: X - 1], refs[X - 1 : 2 * X - 1]
    out_ref, kept_ref, branch_ref, columns_ref = refs[2 * X - 1 : 2 * X + 3]
    extra, held, sems, held_sems = refs[2 * X + 3 :]
    t, feats = sum_ref.shape[1:]
    copies = []
    for i, block in enumerate(firsts):
        rows = block.at[pl.ds(firsts_at[i], extra.shape[1])]
        copies.append(pltpu.make_async_copy(rows, extra.at[i], sems.at[i]))
        copies[-1].start()
    held_copies = []
    for i, block in enumerate(seconds):
        for c in range(Z):
            rows = block.at[pl.ds(seconds_at[i] + c * feats, feats)]
            here = held.at[c, pl.ds(i * feats, feats)]
            held_copies.append(pltpu.make_async_copy(rows, here, held_sems.at[i, c]))
            held_copies[-1].start()
    for copy in copies:
        copy.wait()
    kept_terms, branch_terms, branches = [], [], []
    for i in range(X):
        block = own_ref[...] if i == 0 else extra[i - 1]
        columns = block[:8].astype(f32) + block[8:16].astype(f32)
        columns_ref[i] = columns
        down_0, post_0, pre_1 = [columns[k : k + 1] for k in range(3)]
        kept = residual_keep * block[16:].astype(f32)
        branch_in = sum_ref[i].astype(f32) * down_0
        branch = branch_in * post_0
        kept_ref[i] = kept
        branch_ref[i] = branch
        kept_terms.append((kept * pre_1).astype(bf16))
        branch_terms.append((branch * pre_1).astype(bf16))
        branches.append(branch_in)
    squares = squares_in_rows(branches)
    high = squares.astype(bf16).astype(f32)
    row = lax.broadcasted_iota(jnp.int32, squares.shape, 0)
    squares = jnp.where(row == 0, high, jnp.where(row == 1, squares - high, 0.0)).astype(bf16)
    terms = jnp.concatenate(
        [jnp.concatenate(kept_terms, axis=1), jnp.concatenate(branch_terms, axis=1)], axis=0
    )
    for copy in held_copies:
        copy.wait()
    for c in range(Z):
        part = jnp.dot(terms, held[c], preferred_element_type=f32)
        scale = scale_ref[1:2, c * feats : (c + 1) * feats]
        out_ref[c, : 2 * t] = (part * scale).astype(bf16)
        out_ref[c, 2 * t :] = jnp.zeros((8, feats), bf16)
        out_ref[c, 2 * t :, :t] = squares


def turn(summed, own, scale, firsts, firsts_at, seconds, seconds_at):
    _, t, feats = summed.shape
    return pl.pallas_call(
        lambda *refs: turn_kernel(firsts_at, seconds_at, *refs),
        out_shape=(
            pltpu.VMEM((Z, 2 * t + 8, feats), bf16),
            pltpu.VMEM((X, t, feats), f32),
            pltpu.VMEM((X, t, feats), f32),
            pltpu.VMEM((X, 8, feats), f32),
        ),
        in_specs=[*[VMEM] * 3, *[ANY] * (2 * X - 1)],
        out_specs=(VMEM,) * 4,
        scratch_shapes=[
            pltpu.VMEM((X - 1, 16 + t, feats), bf16),
            pltpu.VMEM((Z, X * feats, feats), bf16),
            pltpu.SemaphoreType.DMA((X - 1,)),
            pltpu.SemaphoreType.DMA((X, Z)),
        ],
        compiler_params=limit(12),
        name="turn",
    )(near(summed), near(own), near(scale), *firsts, *seconds)


def hidden_kernel(width, came_ref, kept_ref, branch_ref, out_ref, stream_ref):
    t = out_ref.shape[1]
    total = came_ref[0].astype(f32)
    for z in range(1, Z):
        total += came_ref[z].astype(f32)
    inv = inverse(total[2 * t : 2 * t + 1] + total[2 * t + 1 : 2 * t + 2], width, t)
    hidden = activation(total[:t] + total[t : 2 * t] * inv)
    for z in range(Z):
        out_ref[z] = hidden
    for i in range(X):
        stream_ref[i] = (kept_ref[i] + branch_ref[i] * inv).astype(bf16)


def second_hidden(came, kept, branch, width):
    _, t, feats = kept.shape
    return pl.pallas_call(
        lambda *refs: hidden_kernel(width, *refs),
        out_shape=(pltpu.VMEM((Z, t, feats), bf16), pltpu.VMEM(kept.shape, bf16)),
        in_specs=[VMEM] * 3,
        out_specs=(VMEM,) * 2,
        compiler_params=limit(8),
        name="second_hidden",
    )(near(came), near(kept), near(branch))


def squares_kernel(sum_ref, columns_ref, out_ref):
    t = sum_ref.shape[1]
    values = [sum_ref[i].astype(f32) * columns_ref[i, 3:4] for i in range(X)]
    squares = squares_in_rows(values)
    for z in range(Z):
        out_ref[z] = jnp.zeros(out_ref.shape[1:], f32)
        out_ref[z, :, :t] = squares


def squares_of(summed, columns):
    return pl.pallas_call(
        squares_kernel,
        out_shape=pltpu.VMEM((Z, 8, summed.shape[2]), f32),
        in_specs=[VMEM] * 2,
        out_specs=VMEM,
        compiler_params=limit(8),
        name="squares",
    )(near(summed), near(columns))


def last_kernel(width, squares_ref, sum_ref, columns_ref, stream_ref, out_ref):
    t = sum_ref.shape[1]
    total = squares_ref[0]
    for z in range(1, Z):
        total += squares_ref[z]
    inv = inverse(total[0:1], width, t)
    x = lax.axis_index("x")
    for i in range(X):
        branch = sum_ref[i].astype(f32) * columns_ref[i, 3:4] * inv * columns_ref[i, 4:5]
        stream = residual_keep * stream_ref[i].astype(f32) + branch
        out_ref[lax.rem(x + i, X)] = stream.astype(bf16)


def last(squares, summed, columns, stream, width):
    return pl.pallas_call(
        lambda *refs: last_kernel(width, *refs),
        out_shape=pltpu.VMEM(summed.shape, bf16),
        in_specs=[VMEM] * 4,
        out_specs=VMEM,
        compiler_params=limit(8),
        name="last",
    )(near(squares), near(summed), near(columns), near(stream))


def inner(tokens, up_weight, up_scale, down_weight, down_scale, pre_gain, post_gain):
    n_tok, feats = tokens.shape
    hid = up_weight.shape[2]
    width = feats * X * Z
    t_x = n_tok // X

    part = up_product(tokens, pre_gain, up_weight, up_scale).reshape(X, t_x, hid)
    part = exchange(part, "x").astype(f32).sum(axis=0)

    def from_x(payload, s):
        return lax.ppermute(payload, "x", [(i, (i - s) % X) for i in range(X)])

    one, two, three, late, own = packed(
        down_weight, up_weight, tokens, down_scale, pre_gain, post_gain
    )
    firsts = [from_x(one, 1), from_x(two, 2), from_x(three, 3)]
    seconds = [late, firsts[0], from_x(late, 2), firsts[2]]
    near_rows = hid + 16 + t_x
    seconds_at = [0, near_rows, 0, near_rows]

    pieces = part.astype(bf16).reshape(t_x, Z, hid // Z).transpose(1, 0, 2)
    summed = exchange(pieces, "z").astype(f32).sum(axis=0)
    hidden = to_all(activation(summed), "z")
    summed = down_sum(hidden, [one, *after(firsts, hidden)], [0] * X)

    firsts, seconds = after(firsts, summed), after(seconds, summed)
    part, kept, branch, columns = turn(
        summed, own, up_scale, firsts, [hid] * (X - 1), seconds, seconds_at
    )
    came = exchange(part, "z")
    hidden, stream = second_hidden(came, kept, branch, width)
    hidden = exchange(hidden, "z")
    summed = down_sum(hidden, seconds, [at + hid for at in seconds_at])

    squares = squares_of(summed, columns)
    squares = exchange(squares, "z")
    out = last(squares, summed, columns, stream, width)
    return exchange(out, "x").reshape(n_tok, feats)


def solution(mesh):
    split = Mesh(mesh.devices.reshape(Z, X, Y, C), ("z", "x", "y", "core"))
    ra, cb = ("z", "x"), ("y", "core")
    return jax.shard_map(
        inner,
        mesh=split,
        in_specs=(
            P(None, ra),
            P(None, ra, cb),
            P(None, cb),
            P(None, cb, ra),
            P(None, ra),
            P(None, ra),
            P(None, ra),
        ),
        out_specs=P(None, ra),
        check_vma=False,
    )
```

```python
import jax
import jax.numpy as jnp
from jax import lax
from jax.experimental import pallas as pl
from jax.experimental.pallas import tpu as pltpu
from jax.sharding import Mesh, PartitionSpec as P


norm_eps = 1e-06
residual_keep = 0.5
Z, X, Y, C = 8, 4, 8, 2
bf16 = jnp.bfloat16
f32 = jnp.float32
VMEM = pl.BlockSpec(memory_space=pltpu.VMEM)
ANY = pl.BlockSpec(memory_space=pl.ANY)


def exchange(pieces, axis):
    return lax.all_to_all(pieces, axis, split_axis=0, concat_axis=0, tiled=True)


def to_all(shard, axis):
    size = lax.axis_size(axis)
    return exchange(jnp.broadcast_to(shard[None], (size, *shard.shape)), axis)


def activation(up):
    return jnp.square(jnp.maximum(up, 0.0)).astype(bf16)


def near(v):
    return pltpu.with_memory_space_constraint(v, pltpu.VMEM)


def far(v):
    return pltpu.with_memory_space_constraint(v, pltpu.HBM)


def after(blocks, value):
    return [lax.optimization_barrier((b, value))[0] for b in blocks]


def limit(mib):
    return pltpu.CompilerParams(vmem_limit_bytes=mib << 20)


def up_kernel(tokens_ref, gain_ref, weight_ref, scale_ref, out_ref, *scratch):
    tokens, gain, weight, scale, out, in_sems, weight_sems, out_sems = scratch
    parts, _, step = weight.shape
    small = [
        pltpu.make_async_copy(tokens_ref, tokens, in_sems.at[0]),
        pltpu.make_async_copy(gain_ref, gain, in_sems.at[1]),
        pltpu.make_async_copy(scale_ref, scale, in_sems.at[2]),
    ]
    for copy in small:
        copy.start()
    copies = []
    for i in range(parts):
        here = weight_ref.at[0, :, pl.ds(i * step, step)]
        copies.append(pltpu.make_async_copy(here, weight.at[i], weight_sems.at[i]))
        copies[-1].start()
    for copy in small:
        copy.wait()
    scaled = (tokens[...].astype(f32) * gain[0:1]).astype(bf16)
    sent = []
    for i in range(parts):
        copies[i].wait()
        part = jnp.dot(scaled, weight[i].astype(bf16), preferred_element_type=f32)
        out[i] = (part * scale[0:1, i * step : (i + 1) * step]).astype(bf16)
        there = out_ref.at[:, pl.ds(i * step, step)]
        sent.append(pltpu.make_async_copy(out.at[i], there, out_sems.at[i]))
        sent[-1].start()
    for copy in sent:
        copy.wait()


def up_product(tokens, gain, weight, scale):
    n_tok, feats = tokens.shape
    hid = weight.shape[2]
    parts = 4
    return pl.pallas_call(
        up_kernel,
        out_shape=jax.ShapeDtypeStruct((n_tok, hid), bf16),
        in_specs=[ANY] * 4,
        out_specs=ANY,
        scratch_shapes=[
            pltpu.VMEM(tokens.shape, bf16),
            pltpu.VMEM(gain.shape, f32),
            pltpu.VMEM((parts, feats, hid // parts), f32),
            pltpu.VMEM(scale.shape, f32),
            pltpu.VMEM((parts, n_tok, hid // parts), bf16),
            pltpu.SemaphoreType.DMA((3,)),
            pltpu.SemaphoreType.DMA((parts,)),
            pltpu.SemaphoreType.DMA((parts,)),
        ],
        compiler_params=limit(12),
        name="up_product",
    )(far(tokens), far(gain), far(weight), far(scale))


def pack_kernel(down_ref, up_ref, tokens_ref, scale_ref, pre_ref, post_ref, *outs):
    one, two, three, late, own = outs
    hid, feats = down_ref.shape[1:]
    t_x = own.shape[0] - 16
    x = lax.axis_index("x")
    scale, pre, post = scale_ref[...], pre_ref[...], post_ref[...]
    columns = [scale[0:1], post[0:1], pre[1:2], scale[1:2], post[1:2], jnp.zeros((3, feats), f32)]
    columns = jnp.concatenate(columns, axis=0)
    high = columns.astype(bf16).astype(f32)
    columns = jnp.concatenate([high, columns - high], axis=0).astype(bf16)
    for s, ref in ((0, own), (1, one), (2, two), (3, three)):
        at = 0 if s == 0 else hid
        if s:
            ref[:hid] = down_ref[0].astype(bf16)
        ref[at : at + 16] = columns
        rows = pl.multiple_of(lax.rem(x + (X - s), X) * t_x, 32)
        ref[at + 16 : at + 16 + t_x] = tokens_ref[pl.ds(rows, t_x)]
    for ref, at in ((one, hid + 16 + t_x), (three, hid + 16 + t_x), (late, 0)):
        for c in range(hid // feats):
            block = up_ref[0, :, c * feats : (c + 1) * feats].astype(bf16)
            ref[at + c * feats : at + (c + 1) * feats] = block
        ref[at + hid : at + 2 * hid] = down_ref[1].astype(bf16)


def packed(down_weight, up_weight, tokens, scale, pre, post):
    _, hid, feats = down_weight.shape
    t_x = tokens.shape[0] // X
    near_rows, far_rows = hid + 16 + t_x, 2 * hid
    whole = lambda v: pl.BlockSpec(v.shape, lambda i: (0,) * v.ndim)
    rows = (near_rows + far_rows, near_rows, near_rows + far_rows, far_rows, 16 + t_x)
    return pl.pallas_call(
        pack_kernel,
        grid=(1,),
        out_shape=tuple(jax.ShapeDtypeStruct((r, feats), bf16) for r in rows),
        in_specs=[
            whole(down_weight),
            pl.BlockSpec((1, feats, hid), lambda i: (1, 0, 0)),
            *[whole(v) for v in (tokens, scale, pre, post)],
        ],
        out_specs=tuple(pl.BlockSpec((r, feats), lambda i: (0, 0)) for r in rows),
        compiler_params=limit(20),
        name="packed",
    )(*[far(v) for v in (down_weight, up_weight, tokens, scale, pre, post)])


def down_kernel(starts, hidden_ref, *refs):
    weights, out_ref, held, sems = refs[:X], refs[X], refs[X + 1], refs[X + 2]
    copies = []
    for i, w in enumerate(weights):
        rows = w.at[pl.ds(starts[i], held.shape[1])]
        copies.append(pltpu.make_async_copy(rows, held.at[i], sems.at[i]))
        copies[-1].start()
    hidden = jnp.concatenate([hidden_ref[z] for z in range(Z)], axis=1)
    for i in range(X):
        copies[i].wait()
        out_ref[i] = jnp.dot(hidden, held[i], preferred_element_type=f32).astype(bf16)


def down_product(hidden, blocks, starts):
    _, t, share = hidden.shape
    feats = blocks[0].shape[1]
    return pl.pallas_call(
        lambda *refs: down_kernel(starts, *refs),
        out_shape=pltpu.VMEM((X, t, feats), bf16),
        in_specs=[VMEM, *[ANY] * X],
        out_specs=VMEM,
        scratch_shapes=[
            pltpu.VMEM((X, Z * share, feats), bf16),
            pltpu.SemaphoreType.DMA((X,)),
        ],
        compiler_params=limit(8),
        name="down_product",
    )(near(hidden), *blocks)


def down_share(hidden, blocks, starts):
    part = down_product(hidden, blocks, starts)
    pieces = part.reshape(Y * C, -1, part.shape[2])
    return exchange(pieces, ("y", "core")).astype(f32).sum(axis=0).astype(bf16)


def down_whole(mine):
    return to_all(mine, ("y", "core")).reshape(X, -1, mine.shape[1])


def squares_in_rows(values):
    total = 0.0
    for v in values:
        total += lax.dot_general(
            jnp.ones((8, v.shape[1]), f32),
            v * v,
            (((1,), (1,)), ((), ())),
            precision=lax.Precision.HIGHEST,
            preferred_element_type=f32,
        )
    return total


def inverse(row, width, t):
    inv = lax.rsqrt(row * (1.0 / width) + norm_eps)
    return jnp.transpose(jnp.broadcast_to(inv, (128, 128)))[:t]


def turn_kernel(firsts_at, seconds_at, sum_ref, own_ref, scale_ref, *refs):
    firsts, seconds = refs[: X - 1], refs[X - 1 : 2 * X - 1]
    out_ref, kept_ref, branch_ref, columns_ref = refs[2 * X - 1 : 2 * X + 3]
    extra, held, sems, held_sems = refs[2 * X + 3 :]
    t, feats = sum_ref.shape[1:]
    copies = []
    for i, block in enumerate(firsts):
        rows = block.at[pl.ds(firsts_at[i], extra.shape[1])]
        copies.append(pltpu.make_async_copy(rows, extra.at[i], sems.at[i]))
        copies[-1].start()
    held_copies = []
    for i, block in enumerate(seconds):
        for c in range(Z):
            rows = block.at[pl.ds(seconds_at[i] + c * feats, feats)]
            here = held.at[c, pl.ds(i * feats, feats)]
            held_copies.append(pltpu.make_async_copy(rows, here, held_sems.at[i, c]))
            held_copies[-1].start()
    for copy in copies:
        copy.wait()
    kept_terms, branch_terms, branches = [], [], []
    for i in range(X):
        block = own_ref[...] if i == 0 else extra[i - 1]
        columns = block[:8].astype(f32) + block[8:16].astype(f32)
        columns_ref[i] = columns
        down_0, post_0, pre_1 = [columns[k : k + 1] for k in range(3)]
        kept = residual_keep * block[16:].astype(f32)
        branch_in = sum_ref[i].astype(f32) * down_0
        branch = branch_in * post_0
        kept_ref[i] = kept
        branch_ref[i] = branch
        kept_terms.append((kept * pre_1).astype(bf16))
        branch_terms.append((branch * pre_1).astype(bf16))
        branches.append(branch_in)
    squares = squares_in_rows(branches)
    high = squares.astype(bf16).astype(f32)
    row = lax.broadcasted_iota(jnp.int32, squares.shape, 0)
    squares = jnp.where(row == 0, high, jnp.where(row == 1, squares - high, 0.0)).astype(bf16)
    terms = jnp.concatenate(
        [jnp.concatenate(kept_terms, axis=1), jnp.concatenate(branch_terms, axis=1)], axis=0
    )
    for copy in held_copies:
        copy.wait()
    for c in range(Z):
        part = jnp.dot(terms, held[c], preferred_element_type=f32)
        scale = scale_ref[1:2, c * feats : (c + 1) * feats]
        out_ref[c, : 2 * t] = (part * scale).astype(bf16)
        out_ref[c, 2 * t :] = jnp.zeros((8, feats), bf16)
        out_ref[c, 2 * t :, :t] = squares


def turn(summed, own, scale, firsts, firsts_at, seconds, seconds_at):
    _, t, feats = summed.shape
    return pl.pallas_call(
        lambda *refs: turn_kernel(firsts_at, seconds_at, *refs),
        out_shape=(
            pltpu.VMEM((Z, 2 * t + 8, feats), bf16),
            pltpu.VMEM((X, t, feats), f32),
            pltpu.VMEM((X, t, feats), f32),
            pltpu.VMEM((X, 8, feats), f32),
        ),
        in_specs=[*[VMEM] * 3, *[ANY] * (2 * X - 1)],
        out_specs=(VMEM,) * 4,
        scratch_shapes=[
            pltpu.VMEM((X - 1, 16 + t, feats), bf16),
            pltpu.VMEM((Z, X * feats, feats), bf16),
            pltpu.SemaphoreType.DMA((X - 1,)),
            pltpu.SemaphoreType.DMA((X, Z)),
        ],
        compiler_params=limit(12),
        name="turn",
    )(near(summed), near(own), near(scale), *firsts, *seconds)


def hidden_kernel(width, came_ref, kept_ref, branch_ref, out_ref, stream_ref):
    t = out_ref.shape[1]
    total = came_ref[0].astype(f32)
    for z in range(1, Z):
        total += came_ref[z].astype(f32)
    inv = inverse(total[2 * t : 2 * t + 1] + total[2 * t + 1 : 2 * t + 2], width, t)
    hidden = activation(total[:t] + total[t : 2 * t] * inv)
    for z in range(Z):
        out_ref[z] = hidden
    for i in range(X):
        stream_ref[i] = (kept_ref[i] + branch_ref[i] * inv).astype(bf16)


def second_hidden(came, kept, branch, width):
    _, t, feats = kept.shape
    return pl.pallas_call(
        lambda *refs: hidden_kernel(width, *refs),
        out_shape=(pltpu.VMEM((Z, t, feats), bf16), pltpu.VMEM(kept.shape, bf16)),
        in_specs=[VMEM] * 3,
        out_specs=(VMEM,) * 2,
        compiler_params=limit(8),
        name="second_hidden",
    )(near(came), near(kept), near(branch))


def squares_kernel(sum_ref, columns_ref, out_ref):
    t = sum_ref.shape[1]
    values = [sum_ref[i].astype(f32) * columns_ref[i, 3:4] for i in range(X)]
    squares = squares_in_rows(values)
    for z in range(Z):
        out_ref[z] = jnp.zeros(out_ref.shape[1:], f32)
        out_ref[z, :, :t] = squares


def squares_of(summed, columns):
    return pl.pallas_call(
        squares_kernel,
        out_shape=pltpu.VMEM((Z, 8, summed.shape[2]), f32),
        in_specs=[VMEM] * 2,
        out_specs=VMEM,
        compiler_params=limit(8),
        name="squares",
    )(near(summed), near(columns))


def last_kernel(width, squares_ref, sum_ref, columns_ref, stream_ref, out_ref):
    t = sum_ref.shape[1]
    total = squares_ref[0]
    for z in range(1, Z):
        total += squares_ref[z]
    inv = inverse(total[0:1], width, t)
    x = lax.axis_index("x")
    for i in range(X):
        branch = sum_ref[i].astype(f32) * columns_ref[i, 3:4] * inv * columns_ref[i, 4:5]
        stream = residual_keep * stream_ref[i].astype(f32) + branch
        out_ref[lax.rem(x + i, X)] = stream.astype(bf16)


def last(squares, summed, columns, stream, width):
    return pl.pallas_call(
        lambda *refs: last_kernel(width, *refs),
        out_shape=pltpu.VMEM(summed.shape, bf16),
        in_specs=[VMEM] * 4,
        out_specs=VMEM,
        compiler_params=limit(8),
        name="last",
    )(near(squares), near(summed), near(columns), near(stream))


def inner(tokens, up_weight, up_scale, down_weight, down_scale, pre_gain, post_gain):
    n_tok, feats = tokens.shape
    hid = up_weight.shape[2]
    width = feats * X * Z
    t_x = n_tok // X

    part = up_product(tokens, pre_gain, up_weight, up_scale).reshape(X, t_x, hid)
    part = exchange(part, "x").astype(f32).sum(axis=0)

    def from_x(payload, s):
        return lax.ppermute(payload, "x", [(i, (i - s) % X) for i in range(X)])

    one, two, three, late, own = packed(
        down_weight, up_weight, tokens, down_scale, pre_gain, post_gain
    )
    firsts = [from_x(one, 1), from_x(two, 2), from_x(three, 3)]
    seconds = [late, firsts[0], from_x(late, 2), firsts[2]]
    near_rows = hid + 16 + t_x
    seconds_at = [0, near_rows, 0, near_rows]

    pieces = part.astype(bf16).reshape(t_x, Z, hid // Z).transpose(1, 0, 2)
    summed = exchange(pieces, "z").astype(f32).sum(axis=0)
    hidden = to_all(activation(summed), "z")
    firsts = after(firsts, hidden)
    mine = down_share(hidden, [one, *firsts], [0] * X)
    summed = down_whole(mine)

    seconds = [seconds[0], firsts[0], *after(seconds[2:3], summed), firsts[2]]
    part, kept, branch, columns = turn(
        summed, own, up_scale, firsts, [hid] * (X - 1), seconds, seconds_at
    )
    came = exchange(part, "z")
    hidden, stream = second_hidden(came, kept, branch, width)
    hidden = exchange(hidden, "z")
    mine = down_share(hidden, seconds, [at + hid for at in seconds_at])
    summed = down_whole(mine)

    squares = squares_of(summed, columns)
    squares = exchange(squares, "z")
    out = last(squares, summed, columns, stream, width)
    return exchange(out, "x").reshape(n_tok, feats)


def solution(mesh):
    split = Mesh(mesh.devices.reshape(Z, X, Y, C), ("z", "x", "y", "core"))
    ra, cb = ("z", "x"), ("y", "core")
    return jax.shard_map(
        inner,
        mesh=split,
        in_specs=(
            P(None, ra),
            P(None, ra, cb),
            P(None, cb),
            P(None, cb, ra),
            P(None, ra),
            P(None, ra),
            P(None, ra),
        ),
        out_specs=P(None, ra),
        check_vma=False,
    )
```

```python
import jax
import jax.numpy as jnp
from jax import lax
from jax.experimental import pallas as pl
from jax.experimental.pallas import tpu as pltpu
from jax.sharding import Mesh, PartitionSpec as P


norm_eps = 1e-06
residual_keep = 0.5
Z, X, Y, C = 8, 4, 8, 2
bf16 = jnp.bfloat16
f32 = jnp.float32
VMEM = pl.BlockSpec(memory_space=pltpu.VMEM)
ANY = pl.BlockSpec(memory_space=pl.ANY)


def exchange(pieces, axis):
    return lax.all_to_all(pieces, axis, split_axis=0, concat_axis=0, tiled=True)


def to_all(shard, axis):
    size = lax.axis_size(axis)
    return exchange(jnp.broadcast_to(shard[None], (size, *shard.shape)), axis)


def activation(up):
    return jnp.square(jnp.maximum(up, 0.0)).astype(bf16)


def near(v):
    return pltpu.with_memory_space_constraint(v, pltpu.VMEM)


def far(v):
    return pltpu.with_memory_space_constraint(v, pltpu.HBM)


def after(blocks, value):
    return [lax.optimization_barrier((b, value))[0] for b in blocks]


def limit(mib):
    return pltpu.CompilerParams(vmem_limit_bytes=mib << 20)


def up_kernel(tokens_ref, gain_ref, weight_ref, scale_ref, out_ref, *scratch):
    tokens, gain, weight, scale, out, in_sems, weight_sems, out_sems = scratch
    parts, _, step = weight.shape
    small = [
        pltpu.make_async_copy(tokens_ref, tokens, in_sems.at[0]),
        pltpu.make_async_copy(gain_ref, gain, in_sems.at[1]),
        pltpu.make_async_copy(scale_ref, scale, in_sems.at[2]),
    ]
    for copy in small:
        copy.start()
    copies = []
    for i in range(parts):
        here = weight_ref.at[0, :, pl.ds(i * step, step)]
        copies.append(pltpu.make_async_copy(here, weight.at[i], weight_sems.at[i]))
        copies[-1].start()
    for copy in small:
        copy.wait()
    scaled = (tokens[...].astype(f32) * gain[0:1]).astype(bf16)
    sent = []
    for i in range(parts):
        copies[i].wait()
        part = jnp.dot(scaled, weight[i].astype(bf16), preferred_element_type=f32)
        out[i] = (part * scale[0:1, i * step : (i + 1) * step]).astype(bf16)
        there = out_ref.at[:, pl.ds(i * step, step)]
        sent.append(pltpu.make_async_copy(out.at[i], there, out_sems.at[i]))
        sent[-1].start()
    for copy in sent:
        copy.wait()


def up_product(tokens, gain, weight, scale):
    n_tok, feats = tokens.shape
    hid = weight.shape[2]
    parts = 4
    return pl.pallas_call(
        up_kernel,
        out_shape=jax.ShapeDtypeStruct((n_tok, hid), bf16),
        in_specs=[ANY] * 4,
        out_specs=ANY,
        scratch_shapes=[
            pltpu.VMEM(tokens.shape, bf16),
            pltpu.VMEM(gain.shape, f32),
            pltpu.VMEM((parts, feats, hid // parts), f32),
            pltpu.VMEM(scale.shape, f32),
            pltpu.VMEM((parts, n_tok, hid // parts), bf16),
            pltpu.SemaphoreType.DMA((3,)),
            pltpu.SemaphoreType.DMA((parts,)),
            pltpu.SemaphoreType.DMA((parts,)),
        ],
        compiler_params=limit(12),
        name="up_product",
    )(far(tokens), far(gain), far(weight), far(scale))


def pack_kernel(down_ref, up_ref, tokens_ref, scale_ref, pre_ref, post_ref, *outs):
    one, two, three, late, own = outs
    hid, feats = down_ref.shape[1:]
    t_x = own.shape[0] - 16
    x = lax.axis_index("x")
    scale, pre, post = scale_ref[...], pre_ref[...], post_ref[...]
    columns = [scale[0:1], post[0:1], pre[1:2], scale[1:2], post[1:2], jnp.zeros((3, feats), f32)]
    columns = jnp.concatenate(columns, axis=0)
    high = columns.astype(bf16).astype(f32)
    columns = jnp.concatenate([high, columns - high], axis=0).astype(bf16)
    for s, ref in ((0, own), (1, one), (2, two), (3, three)):
        at = 0 if s == 0 else hid
        if s:
            ref[:hid] = down_ref[0].astype(bf16)
        ref[at : at + 16] = columns
        rows = pl.multiple_of(lax.rem(x + (X - s), X) * t_x, 32)
        ref[at + 16 : at + 16 + t_x] = tokens_ref[pl.ds(rows, t_x)]
    for ref, at in ((one, hid + 16 + t_x), (three, hid + 16 + t_x), (late, 0)):
        for c in range(hid // feats):
            block = up_ref[0, :, c * feats : (c + 1) * feats].astype(bf16)
            ref[at + c * feats : at + (c + 1) * feats] = block
        ref[at + hid : at + 2 * hid] = down_ref[1].astype(bf16)


def packed(down_weight, up_weight, tokens, scale, pre, post):
    _, hid, feats = down_weight.shape
    t_x = tokens.shape[0] // X
    near_rows, far_rows = hid + 16 + t_x, 2 * hid
    whole = lambda v: pl.BlockSpec(v.shape, lambda i: (0,) * v.ndim)
    rows = (near_rows + far_rows, near_rows, near_rows + far_rows, far_rows, 16 + t_x)
    return pl.pallas_call(
        pack_kernel,
        grid=(1,),
        out_shape=(
            *(pltpu.HBM((r, feats), bf16) for r in rows[:-1]),
            pltpu.VMEM((rows[-1], feats), bf16),
        ),
        in_specs=[
            whole(down_weight),
            pl.BlockSpec((1, feats, hid), lambda i: (1, 0, 0)),
            *[whole(v) for v in (tokens, scale, pre, post)],
        ],
        out_specs=tuple(pl.BlockSpec((r, feats), lambda i: (0, 0)) for r in rows),
        compiler_params=limit(20),
        name="packed",
    )(*[far(v) for v in (down_weight, up_weight, tokens, scale, pre, post)])


def down_kernel(starts, hidden_ref, *refs):
    weights, out_ref, held, sems = refs[:X], refs[X], refs[X + 1], refs[X + 2]
    copies = []
    for i, w in enumerate(weights):
        rows = w.at[pl.ds(starts[i], held.shape[1])]
        copies.append(pltpu.make_async_copy(rows, held.at[i], sems.at[i]))
        copies[-1].start()
    hidden = jnp.concatenate([hidden_ref[z] for z in range(Z)], axis=1)
    for i in range(X):
        copies[i].wait()
        out_ref[i] = jnp.dot(hidden, held[i], preferred_element_type=f32).astype(bf16)


def down_product(hidden, blocks, starts):
    _, t, share = hidden.shape
    feats = blocks[0].shape[1]
    return pl.pallas_call(
        lambda *refs: down_kernel(starts, *refs),
        out_shape=pltpu.VMEM((X, t, feats), bf16),
        in_specs=[VMEM, *[ANY] * X],
        out_specs=VMEM,
        scratch_shapes=[
            pltpu.VMEM((X, Z * share, feats), bf16),
            pltpu.SemaphoreType.DMA((X,)),
        ],
        compiler_params=limit(8),
        name="down_product",
    )(near(hidden), *blocks)


def down_share(hidden, blocks, starts):
    part = down_product(hidden, blocks, starts)
    pieces = part.reshape(Y * C, -1, part.shape[2])
    return exchange(pieces, ("y", "core")).astype(f32).sum(axis=0).astype(bf16)


def down_whole(mine):
    return to_all(mine, ("y", "core")).reshape(X, -1, mine.shape[1])


def squares_in_rows(values):
    total = 0.0
    for v in values:
        total += lax.dot_general(
            jnp.ones((8, v.shape[1]), f32),
            v * v,
            (((1,), (1,)), ((), ())),
            precision=lax.Precision.HIGHEST,
            preferred_element_type=f32,
        )
    return total


def inverse(row, width, t):
    inv = lax.rsqrt(row * (1.0 / width) + norm_eps)
    return jnp.transpose(jnp.broadcast_to(inv, (128, 128)))[:t]


def turn_kernel(firsts_at, seconds_at, lead_ref, sum_ref, own_ref, scale_ref, *refs):
    firsts, seconds = refs[: X - 1], refs[X - 1 : 2 * X - 1]
    out_ref, kept_ref, branch_ref, columns_ref = refs[2 * X - 1 : 2 * X + 3]
    extra, held, scales, sems, held_sems = refs[2 * X + 3 :]
    t, feats = sum_ref.shape[1:]
    copies = [pltpu.make_async_copy(scale_ref, scales, sems.at[X - 1])]
    copies[0].start()
    for i, block in enumerate(firsts):
        rows = block.at[pl.ds(firsts_at[i], extra.shape[1])]
        copies.append(pltpu.make_async_copy(rows, extra.at[i], sems.at[i]))
        copies[-1].start()
    held_copies = []
    for i, block in enumerate(seconds):
        for c in range(Z):
            rows = block.at[pl.ds(seconds_at[i] + c * feats, feats)]
            here = held.at[c, pl.ds(i * feats, feats)]
            held_copies.append(pltpu.make_async_copy(rows, here, held_sems.at[i, c]))
            held_copies[-1].start()
    for copy in copies:
        copy.wait()
    kept_terms, branch_terms, branches = [], [], []
    for i in range(X):
        block = own_ref[...] if i == 0 else extra[i - 1]
        columns = block[:8].astype(f32) + block[8:16].astype(f32)
        columns_ref[i] = columns
        down_0, post_0, pre_1 = [columns[k : k + 1] for k in range(3)]
        kept = residual_keep * block[16:].astype(f32)
        branch_in = (lead_ref[...] if i == 0 else sum_ref[i].astype(f32)) * down_0
        branch = branch_in * post_0
        kept_ref[i] = kept
        branch_ref[i] = branch
        kept_terms.append((kept * pre_1).astype(bf16))
        branch_terms.append((branch * pre_1).astype(bf16))
        branches.append(branch_in)
    squares = squares_in_rows(branches)
    high = squares.astype(bf16).astype(f32)
    row = lax.broadcasted_iota(jnp.int32, squares.shape, 0)
    squares = jnp.where(row == 0, high, jnp.where(row == 1, squares - high, 0.0)).astype(bf16)
    terms = jnp.concatenate(
        [jnp.concatenate(kept_terms, axis=1), jnp.concatenate(branch_terms, axis=1)], axis=0
    )
    for copy in held_copies:
        copy.wait()
    for c in range(Z):
        part = jnp.dot(terms, held[c], preferred_element_type=f32)
        scale = scales[1:2, c * feats : (c + 1) * feats]
        out_ref[c, : 2 * t] = (part * scale).astype(bf16)
        out_ref[c, 2 * t :] = jnp.zeros((8, feats), bf16)
        out_ref[c, 2 * t :, :t] = squares


def turn(summed, own, scale, firsts, firsts_at, seconds, seconds_at):
    _, t, feats = summed.shape
    lead = summed[0].astype(f32)
    return pl.pallas_call(
        lambda *refs: turn_kernel(firsts_at, seconds_at, *refs),
        out_shape=(
            pltpu.VMEM((Z, 2 * t + 8, feats), bf16),
            pltpu.VMEM((X, t, feats), f32),
            pltpu.VMEM((X, t, feats), f32),
            pltpu.VMEM((X, 8, feats), f32),
        ),
        in_specs=[*[VMEM] * 3, *[ANY] * (2 * X)],
        out_specs=(VMEM,) * 4,
        scratch_shapes=[
            pltpu.VMEM((X - 1, 16 + t, feats), bf16),
            pltpu.VMEM((Z, X * feats, feats), bf16),
            pltpu.VMEM(scale.shape, f32),
            pltpu.SemaphoreType.DMA((X,)),
            pltpu.SemaphoreType.DMA((X, Z)),
        ],
        compiler_params=limit(12),
        name="turn",
    )(near(lead), near(summed), near(own), far(scale), *firsts, *seconds)


def hidden_kernel(width, came_ref, kept_ref, branch_ref, out_ref, stream_ref):
    t = out_ref.shape[1]
    total = came_ref[0].astype(f32)
    for z in range(1, Z):
        total += came_ref[z].astype(f32)
    inv = inverse(total[2 * t : 2 * t + 1] + total[2 * t + 1 : 2 * t + 2], width, t)
    hidden = activation(total[:t] + total[t : 2 * t] * inv)
    for z in range(Z):
        out_ref[z] = hidden
    for i in range(X):
        stream_ref[i] = (kept_ref[i] + branch_ref[i] * inv).astype(bf16)


def second_hidden(came, kept, branch, width):
    _, t, feats = kept.shape
    return pl.pallas_call(
        lambda *refs: hidden_kernel(width, *refs),
        out_shape=(pltpu.VMEM((Z, t, feats), bf16), pltpu.VMEM(kept.shape, bf16)),
        in_specs=[VMEM] * 3,
        out_specs=(VMEM,) * 2,
        compiler_params=limit(8),
        name="second_hidden",
    )(near(came), near(kept), near(branch))


def squares_kernel(sum_ref, columns_ref, out_ref):
    t = sum_ref.shape[1]
    values = [sum_ref[i].astype(f32) * columns_ref[i, 3:4] for i in range(X)]
    squares = squares_in_rows(values)
    for z in range(Z):
        out_ref[z] = jnp.zeros(out_ref.shape[1:], f32)
        out_ref[z, :, :t] = squares


def squares_of(summed, columns):
    return pl.pallas_call(
        squares_kernel,
        out_shape=pltpu.VMEM((Z, 8, summed.shape[2]), f32),
        in_specs=[VMEM] * 2,
        out_specs=VMEM,
        compiler_params=limit(8),
        name="squares",
    )(near(summed), near(columns))


def last_kernel(width, squares_ref, sum_ref, columns_ref, stream_ref, out_ref):
    t = sum_ref.shape[1]
    total = squares_ref[0]
    for z in range(1, Z):
        total += squares_ref[z]
    inv = inverse(total[0:1], width, t)
    x = lax.axis_index("x")
    for i in range(X):
        branch = sum_ref[i].astype(f32) * columns_ref[i, 3:4] * inv * columns_ref[i, 4:5]
        stream = residual_keep * stream_ref[i].astype(f32) + branch
        out_ref[lax.rem(x + i, X)] = stream.astype(bf16)


def last(squares, summed, columns, stream, width):
    return pl.pallas_call(
        lambda *refs: last_kernel(width, *refs),
        out_shape=pltpu.VMEM(summed.shape, bf16),
        in_specs=[VMEM] * 4,
        out_specs=VMEM,
        compiler_params=limit(8),
        name="last",
    )(near(squares), near(summed), near(columns), near(stream))


def inner(tokens, up_weight, up_scale, down_weight, down_scale, pre_gain, post_gain):
    n_tok, feats = tokens.shape
    hid = up_weight.shape[2]
    width = feats * X * Z
    t_x = n_tok // X

    part = up_product(tokens, pre_gain, up_weight, up_scale).reshape(X, t_x, hid)
    part = exchange(part, "x").astype(f32).sum(axis=0)

    def from_x(payload, s):
        return lax.ppermute(payload, "x", [(i, (i - s) % X) for i in range(X)])

    one, two, three, late, own = packed(
        down_weight, up_weight, tokens, down_scale, pre_gain, post_gain
    )
    firsts = [from_x(one, 1), from_x(two, 2), from_x(three, 3)]
    seconds = [late, firsts[0], from_x(late, 2), firsts[2]]
    near_rows = hid + 16 + t_x
    seconds_at = [0, near_rows, 0, near_rows]

    pieces = part.astype(bf16).reshape(t_x, Z, hid // Z).transpose(1, 0, 2)
    summed = exchange(pieces, "z").astype(f32).sum(axis=0)
    hidden = to_all(activation(summed), "z")
    firsts = after(firsts, hidden)
    mine = down_share(hidden, [far(one), *firsts], [0] * X)
    summed = down_whole(mine)

    seconds = [far(seconds[0]), firsts[0], *after(seconds[2:3], summed), firsts[2]]
    part, kept, branch, columns = turn(
        summed, own, up_scale, firsts, [hid] * (X - 1), seconds, seconds_at
    )
    came = exchange(part, "z")
    hidden, stream = second_hidden(came, kept, branch, width)
    hidden = exchange(hidden, "z")
    mine = down_share(hidden, seconds, [at + hid for at in seconds_at])
    summed = down_whole(mine)

    squares = squares_of(summed, columns)
    squares = exchange(squares, "z")
    out = last(squares, summed, columns, stream, width)
    return exchange(out, "x").reshape(n_tok, feats)


def solution(mesh):
    split = Mesh(mesh.devices.reshape(Z, X, Y, C), ("z", "x", "y", "core"))
    ra, cb = ("z", "x"), ("y", "core")
    return jax.shard_map(
        inner,
        mesh=split,
        in_specs=(
            P(None, ra),
            P(None, ra, cb),
            P(None, cb),
            P(None, cb, ra),
            P(None, ra),
            P(None, ra),
            P(None, ra),
        ),
        out_specs=P(None, ra),
        check_vma=False,
    )
```

```python
import jax
import jax.numpy as jnp
from jax import lax
from jax.experimental import pallas as pl
from jax.experimental.pallas import tpu as pltpu
from jax.sharding import Mesh, PartitionSpec as P


norm_eps = 1e-06
residual_keep = 0.5
Z, X, Y, C = 8, 4, 8, 2
bf16 = jnp.bfloat16
f32 = jnp.float32
VMEM = pl.BlockSpec(memory_space=pltpu.VMEM)
ANY = pl.BlockSpec(memory_space=pl.ANY)


def exchange(pieces, axis):
    return lax.all_to_all(pieces, axis, split_axis=0, concat_axis=0, tiled=True)


def to_all(shard, axis):
    size = lax.axis_size(axis)
    return exchange(jnp.broadcast_to(shard[None], (size, *shard.shape)), axis)


def activation(up):
    return jnp.square(jnp.maximum(up, 0.0)).astype(bf16)


def near(v):
    return pltpu.with_memory_space_constraint(v, pltpu.VMEM)


def far(v):
    return pltpu.with_memory_space_constraint(v, pltpu.HBM)


def after(blocks, value):
    return [lax.optimization_barrier((b, value))[0] for b in blocks]


def limit(mib):
    return pltpu.CompilerParams(vmem_limit_bytes=mib << 20)


def up_kernel(tokens_ref, gain_ref, weight_ref, scale_ref, out_ref, *scratch):
    tokens, gain, weight, scale, out, in_sems, weight_sems, out_sems = scratch
    parts, feats, step = weight.shape
    small = [
        pltpu.make_async_copy(tokens_ref, tokens, in_sems.at[0]),
        pltpu.make_async_copy(gain_ref, gain, in_sems.at[1]),
        pltpu.make_async_copy(scale_ref, scale, in_sems.at[2]),
    ]
    for copy in small:
        copy.start()
    copies = []
    for i in range(parts):
        here = weight_ref.at[0, :, pl.ds(i * step, step)]
        copies.append(pltpu.make_async_copy(here, weight.at[i], weight_sems.at[i]))
        copies[-1].start()
    for copy in small:
        copy.wait()
    scaled = (tokens[...].astype(f32) * gain[0:1]).astype(bf16)
    sent = []
    for i in range(parts):
        copies[i].wait()
        part = jnp.dot(scaled, weight[i].astype(bf16), preferred_element_type=f32)
        part = (part * scale[0:1, i * step : (i + 1) * step]).astype(bf16)
        for c in range(step // feats):
            z = i * (step // feats) + c
            out[z] = part[:, c * feats : (c + 1) * feats]
            sent.append(pltpu.make_async_copy(out.at[z], out_ref.at[z], out_sems.at[z]))
            sent[-1].start()
    for copy in sent:
        copy.wait()


def up_product(tokens, gain, weight, scale):
    n_tok, feats = tokens.shape
    hid = weight.shape[2]
    parts = 4
    return pl.pallas_call(
        up_kernel,
        out_shape=jax.ShapeDtypeStruct((Z, n_tok, hid // Z), bf16),
        in_specs=[ANY] * 4,
        out_specs=ANY,
        scratch_shapes=[
            pltpu.VMEM(tokens.shape, bf16),
            pltpu.VMEM(gain.shape, f32),
            pltpu.VMEM((parts, feats, hid // parts), f32),
            pltpu.VMEM(scale.shape, f32),
            pltpu.VMEM((Z, n_tok, hid // Z), bf16),
            pltpu.SemaphoreType.DMA((3,)),
            pltpu.SemaphoreType.DMA((parts,)),
            pltpu.SemaphoreType.DMA((Z,)),
        ],
        compiler_params=limit(12),
        name="up_product",
    )(far(tokens), far(gain), far(weight), far(scale))


def pack_kernel(down_ref, up_ref, tokens_ref, scale_ref, pre_ref, post_ref, *outs):
    one, two, three, late, own = outs
    hid, feats = down_ref.shape[1:]
    n = hid // feats
    t_x = own.shape[0] - 16
    x = lax.axis_index("x")
    scale, pre, post = scale_ref[...], pre_ref[...], post_ref[...]
    columns = [scale[0:1], post[0:1], pre[1:2], scale[1:2], post[1:2], jnp.zeros((3, feats), f32)]
    columns = jnp.concatenate(columns, axis=0)
    high = columns.astype(bf16).astype(f32)
    columns = jnp.concatenate([high, columns - high], axis=0).astype(bf16)
    rest = jnp.zeros((feats - 16 - t_x, feats), bf16)
    for s, ref in ((0, own), (1, one), (2, two), (3, three)):
        rows = pl.multiple_of(lax.rem(x + (X - s), X) * t_x, 32)
        block = [columns, tokens_ref[pl.ds(rows, t_x)]]
        if s:
            ref[:n] = down_ref[0].astype(bf16).reshape(n, feats, feats)
            ref[n] = jnp.concatenate([*block, rest], axis=0)
        else:
            ref[...] = jnp.concatenate(block, axis=0)
    for ref, at in ((one, n + 1), (three, n + 1), (late, 0)):
        for c in range(n):
            ref[at + c] = up_ref[0, :, c * feats : (c + 1) * feats].astype(bf16)
        ref[at + n : at + 2 * n] = down_ref[1].astype(bf16).reshape(n, feats, feats)


def packed(down_weight, up_weight, tokens, scale, pre, post):
    _, hid, feats = down_weight.shape
    t_x = tokens.shape[0] // X
    n = hid // feats
    whole = lambda v: pl.BlockSpec(v.shape, lambda i: (0,) * v.ndim)
    blocks = (3 * n + 1, n + 1, 3 * n + 1, 2 * n)
    return pl.pallas_call(
        pack_kernel,
        grid=(1,),
        out_shape=(
            *(pltpu.HBM((b, feats, feats), bf16) for b in blocks),
            pltpu.VMEM((16 + t_x, feats), bf16),
        ),
        in_specs=[
            whole(down_weight),
            pl.BlockSpec((1, feats, hid), lambda i: (1, 0, 0)),
            *[whole(v) for v in (tokens, scale, pre, post)],
        ],
        out_specs=(
            *(pl.BlockSpec((b, feats, feats), lambda i: (0, 0, 0)) for b in blocks),
            pl.BlockSpec((16 + t_x, feats), lambda i: (0, 0)),
        ),
        compiler_params=limit(20),
        name="packed",
    )(*[far(v) for v in (down_weight, up_weight, tokens, scale, pre, post)])


def down_kernel(starts, lead_ref, hidden_ref, *refs):
    weights, out_ref, held, sems = refs[:X], refs[X], refs[X + 1], refs[X + 2]
    copies = []
    for i, w in enumerate(weights):
        blocks = w.at[pl.ds(starts[i], held.shape[1])]
        copies.append(pltpu.make_async_copy(blocks, held.at[i], sems.at[i]))
        copies[-1].start()
    hidden = [lead_ref[...].astype(bf16), *(hidden_ref[z] for z in range(1, Z))]
    hidden = jnp.concatenate(hidden, axis=1)
    for i in (1, 2, 3, 0):
        copies[i].wait()
        weight = held[i].reshape(hidden.shape[1], -1)
        out_ref[i] = jnp.dot(hidden, weight, preferred_element_type=f32).astype(bf16)


def down_product(hidden, blocks, starts):
    _, t, share = hidden.shape
    feats = blocks[0].shape[2]
    lead = hidden[0].astype(f32)
    return pl.pallas_call(
        lambda *refs: down_kernel(starts, *refs),
        out_shape=pltpu.VMEM((X, t, feats), bf16),
        in_specs=[*[VMEM] * 2, *[ANY] * X],
        out_specs=VMEM,
        scratch_shapes=[
            pltpu.VMEM((X, Z * share // feats, feats, feats), bf16),
            pltpu.SemaphoreType.DMA((X,)),
        ],
        compiler_params=limit(8),
        name="down_product",
    )(near(lead), near(hidden), *blocks)


def down_share(hidden, blocks, starts):
    part = down_product(hidden, blocks, starts)
    pieces = part.reshape(Y * C, -1, part.shape[2])
    return exchange(pieces, ("y", "core")).astype(f32).sum(axis=0).astype(bf16)


def down_whole(mine):
    return to_all(mine, ("y", "core")).reshape(X, -1, mine.shape[1])


def squares_in_rows(values):
    total = 0.0
    for v in values:
        total += lax.dot_general(
            jnp.ones((8, v.shape[1]), f32),
            v * v,
            (((1,), (1,)), ((), ())),
            precision=lax.Precision.HIGHEST,
            preferred_element_type=f32,
        )
    return total


def inverse(row, width, t):
    inv = lax.rsqrt(row * (1.0 / width) + norm_eps)
    return jnp.transpose(jnp.broadcast_to(inv, (128, 128)))[:t]


def turn_kernel(firsts_at, seconds_at, lead_ref, sum_ref, own_ref, scale_ref, *refs):
    firsts, seconds = refs[: X - 1], refs[X - 1 : 2 * X - 1]
    out_ref, kept_ref, branch_ref, columns_ref = refs[2 * X - 1 : 2 * X + 3]
    extra, held, scales, sems, held_sems = refs[2 * X + 3 :]
    t, feats = sum_ref.shape[1:]
    copies = [pltpu.make_async_copy(scale_ref, scales, sems.at[X - 1])]
    copies[0].start()
    for i, block in enumerate(firsts):
        rows = block.at[firsts_at, pl.ds(0, extra.shape[1])]
        copies.append(pltpu.make_async_copy(rows, extra.at[i], sems.at[i]))
        copies[-1].start()
    held_copies = []
    for i, block in enumerate(seconds):
        here = held.at[:, pl.ds(i * feats, feats)]
        blocks = block.at[pl.ds(seconds_at[i], Z)]
        held_copies.append(pltpu.make_async_copy(blocks, here, held_sems.at[i]))
        held_copies[-1].start()
    for copy in copies:
        copy.wait()
    kept_terms, branch_terms, branches = [], [], []
    for i in range(X):
        block = own_ref[...] if i == 0 else extra[i - 1]
        columns = block[:8].astype(f32) + block[8:16].astype(f32)
        columns_ref[i] = columns
        down_0, post_0, pre_1 = [columns[k : k + 1] for k in range(3)]
        kept = residual_keep * block[16:].astype(f32)
        branch_in = (lead_ref[...] if i == 0 else sum_ref[i].astype(f32)) * down_0
        branch = branch_in * post_0
        kept_ref[i] = kept
        branch_ref[i] = branch
        kept_terms.append((kept * pre_1).astype(bf16))
        branch_terms.append((branch * pre_1).astype(bf16))
        branches.append(branch_in)
    squares = squares_in_rows(branches)
    high = squares.astype(bf16).astype(f32)
    row = lax.broadcasted_iota(jnp.int32, squares.shape, 0)
    squares = jnp.where(row == 0, high, jnp.where(row == 1, squares - high, 0.0)).astype(bf16)
    terms = jnp.concatenate(
        [jnp.concatenate(kept_terms, axis=1), jnp.concatenate(branch_terms, axis=1)], axis=0
    )
    for copy in held_copies:
        copy.wait()
    for c in range(Z):
        part = jnp.dot(terms, held[c], preferred_element_type=f32)
        scale = scales[1:2, c * feats : (c + 1) * feats]
        out_ref[c, : 2 * t] = (part * scale).astype(bf16)
        out_ref[c, 2 * t :] = jnp.zeros((8, feats), bf16)
        out_ref[c, 2 * t :, :t] = squares


def turn(summed, own, scale, firsts, firsts_at, seconds, seconds_at):
    _, t, feats = summed.shape
    lead = summed[0].astype(f32)
    return pl.pallas_call(
        lambda *refs: turn_kernel(firsts_at, seconds_at, *refs),
        out_shape=(
            pltpu.VMEM((Z, 2 * t + 8, feats), bf16),
            pltpu.VMEM((X, t, feats), f32),
            pltpu.VMEM((X, t, feats), f32),
            pltpu.VMEM((X, 8, feats), f32),
        ),
        in_specs=[*[VMEM] * 3, *[ANY] * (2 * X)],
        out_specs=(VMEM,) * 4,
        scratch_shapes=[
            pltpu.VMEM((X - 1, 16 + t, feats), bf16),
            pltpu.VMEM((Z, X * feats, feats), bf16),
            pltpu.VMEM(scale.shape, f32),
            pltpu.SemaphoreType.DMA((X,)),
            pltpu.SemaphoreType.DMA((X,)),
        ],
        compiler_params=limit(12),
        name="turn",
    )(near(lead), near(summed), near(own), far(scale), *firsts, *seconds)


def hidden_kernel(width, came_ref, kept_ref, branch_ref, out_ref, stream_ref):
    t = out_ref.shape[1]
    total = came_ref[0].astype(f32)
    for z in range(1, Z):
        total += came_ref[z].astype(f32)
    inv = inverse(total[2 * t : 2 * t + 1] + total[2 * t + 1 : 2 * t + 2], width, t)
    hidden = activation(total[:t] + total[t : 2 * t] * inv)
    for z in range(Z):
        out_ref[z] = hidden
    for i in range(X):
        stream_ref[i] = (kept_ref[i] + branch_ref[i] * inv).astype(bf16)


def second_hidden(came, kept, branch, width):
    _, t, feats = kept.shape
    return pl.pallas_call(
        lambda *refs: hidden_kernel(width, *refs),
        out_shape=(pltpu.VMEM((Z, t, feats), bf16), pltpu.VMEM(kept.shape, bf16)),
        in_specs=[VMEM] * 3,
        out_specs=(VMEM,) * 2,
        compiler_params=limit(8),
        name="second_hidden",
    )(near(came), near(kept), near(branch))


def squares_kernel(sum_ref, columns_ref, out_ref):
    t = sum_ref.shape[1]
    values = [sum_ref[i].astype(f32) * columns_ref[i, 3:4] for i in range(X)]
    squares = squares_in_rows(values)
    for z in range(Z):
        out_ref[z] = jnp.zeros(out_ref.shape[1:], f32)
        out_ref[z, :, :t] = squares


def squares_of(summed, columns):
    return pl.pallas_call(
        squares_kernel,
        out_shape=pltpu.VMEM((Z, 8, summed.shape[2]), f32),
        in_specs=[VMEM] * 2,
        out_specs=VMEM,
        compiler_params=limit(8),
        name="squares",
    )(near(summed), near(columns))


def last_kernel(width, squares_ref, sum_ref, columns_ref, stream_ref, out_ref):
    t = sum_ref.shape[1]
    total = squares_ref[0]
    for z in range(1, Z):
        total += squares_ref[z]
    inv = inverse(total[0:1], width, t)
    x = lax.axis_index("x")
    for i in range(X):
        branch = sum_ref[i].astype(f32) * columns_ref[i, 3:4] * inv * columns_ref[i, 4:5]
        stream = residual_keep * stream_ref[i].astype(f32) + branch
        out_ref[lax.rem(x + i, X)] = stream.astype(bf16)


def last(squares, summed, columns, stream, width):
    return pl.pallas_call(
        lambda *refs: last_kernel(width, *refs),
        out_shape=pltpu.VMEM(summed.shape, bf16),
        in_specs=[VMEM] * 4,
        out_specs=VMEM,
        compiler_params=limit(8),
        name="last",
    )(near(squares), near(summed), near(columns), near(stream))


def inner(tokens, up_weight, up_scale, down_weight, down_scale, pre_gain, post_gain):
    n_tok, feats = tokens.shape
    hid = up_weight.shape[2]
    width = feats * X * Z
    t_x = n_tok // X

    part = up_product(tokens, pre_gain, up_weight, up_scale).reshape(Z * X, t_x, feats)
    summed = exchange(part, ("z", "x")).astype(f32).sum(axis=0)

    def from_x(payload, s):
        return lax.ppermute(payload, "x", [(i, (i - s) % X) for i in range(X)])

    one, two, three, late, own = packed(
        down_weight, up_weight, tokens, down_scale, pre_gain, post_gain
    )
    firsts = [from_x(one, 1), from_x(two, 2), from_x(three, 3)]
    seconds = [late, firsts[0], from_x(late, 2), firsts[2]]
    n = hid // feats
    seconds_at = [0, n + 1, 0, n + 1]

    hidden = to_all(activation(summed), "z")
    firsts = after(firsts, hidden)
    mine = down_share(hidden, [far(one), *firsts], [0] * X)
    summed = down_whole(mine)

    seconds = [far(seconds[0]), firsts[0], *after(seconds[2:3], summed), firsts[2]]
    part, kept, branch, columns = turn(
        summed, own, up_scale, firsts, n, seconds, seconds_at
    )
    came = exchange(part, "z")
    hidden, stream = second_hidden(came, kept, branch, width)
    hidden = exchange(hidden, "z")
    mine = down_share(hidden, seconds, [at + n for at in seconds_at])
    summed = down_whole(mine)

    squares = squares_of(summed, columns)
    squares = exchange(squares, "z")
    out = last(squares, summed, columns, stream, width)
    return exchange(out, "x").reshape(n_tok, feats)


def solution(mesh):
    split = Mesh(mesh.devices.reshape(Z, X, Y, C), ("z", "x", "y", "core"))
    ra, cb = ("z", "x"), ("y", "core")
    return jax.shard_map(
        inner,
        mesh=split,
        in_specs=(
            P(None, ra),
            P(None, ra, cb),
            P(None, cb),
            P(None, cb, ra),
            P(None, ra),
            P(None, ra),
            P(None, ra),
        ),
        out_specs=P(None, ra),
        check_vma=False,
    )
```

```python
import jax
import jax.numpy as jnp
from jax import lax
from jax.experimental import pallas as pl
from jax.experimental.pallas import tpu as pltpu
from jax.sharding import Mesh, PartitionSpec as P


norm_eps = 1e-06
residual_keep = 0.5
Z, X, Y, C = 8, 4, 8, 2
bf16 = jnp.bfloat16
f32 = jnp.float32
VMEM = pl.BlockSpec(memory_space=pltpu.VMEM)
ANY = pl.BlockSpec(memory_space=pl.ANY)


def exchange(pieces, axis):
    return lax.all_to_all(pieces, axis, split_axis=0, concat_axis=0, tiled=True)


def to_all(shard, axis):
    size = lax.axis_size(axis)
    return exchange(jnp.broadcast_to(shard[None], (size, *shard.shape)), axis)


def activation(up):
    return jnp.square(jnp.maximum(up, 0.0)).astype(bf16)


def near(v):
    return pltpu.with_memory_space_constraint(v, pltpu.VMEM)


def far(v):
    return pltpu.with_memory_space_constraint(v, pltpu.HBM)


def after(blocks, value):
    return [lax.optimization_barrier((b, value))[0] for b in blocks]


def limit(mib):
    return pltpu.CompilerParams(vmem_limit_bytes=mib << 20)


def up_kernel(tokens_ref, gain_ref, weight_ref, scale_ref, out_ref, *scratch):
    tokens, gain, weight, scale, out, in_sems, weight_sems, out_sems = scratch
    parts, feats, step = weight.shape
    small = [
        pltpu.make_async_copy(tokens_ref, tokens, in_sems.at[0]),
        pltpu.make_async_copy(gain_ref, gain, in_sems.at[1]),
        pltpu.make_async_copy(scale_ref, scale, in_sems.at[2]),
    ]
    for copy in small:
        copy.start()
    copies = []
    for i in range(parts):
        here = weight_ref.at[0, :, pl.ds(i * step, step)]
        copies.append(pltpu.make_async_copy(here, weight.at[i], weight_sems.at[i]))
        copies[-1].start()
    for copy in small:
        copy.wait()
    scaled = (tokens[...].astype(f32) * gain[0:1]).astype(bf16)
    sent = []
    for i in range(parts):
        copies[i].wait()
        part = jnp.dot(scaled, weight[i].astype(bf16), preferred_element_type=f32)
        part = (part * scale[0:1, i * step : (i + 1) * step]).astype(bf16)
        for c in range(step // feats):
            z = i * (step // feats) + c
            out[z] = part[:, c * feats : (c + 1) * feats]
            sent.append(pltpu.make_async_copy(out.at[z], out_ref.at[z], out_sems.at[z]))
            sent[-1].start()
    for copy in sent:
        copy.wait()


def up_product(tokens, gain, weight, scale):
    n_tok, feats = tokens.shape
    hid = weight.shape[2]
    parts = 4
    return pl.pallas_call(
        up_kernel,
        out_shape=jax.ShapeDtypeStruct((Z, n_tok, hid // Z), bf16),
        in_specs=[ANY] * 4,
        out_specs=ANY,
        scratch_shapes=[
            pltpu.VMEM(tokens.shape, bf16),
            pltpu.VMEM(gain.shape, f32),
            pltpu.VMEM((parts, feats, hid // parts), f32),
            pltpu.VMEM(scale.shape, f32),
            pltpu.VMEM((Z, n_tok, hid // Z), bf16),
            pltpu.SemaphoreType.DMA((3,)),
            pltpu.SemaphoreType.DMA((parts,)),
            pltpu.SemaphoreType.DMA((Z,)),
        ],
        compiler_params=limit(12),
        name="up_product",
    )(far(tokens), far(gain), far(weight), far(scale))


def pack_kernel(down_ref, up_ref, tokens_ref, scale_ref, pre_ref, post_ref, *outs):
    one, two, three, late, own = outs
    hid, feats = down_ref.shape[1:]
    n = hid // feats
    t_x = own.shape[0] - 16
    x = lax.axis_index("x")
    scale, pre, post = scale_ref[...], pre_ref[...], post_ref[...]
    columns = [scale[0:1], post[0:1], pre[1:2], scale[1:2], post[1:2], jnp.zeros((3, feats), f32)]
    columns = jnp.concatenate(columns, axis=0)
    high = columns.astype(bf16).astype(f32)
    columns = jnp.concatenate([high, columns - high], axis=0).astype(bf16)
    rest = jnp.zeros((feats - 16 - t_x, feats), bf16)
    for s, ref in ((0, own), (1, one), (2, two), (3, three)):
        rows = pl.multiple_of(lax.rem(x + (X - s), X) * t_x, 32)
        block = [columns, tokens_ref[pl.ds(rows, t_x)]]
        if s:
            ref[:n] = down_ref[0].astype(bf16).reshape(n, feats, feats)
            ref[n] = jnp.concatenate([*block, rest], axis=0)
        else:
            ref[...] = jnp.concatenate(block, axis=0)
    for c in range(n):
        late[c] = up_ref[0, :, c * feats : (c + 1) * feats].astype(bf16)
    late[n:] = down_ref[1].astype(bf16).reshape(n, feats, feats)


def packed(down_weight, up_weight, tokens, scale, pre, post):
    _, hid, feats = down_weight.shape
    t_x = tokens.shape[0] // X
    n = hid // feats
    whole = lambda v: pl.BlockSpec(v.shape, lambda i: (0,) * v.ndim)
    blocks = (n + 1, n + 1, n + 1, 2 * n)
    return pl.pallas_call(
        pack_kernel,
        grid=(1,),
        out_shape=(
            *(pltpu.HBM((b, feats, feats), bf16) for b in blocks),
            pltpu.VMEM((16 + t_x, feats), bf16),
        ),
        in_specs=[
            whole(down_weight),
            pl.BlockSpec((1, feats, hid), lambda i: (1, 0, 0)),
            *[whole(v) for v in (tokens, scale, pre, post)],
        ],
        out_specs=(
            *(pl.BlockSpec((b, feats, feats), lambda i: (0, 0, 0)) for b in blocks),
            pl.BlockSpec((16 + t_x, feats), lambda i: (0, 0)),
        ),
        compiler_params=limit(20),
        name="packed",
    )(*[far(v) for v in (down_weight, up_weight, tokens, scale, pre, post)])


def down_kernel(starts, lead_ref, hidden_ref, *refs):
    weights, out_ref, held, sems = refs[:X], refs[X], refs[X + 1], refs[X + 2]
    copies = []
    for i, w in enumerate(weights):
        blocks = w.at[pl.ds(starts[i], held.shape[1])]
        copies.append(pltpu.make_async_copy(blocks, held.at[i], sems.at[i]))
        copies[-1].start()
    hidden = [lead_ref[...].astype(bf16), *(hidden_ref[z] for z in range(1, Z))]
    hidden = jnp.concatenate(hidden, axis=1)
    for i in (1, 2, 3, 0):
        copies[i].wait()
        weight = held[i].reshape(hidden.shape[1], -1)
        out_ref[i] = jnp.dot(hidden, weight, preferred_element_type=f32).astype(bf16)


def down_product(hidden, blocks, starts):
    _, t, share = hidden.shape
    feats = blocks[0].shape[2]
    lead = hidden[0].astype(f32)
    return pl.pallas_call(
        lambda *refs: down_kernel(starts, *refs),
        out_shape=pltpu.VMEM((X, t, feats), bf16),
        in_specs=[*[VMEM] * 2, *[ANY] * X],
        out_specs=VMEM,
        scratch_shapes=[
            pltpu.VMEM((X, Z * share // feats, feats, feats), bf16),
            pltpu.SemaphoreType.DMA((X,)),
        ],
        compiler_params=limit(8),
        name="down_product",
    )(near(lead), near(hidden), *blocks)


def down_share(hidden, blocks, starts):
    part = down_product(hidden, blocks, starts)
    pieces = part.reshape(Y * C, -1, part.shape[2])
    return exchange(pieces, ("y", "core")).astype(f32).sum(axis=0).astype(bf16)


def down_whole(mine):
    return to_all(mine, ("y", "core")).reshape(X, -1, mine.shape[1])


def squares_in_rows(values):
    total = 0.0
    for v in values:
        total += lax.dot_general(
            jnp.ones((8, v.shape[1]), f32),
            v * v,
            (((1,), (1,)), ((), ())),
            precision=lax.Precision.HIGHEST,
            preferred_element_type=f32,
        )
    return total


def inverse(row, width, t):
    inv = lax.rsqrt(row * (1.0 / width) + norm_eps)
    return jnp.transpose(jnp.broadcast_to(inv, (128, 128)))[:t]


def turn_kernel(firsts_at, seconds_at, lead_ref, sum_ref, own_ref, scale_ref, *refs):
    firsts, seconds = refs[: X - 1], refs[X - 1 : 2 * X - 1]
    out_ref, kept_ref, branch_ref, columns_ref = refs[2 * X - 1 : 2 * X + 3]
    extra, held, scales, sems, held_sems = refs[2 * X + 3 :]
    t, feats = sum_ref.shape[1:]
    copies = [pltpu.make_async_copy(scale_ref, scales, sems.at[X - 1])]
    copies[0].start()
    for i, block in enumerate(firsts):
        rows = block.at[firsts_at, pl.ds(0, extra.shape[1])]
        copies.append(pltpu.make_async_copy(rows, extra.at[i], sems.at[i]))
        copies[-1].start()
    held_copies = []
    for i, block in enumerate(seconds):
        here = held.at[:, pl.ds(i * feats, feats)]
        blocks = block.at[pl.ds(seconds_at[i], Z)]
        held_copies.append(pltpu.make_async_copy(blocks, here, held_sems.at[i]))
        held_copies[-1].start()
    for copy in copies:
        copy.wait()
    kept_terms, branch_terms, branches = [], [], []
    for i in range(X):
        block = own_ref[...] if i == 0 else extra[i - 1]
        columns = block[:8].astype(f32) + block[8:16].astype(f32)
        columns_ref[i] = columns
        down_0, post_0, pre_1 = [columns[k : k + 1] for k in range(3)]
        kept = residual_keep * block[16:].astype(f32)
        branch_in = (lead_ref[...] if i == 0 else sum_ref[i].astype(f32)) * down_0
        branch = branch_in * post_0
        kept_ref[i] = kept
        branch_ref[i] = branch
        kept_terms.append((kept * pre_1).astype(bf16))
        branch_terms.append((branch * pre_1).astype(bf16))
        branches.append(branch_in)
    squares = squares_in_rows(branches)
    high = squares.astype(bf16).astype(f32)
    row = lax.broadcasted_iota(jnp.int32, squares.shape, 0)
    squares = jnp.where(row == 0, high, jnp.where(row == 1, squares - high, 0.0)).astype(bf16)
    terms = jnp.concatenate(
        [jnp.concatenate(kept_terms, axis=1), jnp.concatenate(branch_terms, axis=1)], axis=0
    )
    for copy in held_copies:
        copy.wait()
    for c in range(Z):
        part = jnp.dot(terms, held[c], preferred_element_type=f32)
        scale = scales[1:2, c * feats : (c + 1) * feats]
        out_ref[c, : 2 * t] = (part * scale).astype(bf16)
        out_ref[c, 2 * t :] = jnp.zeros((8, feats), bf16)
        out_ref[c, 2 * t :, :t] = squares


def turn(summed, own, scale, firsts, firsts_at, seconds, seconds_at):
    _, t, feats = summed.shape
    lead = summed[0].astype(f32)
    return pl.pallas_call(
        lambda *refs: turn_kernel(firsts_at, seconds_at, *refs),
        out_shape=(
            pltpu.VMEM((Z, 2 * t + 8, feats), bf16),
            pltpu.VMEM((X, t, feats), f32),
            pltpu.VMEM((X, t, feats), f32),
            pltpu.VMEM((X, 8, feats), f32),
        ),
        in_specs=[*[VMEM] * 3, *[ANY] * (2 * X)],
        out_specs=(VMEM,) * 4,
        scratch_shapes=[
            pltpu.VMEM((X - 1, 16 + t, feats), bf16),
            pltpu.VMEM((Z, X * feats, feats), bf16),
            pltpu.VMEM(scale.shape, f32),
            pltpu.SemaphoreType.DMA((X,)),
            pltpu.SemaphoreType.DMA((X,)),
        ],
        compiler_params=limit(12),
        name="turn",
    )(near(lead), near(summed), near(own), far(scale), *firsts, *seconds)


def hidden_kernel(width, came_ref, kept_ref, branch_ref, out_ref, stream_ref):
    t = out_ref.shape[1]
    total = came_ref[0].astype(f32)
    for z in range(1, Z):
        total += came_ref[z].astype(f32)
    inv = inverse(total[2 * t : 2 * t + 1] + total[2 * t + 1 : 2 * t + 2], width, t)
    hidden = activation(total[:t] + total[t : 2 * t] * inv)
    for z in range(Z):
        out_ref[z] = hidden
    for i in range(X):
        stream_ref[i] = (kept_ref[i] + branch_ref[i] * inv).astype(bf16)


def second_hidden(came, kept, branch, width):
    _, t, feats = kept.shape
    return pl.pallas_call(
        lambda *refs: hidden_kernel(width, *refs),
        out_shape=(pltpu.VMEM((Z, t, feats), bf16), pltpu.VMEM(kept.shape, bf16)),
        in_specs=[VMEM] * 3,
        out_specs=(VMEM,) * 2,
        compiler_params=limit(8),
        name="second_hidden",
    )(near(came), near(kept), near(branch))


def squares_kernel(sum_ref, columns_ref, out_ref):
    t = sum_ref.shape[1]
    values = [sum_ref[i].astype(f32) * columns_ref[i, 3:4] for i in range(X)]
    squares = squares_in_rows(values)
    for z in range(Z):
        out_ref[z] = jnp.zeros(out_ref.shape[1:], f32)
        out_ref[z, :, :t] = squares


def squares_of(summed, columns):
    return pl.pallas_call(
        squares_kernel,
        out_shape=pltpu.VMEM((Z, 8, summed.shape[2]), f32),
        in_specs=[VMEM] * 2,
        out_specs=VMEM,
        compiler_params=limit(8),
        name="squares",
    )(near(summed), near(columns))


def last_kernel(width, squares_ref, sum_ref, columns_ref, stream_ref, out_ref):
    t = sum_ref.shape[1]
    total = squares_ref[0]
    for z in range(1, Z):
        total += squares_ref[z]
    inv = inverse(total[0:1], width, t)
    x = lax.axis_index("x")
    for i in range(X):
        branch = sum_ref[i].astype(f32) * columns_ref[i, 3:4] * inv * columns_ref[i, 4:5]
        stream = residual_keep * stream_ref[i].astype(f32) + branch
        out_ref[lax.rem(x + i, X)] = stream.astype(bf16)


def last(squares, summed, columns, stream, width):
    return pl.pallas_call(
        lambda *refs: last_kernel(width, *refs),
        out_shape=pltpu.VMEM(summed.shape, bf16),
        in_specs=[VMEM] * 4,
        out_specs=VMEM,
        compiler_params=limit(8),
        name="last",
    )(near(squares), near(summed), near(columns), near(stream))


def inner(tokens, up_weight, up_scale, down_weight, down_scale, pre_gain, post_gain):
    n_tok, feats = tokens.shape
    hid = up_weight.shape[2]
    width = feats * X * Z
    t_x = n_tok // X

    part = up_product(tokens, pre_gain, up_weight, up_scale).reshape(Z * X, t_x, feats)
    summed = exchange(part, ("z", "x")).astype(f32).sum(axis=0)

    def from_x(payload, s):
        return lax.ppermute(payload, "x", [(i, (i - s) % X) for i in range(X)])

    one, two, three, late, own = packed(
        down_weight, up_weight, tokens, down_scale, pre_gain, post_gain
    )
    firsts = [from_x(one, 1), from_x(two, 2), from_x(three, 3)]
    seconds = [from_x(late, s) for s in (1, 2, 3)]
    n = hid // feats

    hidden = to_all(activation(summed), "z")
    firsts = after(firsts, hidden)
    mine = down_share(hidden, [far(one), *firsts], [0] * X)
    summed = down_whole(mine)

    seconds = [far(late), *after(seconds, summed)]
    part, kept, branch, columns = turn(
        summed, own, up_scale, firsts, n, seconds, [0] * X
    )
    came = exchange(part, "z")
    hidden, stream = second_hidden(came, kept, branch, width)
    hidden = exchange(hidden, "z")
    mine = down_share(hidden, seconds, [n] * X)
    summed = down_whole(mine)

    squares = squares_of(summed, columns)
    squares = exchange(squares, "z")
    out = last(squares, summed, columns, stream, width)
    return exchange(out, "x").reshape(n_tok, feats)


def solution(mesh):
    split = Mesh(mesh.devices.reshape(Z, X, Y, C), ("z", "x", "y", "core"))
    ra, cb = ("z", "x"), ("y", "core")
    return jax.shard_map(
        inner,
        mesh=split,
        in_specs=(
            P(None, ra),
            P(None, ra, cb),
            P(None, cb),
            P(None, cb, ra),
            P(None, ra),
            P(None, ra),
            P(None, ra),
        ),
        out_specs=P(None, ra),
        check_vma=False,
    )
```

```python
import jax
import jax.numpy as jnp
from jax import lax
from jax.experimental import pallas as pl
from jax.experimental.pallas import tpu as pltpu
from jax.sharding import Mesh, PartitionSpec as P


norm_eps = 1e-06
residual_keep = 0.5
Z, X, Y, C = 8, 4, 8, 2
bf16 = jnp.bfloat16
f32 = jnp.float32
VMEM = pl.BlockSpec(memory_space=pltpu.VMEM)
ANY = pl.BlockSpec(memory_space=pl.ANY)


def exchange(pieces, axis):
    return lax.all_to_all(pieces, axis, split_axis=0, concat_axis=0, tiled=True)


def to_all(shard, axis):
    size = lax.axis_size(axis)
    return exchange(jnp.broadcast_to(shard[None], (size, *shard.shape)), axis)


def activation(up):
    return jnp.square(jnp.maximum(up, 0.0)).astype(bf16)


def near(v):
    return pltpu.with_memory_space_constraint(v, pltpu.VMEM)


def far(v):
    return pltpu.with_memory_space_constraint(v, pltpu.HBM)


def after(blocks, value):
    return [lax.optimization_barrier((b, value))[0] for b in blocks]


def limit(mib):
    return pltpu.CompilerParams(vmem_limit_bytes=mib << 20)


def up_kernel(tokens_ref, gain_ref, weight_ref, scale_ref, down_ref, out_ref, first_ref, *scratch):
    tokens, gain, weight, scale, down, out, first, in_sems, weight_sems, out_sems = scratch
    parts, feats, step = weight.shape
    small = [
        pltpu.make_async_copy(tokens_ref, tokens, in_sems.at[0]),
        pltpu.make_async_copy(gain_ref, gain, in_sems.at[1]),
        pltpu.make_async_copy(scale_ref, scale, in_sems.at[2]),
    ]
    for copy in small:
        copy.start()
    copies = []
    for i in range(parts):
        here = weight_ref.at[0, :, pl.ds(i * step, step)]
        copies.append(pltpu.make_async_copy(here, weight.at[i], weight_sems.at[i]))
        copies[-1].start()
    down_copy = pltpu.make_async_copy(down_ref.at[0], down, in_sems.at[3])
    down_copy.start()
    for copy in small:
        copy.wait()
    scaled = (tokens[...].astype(f32) * gain[0:1]).astype(bf16)
    sent = []
    for i in range(parts):
        copies[i].wait()
        part = jnp.dot(scaled, weight[i].astype(bf16), preferred_element_type=f32)
        part = (part * scale[0:1, i * step : (i + 1) * step]).astype(bf16)
        for c in range(step // feats):
            z = i * (step // feats) + c
            out[z] = part[:, c * feats : (c + 1) * feats]
            sent.append(pltpu.make_async_copy(out.at[z], out_ref.at[z], out_sems.at[z]))
            sent[-1].start()
    down_copy.wait()
    first[...] = down[...].astype(bf16).reshape(first.shape)
    sent.append(pltpu.make_async_copy(first, first_ref, in_sems.at[4]))
    sent[-1].start()
    for copy in sent:
        copy.wait()


def up_product(tokens, gain, weight, scale, down_weight):
    n_tok, feats = tokens.shape
    hid = weight.shape[2]
    parts = 4
    blocks = (hid // feats, feats, feats)
    return pl.pallas_call(
        up_kernel,
        out_shape=(pltpu.HBM((Z, n_tok, hid // Z), bf16), pltpu.HBM(blocks, bf16)),
        in_specs=[ANY] * 5,
        out_specs=(ANY,) * 2,
        scratch_shapes=[
            pltpu.VMEM(tokens.shape, bf16),
            pltpu.VMEM(gain.shape, f32),
            pltpu.VMEM((parts, feats, hid // parts), f32),
            pltpu.VMEM(scale.shape, f32),
            pltpu.VMEM(down_weight.shape[1:], f32),
            pltpu.VMEM((Z, n_tok, hid // Z), bf16),
            pltpu.VMEM(blocks, bf16),
            pltpu.SemaphoreType.DMA((5,)),
            pltpu.SemaphoreType.DMA((parts,)),
            pltpu.SemaphoreType.DMA((Z,)),
        ],
        compiler_params=limit(12),
        name="up_product",
    )(*[far(v) for v in (tokens, gain, weight, scale, down_weight)])


def pack_kernel(down_ref, up_ref, tokens_ref, scale_ref, pre_ref, post_ref, *outs):
    own = outs[-1]
    hid, feats = down_ref.shape[1:]
    n = hid // feats
    t_x = own.shape[0] - 16
    x = lax.axis_index("x")
    scale, pre, post = scale_ref[...], pre_ref[...], post_ref[...]
    columns = [scale[0:1], post[0:1], pre[1:2], scale[1:2], post[1:2], jnp.zeros((3, feats), f32)]
    columns = jnp.concatenate(columns, axis=0)
    high = columns.astype(bf16).astype(f32)
    columns = jnp.concatenate([high, columns - high], axis=0).astype(bf16)
    rest = jnp.zeros((feats - 16 - t_x, feats), bf16)
    down = down_ref[0].astype(bf16).reshape(n, feats, feats)
    for s, ref in enumerate((own, *outs[:-1])):
        rows = pl.multiple_of(lax.rem(x + (X - s), X) * t_x, 32)
        block = [columns, tokens_ref[pl.ds(rows, t_x)]]
        if s == 0:
            ref[...] = jnp.concatenate(block, axis=0)
            continue
        for c in range(n):
            ref[c] = up_ref[0, :, c * feats : (c + 1) * feats].astype(bf16)
        ref[n : 2 * n] = down
        ref[2 * n] = jnp.concatenate([*block, rest], axis=0)


def packed(down_weight, up_weight, tokens, scale, pre, post):
    _, hid, feats = down_weight.shape
    t_x = tokens.shape[0] // X
    blocks = (2 * (hid // feats) + 1, feats, feats)
    whole = lambda v: pl.BlockSpec(v.shape, lambda i: (0,) * v.ndim)
    last_layer = lambda v: pl.BlockSpec((1, *v.shape[1:]), lambda i: (1, 0, 0))
    return pl.pallas_call(
        pack_kernel,
        grid=(1,),
        out_shape=(
            *(pltpu.HBM(blocks, bf16) for _ in range(X - 1)),
            pltpu.VMEM((16 + t_x, feats), bf16),
        ),
        in_specs=[
            last_layer(down_weight),
            last_layer(up_weight),
            *[whole(v) for v in (tokens, scale, pre, post)],
        ],
        out_specs=(
            *(pl.BlockSpec(blocks, lambda i: (0, 0, 0)) for _ in range(X - 1)),
            pl.BlockSpec((16 + t_x, feats), lambda i: (0, 0)),
        ),
        compiler_params=limit(20),
        name="packed",
    )(*[far(v) for v in (down_weight, up_weight, tokens, scale, pre, post)])


def down_kernel(start, lead_ref, hidden_ref, *refs):
    weights, out_ref, held, sems = refs[:X], refs[X], refs[X + 1], refs[X + 2]
    copies = []
    for i, w in enumerate(weights):
        blocks = w.at[pl.ds(start, held.shape[1])]
        copies.append(pltpu.make_async_copy(blocks, held.at[i], sems.at[i]))
        copies[-1].start()
    hidden = [lead_ref[...].astype(bf16), *(hidden_ref[z] for z in range(1, Z))]
    hidden = jnp.concatenate(hidden, axis=1)
    for i in (1, 2, 3, 0):
        copies[i].wait()
        weight = held[i].reshape(hidden.shape[1], -1)
        out_ref[i] = jnp.dot(hidden, weight, preferred_element_type=f32).astype(bf16)


def down_product(hidden, blocks, start):
    _, t, share = hidden.shape
    feats = blocks[0].shape[2]
    lead = hidden[0].astype(f32)
    return pl.pallas_call(
        lambda *refs: down_kernel(start, *refs),
        out_shape=pltpu.VMEM((X, t, feats), bf16),
        in_specs=[*[VMEM] * 2, *[ANY] * X],
        out_specs=VMEM,
        scratch_shapes=[
            pltpu.VMEM((X, Z * share // feats, feats, feats), bf16),
            pltpu.SemaphoreType.DMA((X,)),
        ],
        compiler_params=limit(8),
        name="down_product",
    )(near(lead), near(hidden), *blocks)


def down_share(hidden, blocks, start):
    part = down_product(hidden, blocks, start)
    pieces = part.reshape(Y * C, -1, part.shape[2])
    return exchange(pieces, ("y", "core")).astype(f32).sum(axis=0).astype(bf16)


def down_whole(mine):
    return to_all(mine, ("y", "core")).reshape(X, -1, mine.shape[1])


def squares_in_rows(values):
    total = 0.0
    for v in values:
        total += lax.dot_general(
            jnp.ones((8, v.shape[1]), f32),
            v * v,
            (((1,), (1,)), ((), ())),
            precision=lax.Precision.HIGHEST,
            preferred_element_type=f32,
        )
    return total


def inverse(row, width, t):
    inv = lax.rsqrt(row * (1.0 / width) + norm_eps)
    return jnp.transpose(jnp.broadcast_to(inv, (128, 128)))[:t]


def turn_kernel(lead_ref, sum_ref, own_ref, scale_ref, *refs):
    blocks = refs[:X]
    out_ref, kept_ref, branch_ref, columns_ref = refs[X : X + 4]
    extra, held, scales, sems, held_sems = refs[X + 4 :]
    t, feats = sum_ref.shape[1:]
    copies = [pltpu.make_async_copy(scale_ref, scales, sems.at[X - 1])]
    copies[0].start()
    for i in range(1, X):
        rows = blocks[i].at[2 * Z, pl.ds(0, extra.shape[1])]
        copies.append(pltpu.make_async_copy(rows, extra.at[i - 1], sems.at[i - 1]))
        copies[-1].start()
    held_copies = []
    for i in range(X):
        here = held.at[:, pl.ds(i * feats, feats)]
        held_copies.append(pltpu.make_async_copy(blocks[i].at[pl.ds(0, Z)], here, held_sems.at[i]))
        held_copies[-1].start()
    for copy in copies:
        copy.wait()
    kept_terms, branch_terms, branches = [], [], []
    for i in range(X):
        block = own_ref[...] if i == 0 else extra[i - 1]
        columns = block[:8].astype(f32) + block[8:16].astype(f32)
        columns_ref[i] = columns
        down_0, post_0, pre_1 = [columns[k : k + 1] for k in range(3)]
        kept = residual_keep * block[16:].astype(f32)
        branch_in = (lead_ref[...] if i == 0 else sum_ref[i].astype(f32)) * down_0
        branch = branch_in * post_0
        kept_ref[i] = kept
        branch_ref[i] = branch
        kept_terms.append((kept * pre_1).astype(bf16))
        branch_terms.append((branch * pre_1).astype(bf16))
        branches.append(branch_in)
    squares = squares_in_rows(branches)
    high = squares.astype(bf16).astype(f32)
    row = lax.broadcasted_iota(jnp.int32, squares.shape, 0)
    squares = jnp.where(row == 0, high, jnp.where(row == 1, squares - high, 0.0)).astype(bf16)
    terms = jnp.concatenate(
        [jnp.concatenate(kept_terms, axis=1), jnp.concatenate(branch_terms, axis=1)], axis=0
    )
    for copy in held_copies:
        copy.wait()
    for c in range(Z):
        part = jnp.dot(terms, held[c], preferred_element_type=f32)
        scale = scales[1:2, c * feats : (c + 1) * feats]
        out_ref[c, : 2 * t] = (part * scale).astype(bf16)
        out_ref[c, 2 * t :] = jnp.zeros((8, feats), bf16)
        out_ref[c, 2 * t :, :t] = squares


def turn(summed, own, scale, blocks):
    _, t, feats = summed.shape
    lead = summed[0].astype(f32)
    return pl.pallas_call(
        turn_kernel,
        out_shape=(
            pltpu.VMEM((Z, 2 * t + 8, feats), bf16),
            pltpu.VMEM((X, t, feats), f32),
            pltpu.VMEM((X, t, feats), f32),
            pltpu.VMEM((X, 8, feats), f32),
        ),
        in_specs=[*[VMEM] * 3, *[ANY] * (X + 1)],
        out_specs=(VMEM,) * 4,
        scratch_shapes=[
            pltpu.VMEM((X - 1, 16 + t, feats), bf16),
            pltpu.VMEM((Z, X * feats, feats), bf16),
            pltpu.VMEM(scale.shape, f32),
            pltpu.SemaphoreType.DMA((X,)),
            pltpu.SemaphoreType.DMA((X,)),
        ],
        compiler_params=limit(12),
        name="turn",
    )(near(lead), near(summed), near(own), far(scale), *blocks)


def hidden_kernel(width, came_ref, kept_ref, branch_ref, out_ref, stream_ref):
    t = out_ref.shape[1]
    total = came_ref[0].astype(f32)
    for z in range(1, Z):
        total += came_ref[z].astype(f32)
    inv = inverse(total[2 * t : 2 * t + 1] + total[2 * t + 1 : 2 * t + 2], width, t)
    hidden = activation(total[:t] + total[t : 2 * t] * inv)
    for z in range(Z):
        out_ref[z] = hidden
    for i in range(X):
        stream_ref[i] = (kept_ref[i] + branch_ref[i] * inv).astype(bf16)


def second_hidden(came, kept, branch, width):
    _, t, feats = kept.shape
    return pl.pallas_call(
        lambda *refs: hidden_kernel(width, *refs),
        out_shape=(pltpu.VMEM((Z, t, feats), bf16), pltpu.VMEM(kept.shape, bf16)),
        in_specs=[VMEM] * 3,
        out_specs=(VMEM,) * 2,
        compiler_params=limit(8),
        name="second_hidden",
    )(near(came), near(kept), near(branch))


def squares_kernel(sum_ref, columns_ref, out_ref):
    t = sum_ref.shape[1]
    values = [sum_ref[i].astype(f32) * columns_ref[i, 3:4] for i in range(X)]
    squares = squares_in_rows(values)
    for z in range(Z):
        out_ref[z] = jnp.zeros(out_ref.shape[1:], f32)
        out_ref[z, :, :t] = squares


def squares_of(summed, columns):
    return pl.pallas_call(
        squares_kernel,
        out_shape=pltpu.VMEM((Z, 8, summed.shape[2]), f32),
        in_specs=[VMEM] * 2,
        out_specs=VMEM,
        compiler_params=limit(8),
        name="squares",
    )(near(summed), near(columns))


def last_kernel(width, squares_ref, sum_ref, columns_ref, stream_ref, out_ref):
    t = sum_ref.shape[1]
    total = squares_ref[0]
    for z in range(1, Z):
        total += squares_ref[z]
    inv = inverse(total[0:1], width, t)
    x = lax.axis_index("x")
    for i in range(X):
        branch = sum_ref[i].astype(f32) * columns_ref[i, 3:4] * inv * columns_ref[i, 4:5]
        stream = residual_keep * stream_ref[i].astype(f32) + branch
        out_ref[lax.rem(x + i, X)] = stream.astype(bf16)


def last(squares, summed, columns, stream, width):
    return pl.pallas_call(
        lambda *refs: last_kernel(width, *refs),
        out_shape=pltpu.VMEM(summed.shape, bf16),
        in_specs=[VMEM] * 4,
        out_specs=VMEM,
        compiler_params=limit(8),
        name="last",
    )(near(squares), near(summed), near(columns), near(stream))


def inner(tokens, up_weight, up_scale, down_weight, down_scale, pre_gain, post_gain):
    n_tok, feats = tokens.shape
    hid = up_weight.shape[2]
    width = feats * X * Z
    t_x = n_tok // X

    part, first = up_product(tokens, pre_gain, up_weight, up_scale, down_weight)
    part = part.reshape(Z * X, t_x, feats)
    summed = exchange(part, ("z", "x")).astype(f32).sum(axis=0)

    def from_x(payload, s):
        return lax.ppermute(payload, "x", [(i, (i - s) % X) for i in range(X)])

    *payloads, own = packed(down_weight, up_weight, tokens, down_scale, pre_gain, post_gain)
    firsts = [from_x(first, s) for s in (1, 2, 3)]
    seconds = [from_x(payloads[s - 1], s) for s in (1, 2, 3)]

    hidden = to_all(activation(summed), "z")
    mine = down_share(hidden, [far(first), *after(firsts, hidden)], 0)
    summed = down_whole(mine)

    seconds = [far(payloads[0]), *after(seconds, summed)]
    part, kept, branch, columns = turn(summed, own, up_scale, seconds)
    came = exchange(part, "z")
    hidden, stream = second_hidden(came, kept, branch, width)
    hidden = exchange(hidden, "z")
    mine = down_share(hidden, seconds, hid // feats)
    summed = down_whole(mine)

    squares = squares_of(summed, columns)
    squares = exchange(squares, "z")
    out = last(squares, summed, columns, stream, width)
    return exchange(out, "x").reshape(n_tok, feats)


def solution(mesh):
    split = Mesh(mesh.devices.reshape(Z, X, Y, C), ("z", "x", "y", "core"))
    ra, cb = ("z", "x"), ("y", "core")
    return jax.shard_map(
        inner,
        mesh=split,
        in_specs=(
            P(None, ra),
            P(None, ra, cb),
            P(None, cb),
            P(None, cb, ra),
            P(None, ra),
            P(None, ra),
            P(None, ra),
        ),
        out_specs=P(None, ra),
        check_vma=False,
    )
```

```python
import jax
import jax.numpy as jnp
from jax import lax
from jax.experimental import pallas as pl
from jax.experimental.pallas import tpu as pltpu
from jax.sharding import Mesh, PartitionSpec as P


norm_eps = 1e-06
residual_keep = 0.5
Z, X, Y, C = 8, 4, 8, 2
bf16 = jnp.bfloat16
f32 = jnp.float32
VMEM = pl.BlockSpec(memory_space=pltpu.VMEM)
ANY = pl.BlockSpec(memory_space=pl.ANY)


def exchange(pieces, axis):
    return lax.all_to_all(pieces, axis, split_axis=0, concat_axis=0, tiled=True)


def to_all(shard, axis):
    size = lax.axis_size(axis)
    return exchange(jnp.broadcast_to(shard[None], (size, *shard.shape)), axis)


def activation(up):
    return jnp.square(jnp.maximum(up, 0.0)).astype(bf16)


def near(v):
    return pltpu.with_memory_space_constraint(v, pltpu.VMEM)


def far(v):
    return pltpu.with_memory_space_constraint(v, pltpu.HBM)


def after(blocks, value):
    return [lax.optimization_barrier((b, value))[0] for b in blocks]


def limit(mib):
    return pltpu.CompilerParams(vmem_limit_bytes=mib << 20)


def up_kernel(tokens_ref, gain_ref, weight_ref, scale_ref, down_ref, out_ref, first_ref, *scratch):
    tokens, gain, weight, scale, down, out, first, in_sems, weight_sems, out_sems = scratch
    parts, feats, step = weight.shape
    small = [
        pltpu.make_async_copy(tokens_ref, tokens, in_sems.at[0]),
        pltpu.make_async_copy(gain_ref, gain, in_sems.at[1]),
        pltpu.make_async_copy(scale_ref, scale, in_sems.at[2]),
    ]
    for copy in small:
        copy.start()
    copies = []
    for i in range(parts):
        here = weight_ref.at[0, :, pl.ds(i * step, step)]
        copies.append(pltpu.make_async_copy(here, weight.at[i], weight_sems.at[i]))
        copies[-1].start()
    down_copy = pltpu.make_async_copy(down_ref.at[0], down, in_sems.at[3])
    down_copy.start()
    for copy in small:
        copy.wait()
    scaled = (tokens[...].astype(f32) * gain[0:1]).astype(bf16)
    sent = []
    for i in range(parts):
        copies[i].wait()
        part = jnp.dot(scaled, weight[i].astype(bf16), preferred_element_type=f32)
        part = (part * scale[0:1, i * step : (i + 1) * step]).astype(bf16)
        for c in range(step // feats):
            z = i * (step // feats) + c
            out[z] = part[:, c * feats : (c + 1) * feats]
            sent.append(pltpu.make_async_copy(out.at[z], out_ref.at[z], out_sems.at[z]))
            sent[-1].start()
    down_copy.wait()
    first[...] = down[...].astype(bf16).reshape(first.shape)
    sent.append(pltpu.make_async_copy(first, first_ref, in_sems.at[4]))
    sent[-1].start()
    for copy in sent:
        copy.wait()


def up_product(tokens, gain, weight, scale, down_weight):
    n_tok, feats = tokens.shape
    hid = weight.shape[2]
    parts = 4
    blocks = (hid // feats, feats, feats)
    return pl.pallas_call(
        up_kernel,
        out_shape=(pltpu.HBM((Z, n_tok, hid // Z), bf16), pltpu.HBM(blocks, bf16)),
        in_specs=[ANY] * 5,
        out_specs=(ANY,) * 2,
        scratch_shapes=[
            pltpu.VMEM(tokens.shape, bf16),
            pltpu.VMEM(gain.shape, f32),
            pltpu.VMEM((parts, feats, hid // parts), f32),
            pltpu.VMEM(scale.shape, f32),
            pltpu.VMEM(down_weight.shape[1:], f32),
            pltpu.VMEM((Z, n_tok, hid // Z), bf16),
            pltpu.VMEM(blocks, bf16),
            pltpu.SemaphoreType.DMA((5,)),
            pltpu.SemaphoreType.DMA((parts,)),
            pltpu.SemaphoreType.DMA((Z,)),
        ],
        compiler_params=limit(12),
        name="up_product",
    )(*[far(v) for v in (tokens, gain, weight, scale, down_weight)])


def pack_kernel(down_ref, up_ref, tokens_ref, scale_ref, pre_ref, post_ref, *outs):
    own = outs[-1]
    hid, feats = down_ref.shape[1:]
    n = hid // feats
    t_x = own.shape[0] - 16
    x = lax.axis_index("x")
    scale, pre, post = scale_ref[...], pre_ref[...], post_ref[...]
    columns = [scale[0:1], post[0:1], pre[1:2], scale[1:2], post[1:2], jnp.zeros((3, feats), f32)]
    columns = jnp.concatenate(columns, axis=0)
    high = columns.astype(bf16).astype(f32)
    columns = jnp.concatenate([high, columns - high], axis=0).astype(bf16)
    rest = jnp.zeros((feats - 16 - t_x, feats), bf16)
    down = down_ref[0].astype(bf16).reshape(n, feats, feats)
    for s, ref in enumerate((own, *outs[:-1])):
        rows = pl.multiple_of(lax.rem(x + (X - s), X) * t_x, 32)
        block = [columns, tokens_ref[pl.ds(rows, t_x)]]
        if s == 0:
            ref[...] = jnp.concatenate(block, axis=0)
            continue
        for c in range(n):
            ref[c] = up_ref[0, :, c * feats : (c + 1) * feats].astype(bf16)
        ref[n : 2 * n] = down
        ref[2 * n] = jnp.concatenate([*block, rest], axis=0)


def packed(down_weight, up_weight, tokens, scale, pre, post):
    _, hid, feats = down_weight.shape
    t_x = tokens.shape[0] // X
    blocks = (2 * (hid // feats) + 1, feats, feats)
    whole = lambda v: pl.BlockSpec(v.shape, lambda i: (0,) * v.ndim)
    last_layer = lambda v: pl.BlockSpec((1, *v.shape[1:]), lambda i: (1, 0, 0))
    return pl.pallas_call(
        pack_kernel,
        grid=(1,),
        out_shape=(
            *(pltpu.HBM(blocks, bf16) for _ in range(X - 1)),
            pltpu.VMEM((16 + t_x, feats), bf16),
        ),
        in_specs=[
            last_layer(down_weight),
            last_layer(up_weight),
            *[whole(v) for v in (tokens, scale, pre, post)],
        ],
        out_specs=(
            *(pl.BlockSpec(blocks, lambda i: (0, 0, 0)) for _ in range(X - 1)),
            pl.BlockSpec((16 + t_x, feats), lambda i: (0, 0)),
        ),
        compiler_params=limit(20),
        name="packed",
    )(*[far(v) for v in (down_weight, up_weight, tokens, scale, pre, post)])


def down_kernel(start, rows, lead_ref, hidden_ref, *refs):
    weights, out_ref, held, sems = refs[:X], refs[X], refs[X + 1], refs[X + 2]
    copies = []
    for i, w in enumerate(weights):
        blocks = w.at[pl.ds(start, held.shape[1])]
        copies.append(pltpu.make_async_copy(blocks, held.at[i], sems.at[i]))
        copies[-1].start()
    hidden = [lead_ref[...].astype(bf16), *(hidden_ref[z] for z in range(1, Z))]
    hidden = jnp.concatenate(hidden, axis=1)
    for i in (1, 2, 3, 0):
        copies[i].wait()
        weight = held[i].reshape(hidden.shape[1], -1)
        part = jnp.dot(hidden, weight, preferred_element_type=f32)
        if not rows:
            out_ref[i] = part.astype(bf16)
            continue
        for k in range(Y * C):
            at = k * rows
            piece = part[at : at + rows] if at < part.shape[0] else jnp.zeros((rows, part.shape[1]))
            out_ref[k, i] = piece.astype(bf16)


def down_product(hidden, blocks, start, rows=0):
    _, t, share = hidden.shape
    feats = blocks[0].shape[2]
    lead = hidden[0].astype(f32)
    return pl.pallas_call(
        lambda *refs: down_kernel(start, rows, *refs),
        out_shape=pltpu.VMEM((Y * C, X, rows, feats) if rows else (X, t, feats), bf16),
        in_specs=[*[VMEM] * 2, *[ANY] * X],
        out_specs=VMEM,
        scratch_shapes=[
            pltpu.VMEM((X, Z * share // feats, feats, feats), bf16),
            pltpu.SemaphoreType.DMA((X,)),
        ],
        compiler_params=limit(8),
        name="down_product",
    )(near(lead), near(hidden), *blocks)


def down_share(hidden, blocks, start):
    part = down_product(hidden, blocks, start)
    pieces = part.reshape(Y * C, -1, part.shape[2])
    return exchange(pieces, ("y", "core")).astype(f32).sum(axis=0).astype(bf16)


def down_whole(mine):
    return to_all(mine, ("y", "core")).reshape(X, -1, mine.shape[1])


def squares_in_rows(values):
    total = 0.0
    for v in values:
        total += lax.dot_general(
            jnp.ones((8, v.shape[1]), f32),
            v * v,
            (((1,), (1,)), ((), ())),
            precision=lax.Precision.HIGHEST,
            preferred_element_type=f32,
        )
    return total


def inverse(row, width, t):
    inv = lax.rsqrt(row * (1.0 / width) + norm_eps)
    return jnp.transpose(jnp.broadcast_to(inv, (128, 128)))[:t]


def turn_kernel(lead_ref, sum_ref, own_ref, scale_ref, *refs):
    blocks = refs[:X]
    out_ref, kept_ref, branch_ref, columns_ref = refs[X : X + 4]
    extra, held, scales, sems, held_sems = refs[X + 4 :]
    t, feats = sum_ref.shape[1:]
    copies = [pltpu.make_async_copy(scale_ref, scales, sems.at[X - 1])]
    copies[0].start()
    for i in range(1, X):
        rows = blocks[i].at[2 * Z, pl.ds(0, extra.shape[1])]
        copies.append(pltpu.make_async_copy(rows, extra.at[i - 1], sems.at[i - 1]))
        copies[-1].start()
    held_copies = []
    for i in range(X):
        here = held.at[:, pl.ds(i * feats, feats)]
        held_copies.append(pltpu.make_async_copy(blocks[i].at[pl.ds(0, Z)], here, held_sems.at[i]))
        held_copies[-1].start()
    for copy in copies:
        copy.wait()
    kept_terms, branch_terms, branches = [], [], []
    for i in range(X):
        block = own_ref[...] if i == 0 else extra[i - 1]
        columns = block[:8].astype(f32) + block[8:16].astype(f32)
        columns_ref[i] = columns
        down_0, post_0, pre_1 = [columns[k : k + 1] for k in range(3)]
        kept = residual_keep * block[16:].astype(f32)
        branch_in = (lead_ref[...] if i == 0 else sum_ref[i].astype(f32)) * down_0
        branch = branch_in * post_0
        kept_ref[i] = kept
        branch_ref[i] = branch
        kept_terms.append((kept * pre_1).astype(bf16))
        branch_terms.append((branch * pre_1).astype(bf16))
        branches.append(branch_in)
    squares = squares_in_rows(branches)
    high = squares.astype(bf16).astype(f32)
    row = lax.broadcasted_iota(jnp.int32, squares.shape, 0)
    squares = jnp.where(row == 0, high, jnp.where(row == 1, squares - high, 0.0)).astype(bf16)
    terms = jnp.concatenate(
        [jnp.concatenate(kept_terms, axis=1), jnp.concatenate(branch_terms, axis=1)], axis=0
    )
    for copy in held_copies:
        copy.wait()
    for c in range(Z):
        part = jnp.dot(terms, held[c], preferred_element_type=f32)
        scale = scales[1:2, c * feats : (c + 1) * feats]
        out_ref[c, : 2 * t] = (part * scale).astype(bf16)
        out_ref[c, 2 * t :] = jnp.zeros((8, feats), bf16)
        out_ref[c, 2 * t :, :t] = squares


def turn(summed, own, scale, blocks):
    _, t, feats = summed.shape
    lead = summed[0].astype(f32)
    return pl.pallas_call(
        turn_kernel,
        out_shape=(
            pltpu.VMEM((Z, 2 * t + 8, feats), bf16),
            pltpu.VMEM((X, t, feats), f32),
            pltpu.VMEM((X, t, feats), f32),
            pltpu.VMEM((X, 8, feats), f32),
        ),
        in_specs=[*[VMEM] * 3, *[ANY] * (X + 1)],
        out_specs=(VMEM,) * 4,
        scratch_shapes=[
            pltpu.VMEM((X - 1, 16 + t, feats), bf16),
            pltpu.VMEM((Z, X * feats, feats), bf16),
            pltpu.VMEM(scale.shape, f32),
            pltpu.SemaphoreType.DMA((X,)),
            pltpu.SemaphoreType.DMA((X,)),
        ],
        compiler_params=limit(12),
        name="turn",
    )(near(lead), near(summed), near(own), far(scale), *blocks)


def hidden_kernel(width, came_ref, kept_ref, branch_ref, out_ref, stream_ref):
    t = out_ref.shape[1]
    total = came_ref[0].astype(f32)
    for z in range(1, Z):
        total += came_ref[z].astype(f32)
    inv = inverse(total[2 * t : 2 * t + 1] + total[2 * t + 1 : 2 * t + 2], width, t)
    hidden = activation(total[:t] + total[t : 2 * t] * inv)
    for z in range(Z):
        out_ref[z] = hidden
    for i in range(X):
        stream_ref[i] = (kept_ref[i] + branch_ref[i] * inv).astype(bf16).astype(f32)


def second_hidden(came, kept, branch, width):
    _, t, feats = kept.shape
    return pl.pallas_call(
        lambda *refs: hidden_kernel(width, *refs),
        out_shape=(pltpu.VMEM((Z, t, feats), bf16), pltpu.VMEM(kept.shape, f32)),
        in_specs=[VMEM] * 3,
        out_specs=(VMEM,) * 2,
        compiler_params=limit(8),
        name="second_hidden",
    )(near(came), near(kept), near(branch))


def share_kernel(sum_ref, columns_ref, stream_ref, out_ref):
    rows = sum_ref.shape[2]
    most = stream_ref.shape[1] // rows - 1
    mine = jnp.minimum(lax.axis_index("y") * C + lax.axis_index("core"), most)
    tokens = pl.ds(pl.multiple_of(mine * rows, rows), rows)
    branches = []
    for i in range(X):
        total = sum_ref[0, i].astype(f32)
        for k in range(1, Y * C):
            total += sum_ref[k, i].astype(f32)
        branches.append(total * columns_ref[i, 3:4])
    squares = squares_in_rows(branches)
    high = squares.astype(bf16).astype(f32)
    row = lax.broadcasted_iota(jnp.int32, squares.shape, 0)
    squares = jnp.where(row == 0, high, jnp.where(row == 1, squares - high, 0.0)).astype(bf16)
    x = lax.axis_index("x")
    for i in range(X):
        branch = (branches[i] * columns_ref[i, 4:5]).astype(bf16)
        stream = stream_ref[i, tokens].astype(bf16)
        owner = lax.rem(x + i, X)
        for z in range(Z):
            out_ref[z * X + owner, :rows] = branch
            out_ref[z * X + owner, rows : 2 * rows] = stream
            out_ref[z * X + owner, 2 * rows :] = jnp.zeros((8, branch.shape[1]), bf16)
            out_ref[z * X + owner, 2 * rows :, :rows] = squares


def shares(came, columns, stream):
    rows, feats = came.shape[2:]
    return pl.pallas_call(
        share_kernel,
        out_shape=pltpu.VMEM((Z * X, 2 * rows + 8, feats), bf16),
        in_specs=[VMEM] * 3,
        out_specs=VMEM,
        compiler_params=limit(8),
        name="shares",
    )(near(came), near(columns), near(stream))


def last_kernel(width, came_ref, out_ref):
    rows = out_ref.shape[2]
    z = lax.axis_index("z")
    for i in range(X):
        total = came_ref[i, 2 * rows :].astype(f32)
        for k in range(1, Z):
            total += came_ref[k * X + i, 2 * rows :].astype(f32)
        inv = inverse(total[0:1] + total[1:2], width, rows)
        block = came_ref[z * X + i].astype(f32)
        stream = residual_keep * block[rows : 2 * rows] + block[:rows] * inv
        for k in range(Y * C):
            out_ref[k, i] = stream.astype(bf16)


def last(came, rows, width):
    return pl.pallas_call(
        lambda *refs: last_kernel(width, *refs),
        out_shape=pltpu.VMEM((Y * C, X, rows, came.shape[2]), bf16),
        in_specs=[VMEM],
        out_specs=VMEM,
        compiler_params=limit(8),
        name="last",
    )(near(came))


def inner(tokens, up_weight, up_scale, down_weight, down_scale, pre_gain, post_gain):
    n_tok, feats = tokens.shape
    hid = up_weight.shape[2]
    width = feats * X * Z
    t_x = n_tok // X

    part, first = up_product(tokens, pre_gain, up_weight, up_scale, down_weight)
    part = part.reshape(Z * X, t_x, feats)
    summed = exchange(part, ("z", "x")).astype(f32).sum(axis=0)

    def from_x(payload, s):
        return lax.ppermute(payload, "x", [(i, (i - s) % X) for i in range(X)])

    *payloads, own = packed(down_weight, up_weight, tokens, down_scale, pre_gain, post_gain)
    firsts = [from_x(first, s) for s in (1, 2, 3)]
    seconds = [from_x(payloads[s - 1], s) for s in (1, 2, 3)]

    hidden = to_all(activation(summed), "z")
    mine = down_share(hidden, [far(first), *after(firsts, hidden)], 0)
    summed = down_whole(mine)

    seconds = [far(payloads[0]), *after(seconds, summed)]
    part, kept, branch, columns = turn(summed, own, up_scale, seconds)
    came = exchange(part, "z")
    hidden, stream = second_hidden(came, kept, branch, width)
    hidden = exchange(hidden, "z")

    rows = 8
    part = down_product(hidden, seconds, hid // feats, rows)
    came = exchange(part, ("y", "core"))
    pieces = shares(came, columns, stream)
    came = exchange(pieces, ("z", "x"))
    out = last(came, rows, width)
    out = exchange(out, ("y", "core"))
    return out[: t_x // rows].transpose(1, 0, 2, 3).reshape(n_tok, feats)


def solution(mesh):
    split = Mesh(mesh.devices.reshape(Z, X, Y, C), ("z", "x", "y", "core"))
    ra, cb = ("z", "x"), ("y", "core")
    return jax.shard_map(
        inner,
        mesh=split,
        in_specs=(
            P(None, ra),
            P(None, ra, cb),
            P(None, cb),
            P(None, cb, ra),
            P(None, ra),
            P(None, ra),
            P(None, ra),
        ),
        out_specs=P(None, ra),
        check_vma=False,
    )
```

```python
import jax
import jax.numpy as jnp
from jax import lax
from jax.experimental import pallas as pl
from jax.experimental.pallas import tpu as pltpu
from jax.sharding import Mesh, PartitionSpec as P


norm_eps = 1e-06
residual_keep = 0.5
Z, X, Y, C = 8, 4, 8, 2
bf16 = jnp.bfloat16
f32 = jnp.float32
VMEM = pl.BlockSpec(memory_space=pltpu.VMEM)
ANY = pl.BlockSpec(memory_space=pl.ANY)


def exchange(pieces, axis):
    return lax.all_to_all(pieces, axis, split_axis=0, concat_axis=0, tiled=True)


def to_all(shard, axis):
    size = lax.axis_size(axis)
    return exchange(jnp.broadcast_to(shard[None], (size, *shard.shape)), axis)


def activation(up):
    return jnp.square(jnp.maximum(up, 0.0)).astype(bf16)


def near(v):
    return pltpu.with_memory_space_constraint(v, pltpu.VMEM)


def far(v):
    return pltpu.with_memory_space_constraint(v, pltpu.HBM)


def after(blocks, value):
    return [lax.optimization_barrier((b, value))[0] for b in blocks]


def limit(mib):
    return pltpu.CompilerParams(vmem_limit_bytes=mib << 20)


def up_kernel(tokens_ref, gain_ref, weight_ref, scale_ref, down_ref, out_ref, first_ref, *scratch):
    tokens, gain, weight, scale, down, out, first, in_sems, weight_sems, out_sems = scratch
    parts, feats, step = weight.shape
    small = [
        pltpu.make_async_copy(tokens_ref, tokens, in_sems.at[0]),
        pltpu.make_async_copy(gain_ref, gain, in_sems.at[1]),
        pltpu.make_async_copy(scale_ref, scale, in_sems.at[2]),
    ]
    for copy in small:
        copy.start()
    copies = []
    for i in range(parts):
        here = weight_ref.at[0, :, pl.ds(i * step, step)]
        copies.append(pltpu.make_async_copy(here, weight.at[i], weight_sems.at[i]))
        copies[-1].start()
    down_copy = pltpu.make_async_copy(down_ref.at[0], down, in_sems.at[3])
    down_copy.start()
    for copy in small:
        copy.wait()
    scaled = (tokens[...].astype(f32) * gain[0:1]).astype(bf16)
    sent = []
    for i in range(parts):
        copies[i].wait()
        part = jnp.dot(scaled, weight[i].astype(bf16), preferred_element_type=f32)
        part = (part * scale[0:1, i * step : (i + 1) * step]).astype(bf16)
        for c in range(step // feats):
            z = i * (step // feats) + c
            out[z] = part[:, c * feats : (c + 1) * feats]
            sent.append(pltpu.make_async_copy(out.at[z], out_ref.at[z], out_sems.at[z]))
            sent[-1].start()
    down_copy.wait()
    first[...] = down[...].astype(bf16).reshape(first.shape)
    sent.append(pltpu.make_async_copy(first, first_ref, in_sems.at[4]))
    sent[-1].start()
    for copy in sent:
        copy.wait()


def up_product(tokens, gain, weight, scale, down_weight):
    n_tok, feats = tokens.shape
    hid = weight.shape[2]
    parts = 4
    blocks = (hid // feats, feats, feats)
    return pl.pallas_call(
        up_kernel,
        out_shape=(pltpu.HBM((Z, n_tok, hid // Z), bf16), pltpu.HBM(blocks, bf16)),
        in_specs=[ANY] * 5,
        out_specs=(ANY,) * 2,
        scratch_shapes=[
            pltpu.VMEM(tokens.shape, bf16),
            pltpu.VMEM(gain.shape, f32),
            pltpu.VMEM((parts, feats, hid // parts), f32),
            pltpu.VMEM(scale.shape, f32),
            pltpu.VMEM(down_weight.shape[1:], f32),
            pltpu.VMEM((Z, n_tok, hid // Z), bf16),
            pltpu.VMEM(blocks, bf16),
            pltpu.SemaphoreType.DMA((5,)),
            pltpu.SemaphoreType.DMA((parts,)),
            pltpu.SemaphoreType.DMA((Z,)),
        ],
        compiler_params=limit(12),
        name="up_product",
    )(*[far(v) for v in (tokens, gain, weight, scale, down_weight)])


def pack_kernel(down_ref, up_ref, tokens_ref, scale_ref, pre_ref, post_ref, *outs):
    own = outs[-1]
    hid, feats = down_ref.shape[1:]
    n = hid // feats
    t_x = own.shape[0] - 16
    x = lax.axis_index("x")
    scale, pre, post = scale_ref[...], pre_ref[...], post_ref[...]
    columns = [scale[0:1], post[0:1], pre[1:2], scale[1:2], post[1:2], jnp.zeros((3, feats), f32)]
    columns = jnp.concatenate(columns, axis=0)
    high = columns.astype(bf16).astype(f32)
    columns = jnp.concatenate([high, columns - high], axis=0).astype(bf16)
    rest = jnp.zeros((feats - 16 - t_x, feats), bf16)
    down = down_ref[0].astype(bf16).reshape(n, feats, feats)
    for s, ref in enumerate((own, *outs[:-1])):
        rows = pl.multiple_of(lax.rem(x + (X - s), X) * t_x, 32)
        block = [columns, tokens_ref[pl.ds(rows, t_x)]]
        if s == 0:
            ref[...] = jnp.concatenate(block, axis=0)
            continue
        for c in range(n):
            block_at = c % 2 * (n // 2) + c // 2
            ref[block_at] = up_ref[0, :, c * feats : (c + 1) * feats].astype(bf16)
        ref[n : 2 * n] = down
        ref[2 * n] = jnp.concatenate([*block, rest], axis=0)


def packed(down_weight, up_weight, tokens, scale, pre, post):
    _, hid, feats = down_weight.shape
    t_x = tokens.shape[0] // X
    blocks = (2 * (hid // feats) + 1, feats, feats)
    whole = lambda v: pl.BlockSpec(v.shape, lambda i: (0,) * v.ndim)
    last_layer = lambda v: pl.BlockSpec((1, *v.shape[1:]), lambda i: (1, 0, 0))
    return pl.pallas_call(
        pack_kernel,
        grid=(1,),
        out_shape=(
            *(pltpu.HBM(blocks, bf16) for _ in range(X - 1)),
            pltpu.VMEM((16 + t_x, feats), bf16),
        ),
        in_specs=[
            last_layer(down_weight),
            last_layer(up_weight),
            *[whole(v) for v in (tokens, scale, pre, post)],
        ],
        out_specs=(
            *(pl.BlockSpec(blocks, lambda i: (0, 0, 0)) for _ in range(X - 1)),
            pl.BlockSpec((16 + t_x, feats), lambda i: (0, 0)),
        ),
        compiler_params=limit(20),
        name="packed",
    )(*[far(v) for v in (down_weight, up_weight, tokens, scale, pre, post)])


def down_kernel(start, lead_ref, hidden_ref, *refs):
    weights, out_ref, held, sems = refs[:X], refs[X], refs[X + 1], refs[X + 2]
    feats = out_ref.shape[2]
    copies = []
    for i, w in enumerate(weights):
        here = held.at[i // 2, :, :, pl.ds(i % 2 * feats, feats)]
        copies.append(pltpu.make_async_copy(w.at[pl.ds(start, held.shape[1])], here, sems.at[i]))
        copies[-1].start()
    hidden = [lead_ref[...].astype(bf16), *(hidden_ref[z] for z in range(1, Z))]
    hidden = jnp.concatenate(hidden, axis=1)
    for pair in (1, 0):
        for i in (2 * pair, 2 * pair + 1):
            copies[i].wait()
        weight = held[pair].reshape(hidden.shape[1], 2 * feats)
        part = jnp.dot(hidden, weight, preferred_element_type=f32).astype(bf16)
        out_ref[2 * pair] = part[:, :feats]
        out_ref[2 * pair + 1] = part[:, feats:]


def down_product(hidden, blocks, start):
    _, t, share = hidden.shape
    feats = blocks[0].shape[2]
    lead = hidden[0].astype(f32)
    return pl.pallas_call(
        lambda *refs: down_kernel(start, *refs),
        out_shape=pltpu.VMEM((X, t, feats), bf16),
        in_specs=[*[VMEM] * 2, *[ANY] * X],
        out_specs=VMEM,
        scratch_shapes=[
            pltpu.VMEM((X // 2, Z * share // feats, feats, 2 * feats), bf16),
            pltpu.SemaphoreType.DMA((X,)),
        ],
        compiler_params=limit(8),
        name="down_product",
    )(near(lead), near(hidden), *blocks)


def down_share(hidden, blocks, start):
    part = down_product(hidden, blocks, start)
    pieces = part.reshape(Y * C, -1, part.shape[2])
    return exchange(pieces, ("y", "core")).astype(f32).sum(axis=0).astype(bf16)


def down_whole(mine):
    return to_all(mine, ("y", "core")).reshape(X, -1, mine.shape[1])


def squares_in_rows(values):
    total = 0.0
    for v in values:
        total += lax.dot_general(
            jnp.ones((8, v.shape[1]), f32),
            v * v,
            (((1,), (1,)), ((), ())),
            precision=lax.Precision.HIGHEST,
            preferred_element_type=f32,
        )
    return total


def inverse(row, width, t):
    inv = lax.rsqrt(row * (1.0 / width) + norm_eps)
    return jnp.transpose(jnp.broadcast_to(inv, (128, 128)))[:t]


def turn_kernel(lead_ref, sum_ref, own_ref, scale_ref, *refs):
    blocks = refs[:X]
    out_ref, kept_ref, branch_ref, columns_ref = refs[X : X + 4]
    extra, held, scales, sems, held_sems = refs[X + 4 :]
    t, feats = sum_ref.shape[1:]
    copies = [pltpu.make_async_copy(scale_ref, scales, sems.at[X - 1])]
    copies[0].start()
    for i in range(1, X):
        rows = blocks[i].at[2 * Z, pl.ds(0, extra.shape[1])]
        copies.append(pltpu.make_async_copy(rows, extra.at[i - 1], sems.at[i - 1]))
        copies[-1].start()
    held_copies = []
    for i in range(X):
        for odd in range(2):
            here = held.at[:, pl.ds(i * feats, feats), pl.ds(odd * feats, feats)]
            half = blocks[i].at[pl.ds(odd * Z // 2, Z // 2)]
            held_copies.append(pltpu.make_async_copy(half, here, held_sems.at[i, odd]))
            held_copies[-1].start()
    for copy in copies:
        copy.wait()
    kept_terms, branch_terms, branches = [], [], []
    for i in range(X):
        block = own_ref[...] if i == 0 else extra[i - 1]
        columns = block[:8].astype(f32) + block[8:16].astype(f32)
        columns_ref[i] = columns
        down_0, post_0, pre_1 = [columns[k : k + 1] for k in range(3)]
        kept = residual_keep * block[16:].astype(f32)
        branch_in = (lead_ref[...] if i == 0 else sum_ref[i].astype(f32)) * down_0
        branch = branch_in * post_0
        kept_ref[i] = kept
        branch_ref[i] = branch
        kept_terms.append((kept * pre_1).astype(bf16))
        branch_terms.append((branch * pre_1).astype(bf16))
        branches.append(branch_in)
    squares = squares_in_rows(branches)
    high = squares.astype(bf16).astype(f32)
    row = lax.broadcasted_iota(jnp.int32, squares.shape, 0)
    squares = jnp.where(row == 0, high, jnp.where(row == 1, squares - high, 0.0)).astype(bf16)
    terms = jnp.concatenate(
        [jnp.concatenate(kept_terms, axis=1), jnp.concatenate(branch_terms, axis=1)], axis=0
    )
    for copy in held_copies:
        copy.wait()
    for pair in range(Z // 2):
        part = jnp.dot(terms, held[pair], preferred_element_type=f32)
        scale = scales[1:2, pair * 2 * feats : (pair + 1) * 2 * feats]
        part = (part * scale).astype(bf16)
        for c in (2 * pair, 2 * pair + 1):
            at = c % 2 * feats
            out_ref[c, : 2 * t] = part[:, at : at + feats]
            out_ref[c, 2 * t :] = jnp.zeros((8, feats), bf16)
            out_ref[c, 2 * t :, :t] = squares


def turn(summed, own, scale, blocks):
    _, t, feats = summed.shape
    lead = summed[0].astype(f32)
    return pl.pallas_call(
        turn_kernel,
        out_shape=(
            pltpu.VMEM((Z, 2 * t + 8, feats), bf16),
            pltpu.VMEM((X, t, feats), f32),
            pltpu.VMEM((X, t, feats), f32),
            pltpu.VMEM((X, 8, feats), f32),
        ),
        in_specs=[*[VMEM] * 3, *[ANY] * (X + 1)],
        out_specs=(VMEM,) * 4,
        scratch_shapes=[
            pltpu.VMEM((X - 1, 16 + t, feats), bf16),
            pltpu.VMEM((Z // 2, X * feats, 2 * feats), bf16),
            pltpu.VMEM(scale.shape, f32),
            pltpu.SemaphoreType.DMA((X,)),
            pltpu.SemaphoreType.DMA((X, 2)),
        ],
        compiler_params=limit(12),
        name="turn",
    )(near(lead), near(summed), near(own), far(scale), *blocks)


def hidden_kernel(width, came_ref, kept_ref, branch_ref, out_ref, stream_ref):
    t = out_ref.shape[1]
    total = came_ref[0].astype(f32)
    for z in range(1, Z):
        total += came_ref[z].astype(f32)
    inv = inverse(total[2 * t : 2 * t + 1] + total[2 * t + 1 : 2 * t + 2], width, t)
    hidden = activation(total[:t] + total[t : 2 * t] * inv)
    for z in range(Z):
        out_ref[z] = hidden
    for i in range(X):
        stream_ref[i] = (kept_ref[i] + branch_ref[i] * inv).astype(bf16)


def second_hidden(came, kept, branch, width):
    _, t, feats = kept.shape
    return pl.pallas_call(
        lambda *refs: hidden_kernel(width, *refs),
        out_shape=(pltpu.VMEM((Z, t, feats), bf16), pltpu.VMEM(kept.shape, bf16)),
        in_specs=[VMEM] * 3,
        out_specs=(VMEM,) * 2,
        compiler_params=limit(8),
        name="second_hidden",
    )(near(came), near(kept), near(branch))


def squares_kernel(sum_ref, columns_ref, out_ref):
    t = sum_ref.shape[1]
    values = [sum_ref[i].astype(f32) * columns_ref[i, 3:4] for i in range(X)]
    squares = squares_in_rows(values)
    for z in range(Z):
        out_ref[z] = jnp.zeros(out_ref.shape[1:], f32)
        out_ref[z, :, :t] = squares


def squares_of(summed, columns):
    return pl.pallas_call(
        squares_kernel,
        out_shape=pltpu.VMEM((Z, 8, summed.shape[2]), f32),
        in_specs=[VMEM] * 2,
        out_specs=VMEM,
        compiler_params=limit(8),
        name="squares",
    )(near(summed), near(columns))


def last_kernel(width, squares_ref, sum_ref, columns_ref, stream_ref, out_ref):
    t = sum_ref.shape[1]
    total = squares_ref[0]
    for z in range(1, Z):
        total += squares_ref[z]
    inv = inverse(total[0:1], width, t)
    x = lax.axis_index("x")
    for i in range(X):
        branch = sum_ref[i].astype(f32) * columns_ref[i, 3:4] * inv * columns_ref[i, 4:5]
        stream = residual_keep * stream_ref[i].astype(f32) + branch
        out_ref[lax.rem(x + i, X)] = stream.astype(bf16)


def last(squares, summed, columns, stream, width):
    return pl.pallas_call(
        lambda *refs: last_kernel(width, *refs),
        out_shape=pltpu.VMEM(summed.shape, bf16),
        in_specs=[VMEM] * 4,
        out_specs=VMEM,
        compiler_params=limit(8),
        name="last",
    )(near(squares), near(summed), near(columns), near(stream))


def inner(tokens, up_weight, up_scale, down_weight, down_scale, pre_gain, post_gain):
    n_tok, feats = tokens.shape
    hid = up_weight.shape[2]
    width = feats * X * Z
    t_x = n_tok // X

    part, first = up_product(tokens, pre_gain, up_weight, up_scale, down_weight)
    part = part.reshape(Z * X, t_x, feats)
    summed = exchange(part, ("z", "x")).astype(f32).sum(axis=0)

    def from_x(payload, s):
        return lax.ppermute(payload, "x", [(i, (i - s) % X) for i in range(X)])

    *payloads, own = packed(down_weight, up_weight, tokens, down_scale, pre_gain, post_gain)
    firsts = [from_x(first, s) for s in (1, 2, 3)]
    seconds = [from_x(payloads[s - 1], s) for s in (1, 2, 3)]

    hidden = to_all(activation(summed), "z")
    mine = down_share(hidden, [far(first), *after(firsts, hidden)], 0)
    summed = down_whole(mine)

    seconds = [far(payloads[0]), *after(seconds, summed)]
    part, kept, branch, columns = turn(summed, own, up_scale, seconds)
    came = exchange(part, "z")
    hidden, stream = second_hidden(came, kept, branch, width)
    hidden = exchange(hidden, "z")
    mine = down_share(hidden, seconds, hid // feats)
    summed = down_whole(mine)

    squares = squares_of(summed, columns)
    squares = exchange(squares, "z")
    out = last(squares, summed, columns, stream, width)
    return exchange(out, "x").reshape(n_tok, feats)


def solution(mesh):
    split = Mesh(mesh.devices.reshape(Z, X, Y, C), ("z", "x", "y", "core"))
    ra, cb = ("z", "x"), ("y", "core")
    return jax.shard_map(
        inner,
        mesh=split,
        in_specs=(
            P(None, ra),
            P(None, ra, cb),
            P(None, cb),
            P(None, cb, ra),
            P(None, ra),
            P(None, ra),
            P(None, ra),
        ),
        out_specs=P(None, ra),
        check_vma=False,
    )
```

```python
import jax
import jax.numpy as jnp
from jax import lax
from jax.experimental import pallas as pl
from jax.experimental.pallas import tpu as pltpu
from jax.sharding import Mesh, PartitionSpec as P


norm_eps = 1e-06
residual_keep = 0.5
Z, X, Y, C = 8, 4, 8, 2
bf16 = jnp.bfloat16
f32 = jnp.float32
VMEM = pl.BlockSpec(memory_space=pltpu.VMEM)
ANY = pl.BlockSpec(memory_space=pl.ANY)


def exchange(pieces, axis):
    return lax.all_to_all(pieces, axis, split_axis=0, concat_axis=0, tiled=True)


def to_all(shard, axis):
    size = lax.axis_size(axis)
    return exchange(jnp.broadcast_to(shard[None], (size, *shard.shape)), axis)


def activation(up):
    return jnp.square(jnp.maximum(up, 0.0)).astype(bf16)


def near(v):
    return pltpu.with_memory_space_constraint(v, pltpu.VMEM)


def far(v):
    return pltpu.with_memory_space_constraint(v, pltpu.HBM)


def after(blocks, value):
    return [lax.optimization_barrier((b, value))[0] for b in blocks]


def limit(mib):
    return pltpu.CompilerParams(vmem_limit_bytes=mib << 20)


def up_kernel(tokens_ref, gain_ref, weight_ref, scale_ref, down_ref, out_ref, first_ref, *scratch):
    tokens, gain, weight, scale, down, out, first, in_sems, weight_sems, out_sems = scratch
    parts, feats, step = weight.shape
    small = [
        pltpu.make_async_copy(tokens_ref, tokens, in_sems.at[0]),
        pltpu.make_async_copy(gain_ref, gain, in_sems.at[1]),
        pltpu.make_async_copy(scale_ref, scale, in_sems.at[2]),
    ]
    for copy in small:
        copy.start()
    copies = []
    for i in range(parts):
        here = weight_ref.at[0, :, pl.ds(i * step, step)]
        copies.append(pltpu.make_async_copy(here, weight.at[i], weight_sems.at[i]))
        copies[-1].start()
    down_copy = pltpu.make_async_copy(down_ref.at[0], down, in_sems.at[3])
    down_copy.start()
    for copy in small:
        copy.wait()
    scaled = (tokens[...].astype(f32) * gain[0:1]).astype(bf16)
    sent = []
    for i in range(parts):
        copies[i].wait()
        part = jnp.dot(scaled, weight[i].astype(bf16), preferred_element_type=f32)
        part = (part * scale[0:1, i * step : (i + 1) * step]).astype(bf16)
        for c in range(step // feats):
            z = i * (step // feats) + c
            out[z] = part[:, c * feats : (c + 1) * feats]
            sent.append(pltpu.make_async_copy(out.at[z], out_ref.at[z], out_sems.at[z]))
            sent[-1].start()
    down_copy.wait()
    first[...] = down[...].astype(bf16).reshape(first.shape)
    sent.append(pltpu.make_async_copy(first, first_ref, in_sems.at[4]))
    sent[-1].start()
    for copy in sent:
        copy.wait()


def up_product(tokens, gain, weight, scale, down_weight):
    n_tok, feats = tokens.shape
    hid = weight.shape[2]
    parts = 4
    blocks = (hid // feats, feats, feats)
    return pl.pallas_call(
        up_kernel,
        out_shape=(pltpu.HBM((Z, n_tok, hid // Z), bf16), pltpu.HBM(blocks, bf16)),
        in_specs=[ANY] * 5,
        out_specs=(ANY,) * 2,
        scratch_shapes=[
            pltpu.VMEM(tokens.shape, bf16),
            pltpu.VMEM(gain.shape, f32),
            pltpu.VMEM((parts, feats, hid // parts), f32),
            pltpu.VMEM(scale.shape, f32),
            pltpu.VMEM(down_weight.shape[1:], f32),
            pltpu.VMEM((Z, n_tok, hid // Z), bf16),
            pltpu.VMEM(blocks, bf16),
            pltpu.SemaphoreType.DMA((5,)),
            pltpu.SemaphoreType.DMA((parts,)),
            pltpu.SemaphoreType.DMA((Z,)),
        ],
        compiler_params=limit(12),
        name="up_product",
    )(*[far(v) for v in (tokens, gain, weight, scale, down_weight)])


def pack_kernel(down_ref, up_ref, tokens_ref, scale_ref, pre_ref, post_ref, *outs):
    own = outs[-1]
    hid, feats = down_ref.shape[1:]
    n = hid // feats
    t_x = own.shape[0] - 16
    x = lax.axis_index("x")
    scale, pre, post = scale_ref[...], pre_ref[...], post_ref[...]
    columns = [scale[0:1], post[0:1], pre[1:2], scale[1:2], post[1:2], jnp.zeros((3, feats), f32)]
    columns = jnp.concatenate(columns, axis=0)
    high = columns.astype(bf16).astype(f32)
    columns = jnp.concatenate([high, columns - high], axis=0).astype(bf16)
    rest = jnp.zeros((feats - 16 - t_x, feats), bf16)
    down = down_ref[0].astype(bf16).reshape(n, feats, feats)
    for s, ref in enumerate((own, *outs[:-1])):
        rows = pl.multiple_of(lax.rem(x + (X - s), X) * t_x, 32)
        block = [columns, tokens_ref[pl.ds(rows, t_x)]]
        if s == 0:
            ref[...] = jnp.concatenate(block, axis=0)
            continue
        for c in range(n):
            block_at = c % 2 * (n // 2) + c // 2
            ref[block_at] = up_ref[0, :, c * feats : (c + 1) * feats].astype(bf16)
        ref[n : 2 * n] = down
        ref[2 * n] = jnp.concatenate([*block, rest], axis=0)


def packed(down_weight, up_weight, tokens, scale, pre, post):
    _, hid, feats = down_weight.shape
    t_x = tokens.shape[0] // X
    blocks = (2 * (hid // feats) + 1, feats, feats)
    whole = lambda v: pl.BlockSpec(v.shape, lambda i: (0,) * v.ndim)
    last_layer = lambda v: pl.BlockSpec((1, *v.shape[1:]), lambda i: (1, 0, 0))
    return pl.pallas_call(
        pack_kernel,
        grid=(1,),
        out_shape=(
            *(pltpu.HBM(blocks, bf16) for _ in range(X - 1)),
            pltpu.VMEM((16 + t_x, feats), bf16),
        ),
        in_specs=[
            last_layer(down_weight),
            last_layer(up_weight),
            *[whole(v) for v in (tokens, scale, pre, post)],
        ],
        out_specs=(
            *(pl.BlockSpec(blocks, lambda i: (0, 0, 0)) for _ in range(X - 1)),
            pl.BlockSpec((16 + t_x, feats), lambda i: (0, 0)),
        ),
        compiler_params=limit(20),
        name="packed",
    )(*[far(v) for v in (down_weight, up_weight, tokens, scale, pre, post)])


def down_kernel(start, rows, lead_ref, hidden_ref, *refs):
    weights, out_ref, held, sems = refs[:X], refs[X], refs[X + 1], refs[X + 2]
    copies = []
    for i, w in enumerate(weights):
        blocks = w.at[pl.ds(start, held.shape[1])]
        copies.append(pltpu.make_async_copy(blocks, held.at[i], sems.at[i]))
        copies[-1].start()
    hidden = [lead_ref[...].astype(bf16), *(hidden_ref[z] for z in range(1, Z))]
    hidden = jnp.concatenate(hidden, axis=1)
    for i in (1, 2, 3, 0):
        copies[i].wait()
        weight = held[i].reshape(hidden.shape[1], -1)
        part = jnp.dot(hidden, weight, preferred_element_type=f32)
        if not rows:
            out_ref[i] = part.astype(bf16)
            continue
        for k in range(Y * C):
            at = k * rows
            piece = part[at : at + rows] if at < part.shape[0] else jnp.zeros((rows, part.shape[1]))
            out_ref[k, i] = piece.astype(bf16)


def down_product(hidden, blocks, start, rows=0):
    _, t, share = hidden.shape
    feats = blocks[0].shape[2]
    lead = hidden[0].astype(f32)
    return pl.pallas_call(
        lambda *refs: down_kernel(start, rows, *refs),
        out_shape=pltpu.VMEM((Y * C, X, rows, feats) if rows else (X, t, feats), bf16),
        in_specs=[*[VMEM] * 2, *[ANY] * X],
        out_specs=VMEM,
        scratch_shapes=[
            pltpu.VMEM((X, Z * share // feats, feats, feats), bf16),
            pltpu.SemaphoreType.DMA((X,)),
        ],
        compiler_params=limit(8),
        name="down_product",
    )(near(lead), near(hidden), *blocks)


def down_share(hidden, blocks, start):
    part = down_product(hidden, blocks, start)
    pieces = part.reshape(Y * C, -1, part.shape[2])
    return exchange(pieces, ("y", "core")).astype(f32).sum(axis=0).astype(bf16)


def down_whole(mine):
    return to_all(mine, ("y", "core")).reshape(X, -1, mine.shape[1])


def squares_in_rows(values):
    total = 0.0
    for v in values:
        total += lax.dot_general(
            jnp.ones((8, v.shape[1]), f32),
            v * v,
            (((1,), (1,)), ((), ())),
            precision=lax.Precision.HIGHEST,
            preferred_element_type=f32,
        )
    return total


def inverse(row, width, t):
    inv = lax.rsqrt(row * (1.0 / width) + norm_eps)
    return jnp.transpose(jnp.broadcast_to(inv, (128, 128)))[:t]


def turn_kernel(lead_ref, sum_ref, own_ref, scale_ref, *refs):
    blocks = refs[:X]
    out_ref, kept_ref, branch_ref, columns_ref = refs[X : X + 4]
    extra, held, scales, sems, held_sems = refs[X + 4 :]
    t, feats = sum_ref.shape[1:]
    copies = [pltpu.make_async_copy(scale_ref, scales, sems.at[X - 1])]
    copies[0].start()
    for i in range(1, X):
        rows = blocks[i].at[2 * Z, pl.ds(0, extra.shape[1])]
        copies.append(pltpu.make_async_copy(rows, extra.at[i - 1], sems.at[i - 1]))
        copies[-1].start()
    held_copies = []
    for i in range(X):
        for odd in range(2):
            here = held.at[:, pl.ds(i * feats, feats), pl.ds(odd * feats, feats)]
            half = blocks[i].at[pl.ds(odd * Z // 2, Z // 2)]
            held_copies.append(pltpu.make_async_copy(half, here, held_sems.at[i, odd]))
            held_copies[-1].start()
    for copy in copies:
        copy.wait()
    kept_terms, branch_terms, branches = [], [], []
    for i in range(X):
        block = own_ref[...] if i == 0 else extra[i - 1]
        columns = block[:8].astype(f32) + block[8:16].astype(f32)
        columns_ref[i] = columns
        down_0, post_0, pre_1 = [columns[k : k + 1] for k in range(3)]
        kept = residual_keep * block[16:].astype(f32)
        branch_in = (lead_ref[...] if i == 0 else sum_ref[i].astype(f32)) * down_0
        branch = branch_in * post_0
        kept_ref[i] = kept
        branch_ref[i] = branch
        kept_terms.append((kept * pre_1).astype(bf16))
        branch_terms.append((branch * pre_1).astype(bf16))
        branches.append(branch_in)
    squares = squares_in_rows(branches)
    high = squares.astype(bf16).astype(f32)
    row = lax.broadcasted_iota(jnp.int32, squares.shape, 0)
    squares = jnp.where(row == 0, high, jnp.where(row == 1, squares - high, 0.0)).astype(bf16)
    terms = jnp.concatenate(
        [jnp.concatenate(kept_terms, axis=1), jnp.concatenate(branch_terms, axis=1)], axis=0
    )
    for copy in held_copies:
        copy.wait()
    for pair in range(Z // 2):
        part = jnp.dot(terms, held[pair], preferred_element_type=f32)
        scale = scales[1:2, pair * 2 * feats : (pair + 1) * 2 * feats]
        part = (part * scale).astype(bf16)
        for c in (2 * pair, 2 * pair + 1):
            at = c % 2 * feats
            out_ref[c, : 2 * t] = part[:, at : at + feats]
            out_ref[c, 2 * t :] = jnp.zeros((8, feats), bf16)
            out_ref[c, 2 * t :, :t] = squares


def turn(summed, own, scale, blocks):
    _, t, feats = summed.shape
    lead = summed[0].astype(f32)
    return pl.pallas_call(
        turn_kernel,
        out_shape=(
            pltpu.VMEM((Z, 2 * t + 8, feats), bf16),
            pltpu.VMEM((X, t, feats), f32),
            pltpu.VMEM((X, t, feats), f32),
            pltpu.VMEM((X, 8, feats), f32),
        ),
        in_specs=[*[VMEM] * 3, *[ANY] * (X + 1)],
        out_specs=(VMEM,) * 4,
        scratch_shapes=[
            pltpu.VMEM((X - 1, 16 + t, feats), bf16),
            pltpu.VMEM((Z // 2, X * feats, 2 * feats), bf16),
            pltpu.VMEM(scale.shape, f32),
            pltpu.SemaphoreType.DMA((X,)),
            pltpu.SemaphoreType.DMA((X, 2)),
        ],
        compiler_params=limit(12),
        name="turn",
    )(near(lead), near(summed), near(own), far(scale), *blocks)


def hidden_kernel(width, came_ref, kept_ref, branch_ref, out_ref, stream_ref):
    t = out_ref.shape[1]
    total = came_ref[0].astype(f32)
    for z in range(1, Z):
        total += came_ref[z].astype(f32)
    inv = inverse(total[2 * t : 2 * t + 1] + total[2 * t + 1 : 2 * t + 2], width, t)
    hidden = activation(total[:t] + total[t : 2 * t] * inv)
    for z in range(Z):
        out_ref[z] = hidden
    for i in range(X):
        stream_ref[i] = (kept_ref[i] + branch_ref[i] * inv).astype(bf16).astype(f32)


def second_hidden(came, kept, branch, width):
    _, t, feats = kept.shape
    return pl.pallas_call(
        lambda *refs: hidden_kernel(width, *refs),
        out_shape=(pltpu.VMEM((Z, t, feats), bf16), pltpu.VMEM(kept.shape, f32)),
        in_specs=[VMEM] * 3,
        out_specs=(VMEM,) * 2,
        compiler_params=limit(8),
        name="second_hidden",
    )(near(came), near(kept), near(branch))


def share_kernel(sum_ref, columns_ref, stream_ref, out_ref):
    rows = sum_ref.shape[2]
    most = stream_ref.shape[1] // rows - 1
    mine = jnp.minimum(lax.axis_index("y") * C + lax.axis_index("core"), most)
    tokens = pl.ds(pl.multiple_of(mine * rows, rows), rows)
    branches = []
    for i in range(X):
        total = sum_ref[0, i].astype(f32)
        for k in range(1, Y * C):
            total += sum_ref[k, i].astype(f32)
        branches.append(total * columns_ref[i, 3:4])
    squares = squares_in_rows(branches)
    high = squares.astype(bf16).astype(f32)
    row = lax.broadcasted_iota(jnp.int32, squares.shape, 0)
    squares = jnp.where(row == 0, high, jnp.where(row == 1, squares - high, 0.0)).astype(bf16)
    x = lax.axis_index("x")
    for i in range(X):
        branch = (branches[i] * columns_ref[i, 4:5]).astype(bf16)
        stream = stream_ref[i, tokens].astype(bf16)
        owner = lax.rem(x + i, X)
        for z in range(Z):
            out_ref[z * X + owner, :rows] = branch
            out_ref[z * X + owner, rows : 2 * rows] = stream
            out_ref[z * X + owner, 2 * rows :] = jnp.zeros((8, branch.shape[1]), bf16)
            out_ref[z * X + owner, 2 * rows :, :rows] = squares


def shares(came, columns, stream):
    rows, feats = came.shape[2:]
    return pl.pallas_call(
        share_kernel,
        out_shape=pltpu.VMEM((Z * X, 2 * rows + 8, feats), bf16),
        in_specs=[VMEM] * 3,
        out_specs=VMEM,
        compiler_params=limit(8),
        name="shares",
    )(near(came), near(columns), near(stream))


def last_kernel(width, came_ref, out_ref):
    rows = out_ref.shape[2]
    z = lax.axis_index("z")
    for i in range(X):
        total = came_ref[i, 2 * rows :].astype(f32)
        for k in range(1, Z):
            total += came_ref[k * X + i, 2 * rows :].astype(f32)
        inv = inverse(total[0:1] + total[1:2], width, rows)
        block = came_ref[z * X + i].astype(f32)
        stream = residual_keep * block[rows : 2 * rows] + block[:rows] * inv
        for k in range(Y * C):
            out_ref[k, i] = stream.astype(bf16)


def last(came, rows, width):
    return pl.pallas_call(
        lambda *refs: last_kernel(width, *refs),
        out_shape=pltpu.VMEM((Y * C, X, rows, came.shape[2]), bf16),
        in_specs=[VMEM],
        out_specs=VMEM,
        compiler_params=limit(8),
        name="last",
    )(near(came))


def inner(tokens, up_weight, up_scale, down_weight, down_scale, pre_gain, post_gain):
    n_tok, feats = tokens.shape
    hid = up_weight.shape[2]
    width = feats * X * Z
    t_x = n_tok // X

    part, first = up_product(tokens, pre_gain, up_weight, up_scale, down_weight)
    part = part.reshape(Z * X, t_x, feats)
    summed = exchange(part, ("z", "x")).astype(f32).sum(axis=0)

    def from_x(payload, s):
        return lax.ppermute(payload, "x", [(i, (i - s) % X) for i in range(X)])

    *payloads, own = packed(down_weight, up_weight, tokens, down_scale, pre_gain, post_gain)
    firsts = [from_x(first, s) for s in (1, 2, 3)]
    seconds = [from_x(payloads[s - 1], s) for s in (1, 2, 3)]

    hidden = to_all(activation(summed), "z")
    mine = down_share(hidden, [far(first), *after(firsts, hidden)], 0)
    summed = down_whole(mine)

    seconds = [far(payloads[0]), *after(seconds, summed)]
    part, kept, branch, columns = turn(summed, own, up_scale, seconds)
    came = exchange(part, "z")
    hidden, stream = second_hidden(came, kept, branch, width)
    hidden = exchange(hidden, "z")

    rows = 8
    part = down_product(hidden, seconds, hid // feats, rows)
    came = exchange(part, ("y", "core"))
    pieces = shares(came, columns, stream)
    came = exchange(pieces, ("z", "x"))
    out = last(came, rows, width)
    out = exchange(out, ("y", "core"))
    return out[: t_x // rows].transpose(1, 0, 2, 3).reshape(n_tok, feats)


def solution(mesh):
    split = Mesh(mesh.devices.reshape(Z, X, Y, C), ("z", "x", "y", "core"))
    ra, cb = ("z", "x"), ("y", "core")
    return jax.shard_map(
        inner,
        mesh=split,
        in_specs=(
            P(None, ra),
            P(None, ra, cb),
            P(None, cb),
            P(None, cb, ra),
            P(None, ra),
            P(None, ra),
            P(None, ra),
        ),
        out_specs=P(None, ra),
        check_vma=False,
    )
```

```python
import jax
import jax.numpy as jnp
from jax import lax
from jax.experimental import pallas as pl
from jax.experimental.pallas import tpu as pltpu
from jax.sharding import Mesh, PartitionSpec as P


norm_eps = 1e-06
residual_keep = 0.5
Z, X, Y, C = 8, 4, 8, 2
bf16 = jnp.bfloat16
f32 = jnp.float32
VMEM = pl.BlockSpec(memory_space=pltpu.VMEM)
ANY = pl.BlockSpec(memory_space=pl.ANY)


def exchange(pieces, axis):
    return lax.all_to_all(pieces, axis, split_axis=0, concat_axis=0, tiled=True)


def to_all(shard, axis):
    size = lax.axis_size(axis)
    return exchange(jnp.broadcast_to(shard[None], (size, *shard.shape)), axis)


def activation(up):
    return jnp.square(jnp.maximum(up, 0.0)).astype(bf16)


def near(v):
    return pltpu.with_memory_space_constraint(v, pltpu.VMEM)


def far(v):
    return pltpu.with_memory_space_constraint(v, pltpu.HBM)


def after(blocks, value):
    return [lax.optimization_barrier((b, value))[0] for b in blocks]


def limit(mib):
    return pltpu.CompilerParams(vmem_limit_bytes=mib << 20)


def up_kernel(tokens_ref, gain_ref, weight_ref, scale_ref, down_ref, out_ref, first_ref, *scratch):
    tokens, gain, weight, scale, down, out, first, in_sems, weight_sems, out_sems = scratch
    parts, feats, step = weight.shape
    small = [
        pltpu.make_async_copy(tokens_ref, tokens, in_sems.at[0]),
        pltpu.make_async_copy(gain_ref, gain, in_sems.at[1]),
        pltpu.make_async_copy(scale_ref, scale, in_sems.at[2]),
    ]
    for copy in small:
        copy.start()
    copies = []
    for i in range(parts):
        here = weight_ref.at[0, :, pl.ds(i * step, step)]
        copies.append(pltpu.make_async_copy(here, weight.at[i], weight_sems.at[i]))
        copies[-1].start()
    down_copy = pltpu.make_async_copy(down_ref.at[0], down, in_sems.at[3])
    down_copy.start()
    for copy in small:
        copy.wait()
    scaled = (tokens[...].astype(f32) * gain[0:1]).astype(bf16)
    sent = []
    for i in range(parts):
        if i == parts // 2:
            down_copy.wait()
            first[...] = down[...].astype(bf16).reshape(first.shape)
            sent.append(pltpu.make_async_copy(first, first_ref, in_sems.at[4]))
            sent[-1].start()
        copies[i].wait()
        part = jnp.dot(scaled, weight[i].astype(bf16), preferred_element_type=f32)
        part = (part * scale[0:1, i * step : (i + 1) * step]).astype(bf16)
        for c in range(step // feats):
            z = i * (step // feats) + c
            out[z] = part[:, c * feats : (c + 1) * feats]
            sent.append(pltpu.make_async_copy(out.at[z], out_ref.at[z], out_sems.at[z]))
            sent[-1].start()
    for copy in sent:
        copy.wait()


def up_product(tokens, gain, weight, scale, down_weight):
    n_tok, feats = tokens.shape
    hid = weight.shape[2]
    parts = 4
    blocks = (hid // feats, feats, feats)
    return pl.pallas_call(
        up_kernel,
        out_shape=(pltpu.HBM((Z, n_tok, hid // Z), bf16), pltpu.HBM(blocks, bf16)),
        in_specs=[ANY] * 5,
        out_specs=(ANY,) * 2,
        scratch_shapes=[
            pltpu.VMEM(tokens.shape, bf16),
            pltpu.VMEM(gain.shape, f32),
            pltpu.VMEM((parts, feats, hid // parts), f32),
            pltpu.VMEM(scale.shape, f32),
            pltpu.VMEM(down_weight.shape[1:], f32),
            pltpu.VMEM((Z, n_tok, hid // Z), bf16),
            pltpu.VMEM(blocks, bf16),
            pltpu.SemaphoreType.DMA((5,)),
            pltpu.SemaphoreType.DMA((parts,)),
            pltpu.SemaphoreType.DMA((Z,)),
        ],
        compiler_params=limit(12),
        name="up_product",
    )(*[far(v) for v in (tokens, gain, weight, scale, down_weight)])


def pack_kernel(down_ref, up_ref, tokens_ref, scale_ref, pre_ref, post_ref, *outs):
    own = outs[-1]
    hid, feats = down_ref.shape[1:]
    n = hid // feats
    t_x = own.shape[0] - 16
    x = lax.axis_index("x")
    scale, pre, post = scale_ref[...], pre_ref[...], post_ref[...]
    columns = [scale[0:1], post[0:1], pre[1:2], scale[1:2], post[1:2], jnp.zeros((3, feats), f32)]
    columns = jnp.concatenate(columns, axis=0)
    high = columns.astype(bf16).astype(f32)
    columns = jnp.concatenate([high, columns - high], axis=0).astype(bf16)
    rest = jnp.zeros((feats - 16 - t_x, feats), bf16)
    down = down_ref[0].astype(bf16).reshape(n, feats, feats)
    for s, ref in enumerate((own, *outs[:-1])):
        rows = pl.multiple_of(lax.rem(x + (X - s), X) * t_x, 32)
        block = [columns, tokens_ref[pl.ds(rows, t_x)]]
        if s == 0:
            ref[...] = jnp.concatenate(block, axis=0)
            continue
        for c in range(n):
            block_at = c % 2 * (n // 2) + c // 2
            ref[block_at] = up_ref[0, :, c * feats : (c + 1) * feats].astype(bf16)
        ref[n : 2 * n] = down
        ref[2 * n] = jnp.concatenate([*block, rest], axis=0)


def packed(down_weight, up_weight, tokens, scale, pre, post):
    _, hid, feats = down_weight.shape
    t_x = tokens.shape[0] // X
    blocks = (2 * (hid // feats) + 1, feats, feats)
    whole = lambda v: pl.BlockSpec(v.shape, lambda i: (0,) * v.ndim)
    last_layer = lambda v: pl.BlockSpec((1, *v.shape[1:]), lambda i: (1, 0, 0))
    return pl.pallas_call(
        pack_kernel,
        grid=(1,),
        out_shape=(
            *(pltpu.HBM(blocks, bf16) for _ in range(X - 1)),
            pltpu.VMEM((16 + t_x, feats), bf16),
        ),
        in_specs=[
            last_layer(down_weight),
            last_layer(up_weight),
            *[whole(v) for v in (tokens, scale, pre, post)],
        ],
        out_specs=(
            *(pl.BlockSpec(blocks, lambda i: (0, 0, 0)) for _ in range(X - 1)),
            pl.BlockSpec((16 + t_x, feats), lambda i: (0, 0)),
        ),
        compiler_params=limit(20),
        name="packed",
    )(*[far(v) for v in (down_weight, up_weight, tokens, scale, pre, post)])


def down_kernel(start, lead_ref, hidden_ref, own_ref, *refs):
    others, (out_ref, held, sem) = refs[: X - 1], refs[X - 1 :]
    n = held.shape[0]
    copy = pltpu.make_async_copy(own_ref.at[pl.ds(start, n)], held, sem)
    copy.start()
    hidden = [lead_ref[...].astype(bf16), *(hidden_ref[z] for z in range(1, Z))]
    hidden = jnp.concatenate(hidden, axis=1)
    for i in (1, 2, 3, 0):
        if i == 0:
            copy.wait()
        weight = others[i - 1][start : start + n] if i else held[...]
        weight = weight.reshape(hidden.shape[1], -1)
        out_ref[i] = jnp.dot(hidden, weight, preferred_element_type=f32).astype(bf16)


def down_product(hidden, blocks, start):
    _, t, share = hidden.shape
    feats = blocks[0].shape[2]
    lead = hidden[0].astype(f32)
    return pl.pallas_call(
        lambda *refs: down_kernel(start, *refs),
        out_shape=pltpu.VMEM((X, t, feats), bf16),
        in_specs=[*[VMEM] * 2, ANY, *[VMEM] * (X - 1)],
        out_specs=VMEM,
        scratch_shapes=[
            pltpu.VMEM((Z * share // feats, feats, feats), bf16),
            pltpu.SemaphoreType.DMA,
        ],
        compiler_params=limit(8),
        name="down_product",
    )(near(lead), near(hidden), blocks[0], *[near(b) for b in blocks[1:]])


def down_share(hidden, blocks, start):
    part = down_product(hidden, blocks, start)
    pieces = part.reshape(Y * C, -1, part.shape[2])
    return exchange(pieces, ("y", "core")).astype(f32).sum(axis=0).astype(bf16)


def down_whole(mine):
    return to_all(mine, ("y", "core")).reshape(X, -1, mine.shape[1])


def squares_in_rows(values):
    total = 0.0
    for v in values:
        total += lax.dot_general(
            jnp.ones((8, v.shape[1]), f32),
            v * v,
            (((1,), (1,)), ((), ())),
            precision=lax.Precision.HIGHEST,
            preferred_element_type=f32,
        )
    return total


def inverse(row, width, t):
    inv = lax.rsqrt(row * (1.0 / width) + norm_eps)
    return jnp.transpose(jnp.broadcast_to(inv, (128, 128)))[:t]


def turn_kernel(lead_ref, sum_ref, own_ref, scale_ref, *refs):
    blocks = refs[:X]
    out_ref, kept_ref, branch_ref, columns_ref = refs[X : X + 4]
    extra, held, scales, sems, held_sems = refs[X + 4 :]
    t, feats = sum_ref.shape[1:]
    copies = [pltpu.make_async_copy(scale_ref, scales, sems.at[X - 1])]
    copies[0].start()
    for i in range(1, X):
        rows = blocks[i].at[2 * Z, pl.ds(0, extra.shape[1])]
        copies.append(pltpu.make_async_copy(rows, extra.at[i - 1], sems.at[i - 1]))
        copies[-1].start()
    held_copies = []
    for i in range(X):
        for odd in range(2):
            here = held.at[:, pl.ds(i * feats, feats), pl.ds(odd * feats, feats)]
            half = blocks[i].at[pl.ds(odd * Z // 2, Z // 2)]
            held_copies.append(pltpu.make_async_copy(half, here, held_sems.at[i, odd]))
            held_copies[-1].start()
    for copy in copies:
        copy.wait()
    kept_terms, branch_terms, branches = [], [], []
    for i in range(X):
        block = own_ref[...] if i == 0 else extra[i - 1]
        columns = block[:8].astype(f32) + block[8:16].astype(f32)
        columns_ref[i] = columns
        down_0, post_0, pre_1 = [columns[k : k + 1] for k in range(3)]
        kept = residual_keep * block[16:].astype(f32)
        branch_in = (lead_ref[...] if i == 0 else sum_ref[i].astype(f32)) * down_0
        branch = branch_in * post_0
        kept_ref[i] = kept
        branch_ref[i] = branch
        kept_terms.append((kept * pre_1).astype(bf16))
        branch_terms.append((branch * pre_1).astype(bf16))
        branches.append(branch_in)
    squares = squares_in_rows(branches)
    high = squares.astype(bf16).astype(f32)
    row = lax.broadcasted_iota(jnp.int32, squares.shape, 0)
    squares = jnp.where(row == 0, high, jnp.where(row == 1, squares - high, 0.0)).astype(bf16)
    terms = jnp.concatenate(
        [jnp.concatenate(kept_terms, axis=1), jnp.concatenate(branch_terms, axis=1)], axis=0
    )
    for copy in held_copies:
        copy.wait()
    for pair in range(Z // 2):
        part = jnp.dot(terms, held[pair], preferred_element_type=f32)
        scale = scales[1:2, pair * 2 * feats : (pair + 1) * 2 * feats]
        part = (part * scale).astype(bf16)
        for c in (2 * pair, 2 * pair + 1):
            at = c % 2 * feats
            out_ref[c, : 2 * t] = part[:, at : at + feats]
            out_ref[c, 2 * t :] = jnp.zeros((8, feats), bf16)
            out_ref[c, 2 * t :, :t] = squares


def turn(summed, own, scale, blocks):
    _, t, feats = summed.shape
    lead = summed[0].astype(f32)
    return pl.pallas_call(
        turn_kernel,
        out_shape=(
            pltpu.VMEM((Z, 2 * t + 8, feats), bf16),
            pltpu.VMEM((X, t, feats), f32),
            pltpu.VMEM((X, t, feats), f32),
            pltpu.VMEM((X, 8, feats), f32),
        ),
        in_specs=[*[VMEM] * 3, *[ANY] * (X + 1)],
        out_specs=(VMEM,) * 4,
        scratch_shapes=[
            pltpu.VMEM((X - 1, 16 + t, feats), bf16),
            pltpu.VMEM((Z // 2, X * feats, 2 * feats), bf16),
            pltpu.VMEM(scale.shape, f32),
            pltpu.SemaphoreType.DMA((X,)),
            pltpu.SemaphoreType.DMA((X, 2)),
        ],
        compiler_params=limit(12),
        name="turn",
    )(near(lead), near(summed), near(own), far(scale), *blocks)


def hidden_kernel(width, came_ref, kept_ref, branch_ref, out_ref, stream_ref):
    t = out_ref.shape[1]
    total = came_ref[0].astype(f32)
    for z in range(1, Z):
        total += came_ref[z].astype(f32)
    inv = inverse(total[2 * t : 2 * t + 1] + total[2 * t + 1 : 2 * t + 2], width, t)
    hidden = activation(total[:t] + total[t : 2 * t] * inv)
    for z in range(Z):
        out_ref[z] = hidden
    for i in range(X):
        stream_ref[i] = (kept_ref[i] + branch_ref[i] * inv).astype(bf16)


def second_hidden(came, kept, branch, width):
    _, t, feats = kept.shape
    return pl.pallas_call(
        lambda *refs: hidden_kernel(width, *refs),
        out_shape=(pltpu.VMEM((Z, t, feats), bf16), pltpu.VMEM(kept.shape, bf16)),
        in_specs=[VMEM] * 3,
        out_specs=(VMEM,) * 2,
        compiler_params=limit(8),
        name="second_hidden",
    )(near(came), near(kept), near(branch))


def squares_kernel(sum_ref, columns_ref, out_ref):
    t = sum_ref.shape[1]
    values = [sum_ref[i].astype(f32) * columns_ref[i, 3:4] for i in range(X)]
    squares = squares_in_rows(values)
    for z in range(Z):
        out_ref[z] = jnp.zeros(out_ref.shape[1:], f32)
        out_ref[z, :, :t] = squares[0:1]


def squares_of(summed, columns):
    return pl.pallas_call(
        squares_kernel,
        out_shape=pltpu.VMEM((Z, 1, summed.shape[2]), f32),
        in_specs=[VMEM] * 2,
        out_specs=VMEM,
        compiler_params=limit(8),
        name="squares",
    )(near(summed), near(columns))


def last_kernel(width, squares_ref, sum_ref, columns_ref, stream_ref, out_ref):
    t = sum_ref.shape[1]
    total = squares_ref[0]
    for z in range(1, Z):
        total += squares_ref[z]
    inv = inverse(total[0:1], width, t)
    x = lax.axis_index("x")
    for i in range(X):
        branch = sum_ref[i].astype(f32) * columns_ref[i, 3:4] * inv * columns_ref[i, 4:5]
        stream = residual_keep * stream_ref[i].astype(f32) + branch
        out_ref[lax.rem(x + i, X)] = stream.astype(bf16)


def last(squares, summed, columns, stream, width):
    return pl.pallas_call(
        lambda *refs: last_kernel(width, *refs),
        out_shape=pltpu.VMEM(summed.shape, bf16),
        in_specs=[VMEM] * 4,
        out_specs=VMEM,
        compiler_params=limit(8),
        name="last",
    )(near(squares), near(summed), near(columns), near(stream))


def inner(tokens, up_weight, up_scale, down_weight, down_scale, pre_gain, post_gain):
    n_tok, feats = tokens.shape
    hid = up_weight.shape[2]
    width = feats * X * Z
    t_x = n_tok // X

    part, first = up_product(tokens, pre_gain, up_weight, up_scale, down_weight)
    part = part.reshape(Z * X, t_x, feats)
    summed = exchange(part, ("z", "x")).astype(f32).sum(axis=0)

    def from_x(payload, s):
        return lax.ppermute(payload, "x", [(i, (i - s) % X) for i in range(X)])

    *payloads, own = packed(down_weight, up_weight, tokens, down_scale, pre_gain, post_gain)
    firsts = [from_x(first, s) for s in (1, 2, 3)]
    seconds = [from_x(payloads[s - 1], s) for s in (1, 2, 3)]

    hidden = to_all(activation(summed), "z")
    mine = down_share(hidden, [far(first), *after(firsts, hidden)], 0)
    summed = down_whole(mine)

    seconds = [far(payloads[0]), *after(seconds, summed)]
    part, kept, branch, columns = turn(summed, own, up_scale, seconds)
    came = exchange(part, "z")
    hidden, stream = second_hidden(came, kept, branch, width)
    hidden = exchange(hidden, "z")
    mine = down_share(hidden, seconds, hid // feats)
    summed = down_whole(mine)

    squares = squares_of(summed, columns)
    squares = exchange(squares, "z")
    out = last(squares, summed, columns, stream, width)
    return exchange(out, "x").reshape(n_tok, feats)


def solution(mesh):
    split = Mesh(mesh.devices.reshape(Z, X, Y, C), ("z", "x", "y", "core"))
    ra, cb = ("z", "x"), ("y", "core")
    return jax.shard_map(
        inner,
        mesh=split,
        in_specs=(
            P(None, ra),
            P(None, ra, cb),
            P(None, cb),
            P(None, cb, ra),
            P(None, ra),
            P(None, ra),
            P(None, ra),
        ),
        out_specs=P(None, ra),
        check_vma=False,
    )
```

```python
import jax
import jax.numpy as jnp
from jax import lax
from jax.experimental import pallas as pl
from jax.experimental.pallas import tpu as pltpu
from jax.sharding import Mesh, PartitionSpec as P


norm_eps = 1e-06
residual_keep = 0.5
Z, X, Y, C = 8, 4, 8, 2
bf16 = jnp.bfloat16
f32 = jnp.float32
VMEM = pl.BlockSpec(memory_space=pltpu.VMEM)
ANY = pl.BlockSpec(memory_space=pl.ANY)


def exchange(pieces, axis):
    return lax.all_to_all(pieces, axis, split_axis=0, concat_axis=0, tiled=True)


def to_all(shard, axis):
    size = lax.axis_size(axis)
    return exchange(jnp.broadcast_to(shard[None], (size, *shard.shape)), axis)


def activation(up):
    return jnp.square(jnp.maximum(up, 0.0)).astype(bf16)


def near(v):
    return pltpu.with_memory_space_constraint(v, pltpu.VMEM)


def far(v):
    return pltpu.with_memory_space_constraint(v, pltpu.HBM)


def after(blocks, value):
    return [lax.optimization_barrier((b, value))[0] for b in blocks]


def limit(mib):
    return pltpu.CompilerParams(vmem_limit_bytes=mib << 20)


def up_kernel(tokens_ref, gain_ref, weight_ref, scale_ref, down_ref, out_ref, first_ref, *scratch):
    tokens, gain, weight, scale, down, out, first, in_sems, weight_sems, out_sems = scratch
    parts, feats, step = weight.shape
    small = [
        pltpu.make_async_copy(tokens_ref, tokens, in_sems.at[0]),
        pltpu.make_async_copy(gain_ref, gain, in_sems.at[1]),
        pltpu.make_async_copy(scale_ref, scale, in_sems.at[2]),
    ]
    for copy in small:
        copy.start()
    copies = []
    for i in range(parts):
        here = weight_ref.at[0, :, pl.ds(i * step, step)]
        copies.append(pltpu.make_async_copy(here, weight.at[i], weight_sems.at[i]))
        copies[-1].start()
    down_copy = pltpu.make_async_copy(down_ref.at[0], down, in_sems.at[3])
    down_copy.start()
    for copy in small:
        copy.wait()
    scaled = (tokens[...].astype(f32) * gain[0:1]).astype(bf16)
    sent = []
    for i in range(parts):
        if i == parts // 2:
            down_copy.wait()
            first[...] = down[...].astype(bf16).reshape(first.shape)
            sent.append(pltpu.make_async_copy(first, first_ref, in_sems.at[4]))
            sent[-1].start()
        copies[i].wait()
        part = jnp.dot(scaled, weight[i].astype(bf16), preferred_element_type=f32)
        part = (part * scale[0:1, i * step : (i + 1) * step]).astype(bf16)
        for c in range(step // feats):
            z = i * (step // feats) + c
            out[z] = part[:, c * feats : (c + 1) * feats]
            sent.append(pltpu.make_async_copy(out.at[z], out_ref.at[z], out_sems.at[z]))
            sent[-1].start()
    for copy in sent:
        copy.wait()


def up_product(tokens, gain, weight, scale, down_weight):
    n_tok, feats = tokens.shape
    hid = weight.shape[2]
    parts = 4
    blocks = (hid // feats, feats, feats)
    return pl.pallas_call(
        up_kernel,
        out_shape=(pltpu.HBM((Z, n_tok, hid // Z), bf16), pltpu.HBM(blocks, bf16)),
        in_specs=[ANY] * 5,
        out_specs=(ANY,) * 2,
        scratch_shapes=[
            pltpu.VMEM(tokens.shape, bf16),
            pltpu.VMEM(gain.shape, f32),
            pltpu.VMEM((parts, feats, hid // parts), f32),
            pltpu.VMEM(scale.shape, f32),
            pltpu.VMEM(down_weight.shape[1:], f32),
            pltpu.VMEM((Z, n_tok, hid // Z), bf16),
            pltpu.VMEM(blocks, bf16),
            pltpu.SemaphoreType.DMA((5,)),
            pltpu.SemaphoreType.DMA((parts,)),
            pltpu.SemaphoreType.DMA((Z,)),
        ],
        compiler_params=limit(12),
        name="up_product",
    )(*[far(v) for v in (tokens, gain, weight, scale, down_weight)])


def pack_kernel(down_ref, up_ref, tokens_ref, scale_ref, pre_ref, post_ref, *outs):
    own = outs[-1]
    hid, feats = down_ref.shape[1:]
    n = hid // feats
    t_x = own.shape[0] - 16
    x = lax.axis_index("x")
    scale, pre, post = scale_ref[...], pre_ref[...], post_ref[...]
    columns = [scale[0:1], post[0:1], pre[1:2], scale[1:2], post[1:2], jnp.zeros((3, feats), f32)]
    columns = jnp.concatenate(columns, axis=0)
    high = columns.astype(bf16).astype(f32)
    columns = jnp.concatenate([high, columns - high], axis=0).astype(bf16)
    rest = jnp.zeros((feats - 16 - t_x, feats), bf16)
    down = down_ref[0].astype(bf16).reshape(n, feats, feats)
    for s, ref in enumerate((own, *outs[:-1])):
        rows = pl.multiple_of(lax.rem(x + (X - s), X) * t_x, 32)
        block = [columns, tokens_ref[pl.ds(rows, t_x)]]
        if s == 0:
            ref[...] = jnp.concatenate(block, axis=0)
            continue
        for c in range(n):
            block_at = c % 2 * (n // 2) + c // 2
            ref[block_at] = up_ref[0, :, c * feats : (c + 1) * feats].astype(bf16)
        ref[n : 2 * n] = down
        ref[2 * n] = jnp.concatenate([*block, rest], axis=0)


def packed(down_weight, up_weight, tokens, scale, pre, post):
    _, hid, feats = down_weight.shape
    t_x = tokens.shape[0] // X
    blocks = (2 * (hid // feats) + 1, feats, feats)
    whole = lambda v: pl.BlockSpec(v.shape, lambda i: (0,) * v.ndim)
    last_layer = lambda v: pl.BlockSpec((1, *v.shape[1:]), lambda i: (1, 0, 0))
    return pl.pallas_call(
        pack_kernel,
        grid=(1,),
        out_shape=(
            *(pltpu.HBM(blocks, bf16) for _ in range(X - 1)),
            pltpu.VMEM((16 + t_x, feats), bf16),
        ),
        in_specs=[
            last_layer(down_weight),
            last_layer(up_weight),
            *[whole(v) for v in (tokens, scale, pre, post)],
        ],
        out_specs=(
            *(pl.BlockSpec(blocks, lambda i: (0, 0, 0)) for _ in range(X - 1)),
            pl.BlockSpec((16 + t_x, feats), lambda i: (0, 0)),
        ),
        compiler_params=limit(20),
        name="packed",
    )(*[far(v) for v in (down_weight, up_weight, tokens, scale, pre, post)])


def down_kernel(start, lead_ref, hidden_ref, *refs):
    weights, out_ref, held, sems = refs[:X], refs[X], refs[X + 1], refs[X + 2]
    copies = []
    for i, w in enumerate(weights):
        blocks = w.at[pl.ds(start, held.shape[1])]
        copies.append(pltpu.make_async_copy(blocks, held.at[i], sems.at[i]))
        copies[-1].start()
    hidden = [lead_ref[...].astype(bf16), *(hidden_ref[z] for z in range(1, Z))]
    hidden = jnp.concatenate(hidden, axis=1)
    for i in (1, 2, 3, 0):
        copies[i].wait()
        weight = held[i].reshape(hidden.shape[1], -1)
        out_ref[i] = jnp.dot(hidden, weight, preferred_element_type=f32).astype(bf16)


def down_product(hidden, blocks, start):
    _, t, share = hidden.shape
    feats = blocks[0].shape[2]
    lead = hidden[0].astype(f32)
    return pl.pallas_call(
        lambda *refs: down_kernel(start, *refs),
        out_shape=pltpu.VMEM((X, t, feats), bf16),
        in_specs=[*[VMEM] * 2, *[ANY] * X],
        out_specs=VMEM,
        scratch_shapes=[
            pltpu.VMEM((X, Z * share // feats, feats, feats), bf16),
            pltpu.SemaphoreType.DMA((X,)),
        ],
        compiler_params=limit(8),
        name="down_product",
    )(near(lead), near(hidden), *blocks)


def down_share(hidden, blocks, start):
    part = down_product(hidden, blocks, start)
    pieces = part.reshape(Y * C, -1, part.shape[2])
    return exchange(pieces, ("y", "core")).astype(f32).sum(axis=0).astype(bf16)


def down_whole(mine):
    return to_all(mine, ("y", "core")).reshape(X, -1, mine.shape[1])


def squares_in_rows(values):
    total = 0.0
    for v in values:
        total += lax.dot_general(
            jnp.ones((8, v.shape[1]), f32),
            v * v,
            (((1,), (1,)), ((), ())),
            precision=lax.Precision.HIGHEST,
            preferred_element_type=f32,
        )
    return total


def inverse(row, width, t):
    inv = lax.rsqrt(row * (1.0 / width) + norm_eps)
    return jnp.transpose(jnp.broadcast_to(inv, (128, 128)))[:t]


def turn_kernel(lead_ref, sum_ref, own_ref, scale_ref, *refs):
    blocks = refs[:X]
    out_ref, kept_ref, branch_ref, columns_ref = refs[X : X + 4]
    extra, held, scales, sems, held_sems = refs[X + 4 :]
    t, feats = sum_ref.shape[1:]
    copies = [pltpu.make_async_copy(scale_ref, scales, sems.at[X - 1])]
    copies[0].start()
    for i in range(1, X):
        rows = blocks[i].at[2 * Z, pl.ds(0, extra.shape[1])]
        copies.append(pltpu.make_async_copy(rows, extra.at[i - 1], sems.at[i - 1]))
        copies[-1].start()
    held_copies = []
    for i in range(X):
        for odd in range(2):
            here = held.at[:, pl.ds(i * feats, feats), pl.ds(odd * feats, feats)]
            half = blocks[i].at[pl.ds(odd * Z // 2, Z // 2)]
            held_copies.append(pltpu.make_async_copy(half, here, held_sems.at[i, odd]))
            held_copies[-1].start()
    for copy in copies:
        copy.wait()
    kept_terms, branch_terms, branches = [], [], []
    for i in range(X):
        block = own_ref[...] if i == 0 else extra[i - 1]
        columns = block[:8].astype(f32) + block[8:16].astype(f32)
        columns_ref[i] = columns
        down_0, post_0, pre_1 = [columns[k : k + 1] for k in range(3)]
        kept = residual_keep * block[16:].astype(f32)
        branch_in = (lead_ref[...] if i == 0 else sum_ref[i].astype(f32)) * down_0
        branch = branch_in * post_0
        kept_ref[i] = kept
        branch_ref[i] = branch
        kept_terms.append((kept * pre_1).astype(bf16))
        branch_terms.append((branch * pre_1).astype(bf16))
        branches.append(branch_in)
    squares = squares_in_rows(branches)
    high = squares.astype(bf16).astype(f32)
    row = lax.broadcasted_iota(jnp.int32, squares.shape, 0)
    squares = jnp.where(row == 0, high, jnp.where(row == 1, squares - high, 0.0)).astype(bf16)
    terms = jnp.concatenate(
        [jnp.concatenate(kept_terms, axis=1), jnp.concatenate(branch_terms, axis=1)], axis=0
    )
    for copy in held_copies:
        copy.wait()
    for pair in range(Z // 2):
        part = jnp.dot(terms, held[pair], preferred_element_type=f32)
        scale = scales[1:2, pair * 2 * feats : (pair + 1) * 2 * feats]
        part = (part * scale).astype(bf16)
        for c in (2 * pair, 2 * pair + 1):
            at = c % 2 * feats
            out_ref[c, : 2 * t] = part[:, at : at + feats]
            out_ref[c, 2 * t :] = jnp.zeros((8, feats), bf16)
            out_ref[c, 2 * t :, :t] = squares


def turn(summed, own, scale, blocks):
    _, t, feats = summed.shape
    lead = summed[0].astype(f32)
    return pl.pallas_call(
        turn_kernel,
        out_shape=(
            pltpu.VMEM((Z, 2 * t + 8, feats), bf16),
            pltpu.VMEM((X, t, feats), f32),
            pltpu.VMEM((X, t, feats), f32),
            pltpu.VMEM((X, 8, feats), f32),
        ),
        in_specs=[*[VMEM] * 3, *[ANY] * (X + 1)],
        out_specs=(VMEM,) * 4,
        scratch_shapes=[
            pltpu.VMEM((X - 1, 16 + t, feats), bf16),
            pltpu.VMEM((Z // 2, X * feats, 2 * feats), bf16),
            pltpu.VMEM(scale.shape, f32),
            pltpu.SemaphoreType.DMA((X,)),
            pltpu.SemaphoreType.DMA((X, 2)),
        ],
        compiler_params=limit(12),
        name="turn",
    )(near(lead), near(summed), near(own), far(scale), *blocks)


def hidden_kernel(width, came_ref, kept_ref, branch_ref, out_ref, stream_ref):
    t = out_ref.shape[1]
    total = came_ref[0].astype(f32)
    for z in range(1, Z):
        total += came_ref[z].astype(f32)
    inv = inverse(total[2 * t : 2 * t + 1] + total[2 * t + 1 : 2 * t + 2], width, t)
    hidden = activation(total[:t] + total[t : 2 * t] * inv)
    for z in range(Z):
        out_ref[z] = hidden
    for i in range(X):
        stream_ref[i] = (kept_ref[i] + branch_ref[i] * inv).astype(bf16)


def second_hidden(came, kept, branch, width):
    _, t, feats = kept.shape
    return pl.pallas_call(
        lambda *refs: hidden_kernel(width, *refs),
        out_shape=(pltpu.VMEM((Z, t, feats), bf16), pltpu.VMEM(kept.shape, bf16)),
        in_specs=[VMEM] * 3,
        out_specs=(VMEM,) * 2,
        compiler_params=limit(8),
        name="second_hidden",
    )(near(came), near(kept), near(branch))


def squares_kernel(sum_ref, columns_ref, out_ref):
    t = sum_ref.shape[1]
    values = [sum_ref[i].astype(f32) * columns_ref[i, 3:4] for i in range(X)]
    squares = squares_in_rows(values)
    for z in range(Z):
        out_ref[z] = jnp.zeros(out_ref.shape[1:], f32)
        out_ref[z, :, :t] = squares[0:1]


def squares_of(summed, columns):
    return pl.pallas_call(
        squares_kernel,
        out_shape=pltpu.VMEM((Z, 1, summed.shape[2]), f32),
        in_specs=[VMEM] * 2,
        out_specs=VMEM,
        compiler_params=limit(8),
        name="squares",
    )(near(summed), near(columns))


def last_kernel(width, squares_ref, sum_ref, columns_ref, stream_ref, out_ref):
    t = sum_ref.shape[1]
    total = squares_ref[0]
    for z in range(1, Z):
        total += squares_ref[z]
    inv = inverse(total[0:1], width, t)
    x = lax.axis_index("x")
    for i in range(X):
        branch = sum_ref[i].astype(f32) * columns_ref[i, 3:4] * inv * columns_ref[i, 4:5]
        stream = residual_keep * stream_ref[i].astype(f32) + branch
        out_ref[lax.rem(x + i, X)] = stream.astype(bf16)


def last(squares, summed, columns, stream, width):
    return pl.pallas_call(
        lambda *refs: last_kernel(width, *refs),
        out_shape=pltpu.VMEM(summed.shape, bf16),
        in_specs=[VMEM] * 4,
        out_specs=VMEM,
        compiler_params=limit(8),
        name="last",
    )(near(squares), near(summed), near(columns), near(stream))


def inner(tokens, up_weight, up_scale, down_weight, down_scale, pre_gain, post_gain):
    n_tok, feats = tokens.shape
    hid = up_weight.shape[2]
    width = feats * X * Z
    t_x = n_tok // X

    part, first = up_product(tokens, pre_gain, up_weight, up_scale, down_weight)
    part = part.reshape(Z * X, t_x, feats)
    summed = exchange(part, ("z", "x")).astype(f32).sum(axis=0)

    def from_x(payload, s):
        return lax.ppermute(payload, "x", [(i, (i - s) % X) for i in range(X)])

    *payloads, own = packed(down_weight, up_weight, tokens, down_scale, pre_gain, post_gain)
    firsts = [from_x(first, s) for s in (1, 2, 3)]
    seconds = [from_x(payloads[s - 1], s) for s in (1, 2, 3)]

    hidden = to_all(activation(summed), "z")
    mine = down_share(hidden, [far(first), *after(firsts, hidden)], 0)
    summed = down_whole(mine)

    seconds = [far(payloads[0]), *after(seconds, summed)]
    part, kept, branch, columns = turn(summed, own, up_scale, seconds)
    came = exchange(part, "z")
    hidden, stream = second_hidden(came, kept, branch, width)
    hidden = exchange(hidden, "z")
    mine = down_share(hidden, seconds, hid // feats)
    summed = down_whole(mine)

    squares = squares_of(summed, columns)
    squares = exchange(squares, "z")
    out = last(squares, summed, columns, stream, width)
    return exchange(out, "x").reshape(n_tok, feats)


def solution(mesh):
    split = Mesh(mesh.devices.reshape(Z, X, Y, C), ("z", "x", "y", "core"))
    ra, cb = ("z", "x"), ("y", "core")
    return jax.shard_map(
        inner,
        mesh=split,
        in_specs=(
            P(None, ra),
            P(None, ra, cb),
            P(None, cb),
            P(None, cb, ra),
            P(None, ra),
            P(None, ra),
            P(None, ra),
        ),
        out_specs=P(None, ra),
        check_vma=False,
    )
```
